32 devices in a mesh: sp: 8 (over z, y), tp: 4 (over x, core).
Axes of the slice: x: 2, y: 2, z: 4, core: 2. Of those that a mesh axis runs over, the one named last changes fastest.
Arguments:
- queries: bfloat16 [1024, 1280], P('sp', 'tp'), may hold values from -4000 to 4000
- latents: bfloat16 [1024, 512], P('sp'), may hold values from -6 to 6
- shared_key: bfloat16 [1024, 64], P('sp'), may hold values from -4 to 4
- expand_weight: bfloat16 [512, 1536], P(None, 'tp'), may hold values from -0.25 to 0.25
- residual: bfloat16 [1024, 2048], P('sp'), may hold values from -3 to 3
- out_weight: bfloat16 [768, 2048], replicated, may hold values from -0.21875 to 0.21875
- norm_gain: bfloat16 [2048], replicated, may hold values from 0.099609375 to 1.8984375
- gate_weight: bfloat16 [2048, 3072], P('sp', 'tp'), may hold values from -0.125 to 0.125
- value_weight: bfloat16 [2048, 3072], P('sp', 'tp'), may hold values from -0.125 to 0.125
- conv_weight: bfloat16 [3, 3072], P(None, 'tp'), may hold values from -3.5 to 3.5
- down_weight: bfloat16 [3072, 2048], P('tp', 'sp'), may hold values from -0.109375 to 0.109375
Outputs:
- output: bfloat16 [1024, 2048], P(('sp', 'tp'))
The draws below stay inside these ranges and needn't reach their ends.
All inputs are finite; a program needn't handle non-finite values.
Results may differ from the reference program's by a relative error of at most 0.018.
Values may be sent and summed in bfloat16 or wider, within the bound.
A program may use at most 128 MiB of HBM per device.

```python
import jax
import jax.numpy as jnp
from jax import lax

D = 2048
HEADS = 4
NOPE_A = 128
VAL_A = 128
NOPE_B = 64
VAL_B = 64
ROPE = 64
RANK = 512
FF = 3072
CONV = 3
TOK_DEV = 128
TOKENS = 1024


def shared_rows(key):
    drawn = jax.random.normal(jax.random.fold_in(key, 11), (TOKENS, ROPE), jnp.float32)
    return jnp.clip(drawn, -4.0, 4.0).astype(jnp.float32)


def draw_shared_key(key, part):
    return shared_rows(key).reshape(TOKENS, ROPE).astype(jnp.bfloat16)


def draw_queries(key, part):
    q_width = NOPE_A + NOPE_B + 2 * ROPE
    base_draw = jnp.clip(3.0 * jax.random.normal(jax.random.fold_in(key, 23), (TOKENS, HEADS, q_width), jnp.float32), -18.0, 18.0)
    return jnp.clip(base_draw, -4000.0, 4000.0).reshape(TOKENS, HEADS * q_width).astype(jnp.bfloat16)


def steps_of(own_key, extent, pieces, low, high):
    gain, own = 1.0, jax.random.fold_in(own_key, 6)
    for dim, parts in pieces:
        heights = jnp.exp(jax.random.uniform(jax.random.fold_in(own, dim), (parts,), jnp.float32, low / len(pieces), high / len(pieces)))
        gain = gain * jnp.repeat(heights, extent[dim] // parts).reshape([-1 if axis == dim else 1 for axis in range(len(extent))])
    return gain


def noise(stream_key, shape, deviation, limit, pieces=(), held_as=jnp.bfloat16):
    array = jax.random.normal(stream_key, shape, jnp.float32) * deviation
    if len(pieces) > 0:
        array = steps_of(stream_key, shape, pieces, -0.22, 0.18) * array
    return jnp.clip(array, min=-limit, max=limit).astype(held_as)


def setup_inputs(seed: int = 0) -> dict:
    key_of = jax.random.split(jax.random.key(seed), 12)
    return {
        "queries": draw_queries(jax.random.fold_in(key_of[11], 71), 0),
        "latents": noise(key_of[1], (TOKENS, RANK), 1.0, 6.0, ((0, 8),)),
        "shared_key": draw_shared_key(jax.random.fold_in(key_of[11], 71), 0),
        "expand_weight": noise(key_of[3], (RANK, HEADS * (NOPE_A + VAL_A + NOPE_B + VAL_B)), RANK ** -0.5, 0.25, ((1, 4),)),
        "residual": noise(key_of[4], (TOKENS, D), 0.5, 3.0, ((0, 8),)),
        "out_weight": noise(key_of[5], (HEADS * (VAL_A + VAL_B), D), (HEADS * (VAL_A + VAL_B)) ** -0.5, 0.21875),
        "norm_gain": jnp.clip(1.0 + 0.18 * jax.random.normal(key_of[6], (D,), jnp.float32), 0.099609375, 1.8984375).astype(jnp.bfloat16),
        "gate_weight": noise(key_of[7], (D, FF), D ** -0.5, 0.125, ((0, 8), (1, 4))),
        "value_weight": noise(key_of[8], (D, FF), D ** -0.5, 0.125, ((0, 8), (1, 4))),
        "conv_weight": noise(key_of[9], (CONV, FF), CONV ** -0.5, 3.5, ((1, 4),)),
        "down_weight": noise(key_of[10], (FF, D), FF ** -0.5, 0.109375, ((0, 4), (1, 8))),
    }


def tables(positions, width):
    half_width = width // 2
    frequency = 10000.0 ** (-jnp.arange(half_width, dtype=jnp.float32) / half_width)
    angles = positions.astype(jnp.float32)[:, None] * frequency[None, :]
    return (jnp.cos(angles), jnp.sin(angles))

def rotate(vectors, cos_table, sine_table):
    half_width = vectors.shape[-1] // 2
    first_half = vectors[:, :half_width].astype(jnp.float32)
    second_half = vectors[:, half_width:].astype(jnp.float32)
    turned = jnp.concatenate([first_half * cos_table - second_half * sine_table, second_half * cos_table + first_half * sine_table], axis=1)
    return turned.astype(jnp.bfloat16)

def attend_head(q_content, q_turned, k_content, k_turned, values, score_scale):
    tokens = q_content.shape[0]
    blocks = tokens // TOK_DEV

    def one_block(block_index):
        first_row = (block_index * TOK_DEV).astype(jnp.int32)
        content = lax.dynamic_slice_in_dim(q_content, first_row, TOK_DEV, 0)
        rotary = lax.dynamic_slice_in_dim(q_turned, first_row, TOK_DEV, 0)
        scores = (jnp.dot(content, k_content.T, preferred_element_type=jnp.float32) + jnp.dot(rotary, k_turned.T, preferred_element_type=jnp.float32)) * score_scale
        row_max = lax.optimization_barrier(jnp.max(scores, axis=1, keepdims=True))
        weights = jnp.exp(scores - row_max)
        row_sum = lax.optimization_barrier(jnp.sum(weights, axis=1, keepdims=True))
        weighted = jnp.dot(weights.astype(jnp.bfloat16), values, preferred_element_type=jnp.float32)
        return (weighted / row_sum).astype(jnp.bfloat16)
    result = lax.map(one_block, jnp.arange(blocks, dtype=jnp.int32))
    return result.reshape(tokens, values.shape[1])

def reference(queries, latents, shared_key, expand_weight, residual, out_weight, norm_gain, gate_weight, value_weight, conv_weight, down_weight):
    tokens = queries.shape[0]
    q_width = NOPE_A + NOPE_B + 2 * ROPE
    kv_width = NOPE_A + VAL_A + NOPE_B + VAL_B
    cos_table, sine_table = tables(jnp.arange(tokens, dtype=jnp.int32), ROPE)
    key_turned = rotate(shared_key, cos_table, sine_table)
    expanded = jnp.dot(latents, expand_weight, preferred_element_type=jnp.float32).astype(jnp.bfloat16)
    scale_wide = (NOPE_A + ROPE) ** (-0.5)
    scale_narrow = (NOPE_B + ROPE) ** (-0.5)
    outputs = []
    for pair_index in range(HEADS):
        q_base = pair_index * q_width
        kv_base = pair_index * kv_width
        wide_content = queries[:, q_base:q_base + NOPE_A]
        narrow_content = queries[:, q_base + NOPE_A:q_base + NOPE_A + NOPE_B]
        rotary_base = q_base + NOPE_A + NOPE_B
        wide_turned = rotate(queries[:, rotary_base:rotary_base + ROPE], cos_table, sine_table)
        narrow_turned = rotate(queries[:, rotary_base + ROPE:rotary_base + 2 * ROPE], cos_table, sine_table)
        wide_keys = expanded[:, kv_base:kv_base + NOPE_A]
        wide_values = expanded[:, kv_base + NOPE_A:kv_base + NOPE_A + VAL_A]
        narrow_base = kv_base + NOPE_A + VAL_A
        narrow_keys = expanded[:, narrow_base:narrow_base + NOPE_B]
        narrow_values = expanded[:, narrow_base + NOPE_B:narrow_base + NOPE_B + VAL_B]
        outputs.append(attend_head(wide_content, wide_turned, wide_keys, key_turned, wide_values, scale_wide))
        outputs.append(attend_head(narrow_content, narrow_turned, narrow_keys, key_turned, narrow_values, scale_narrow))
    attended = jnp.concatenate(outputs, axis=1)
    projected = jnp.dot(attended, out_weight, preferred_element_type=jnp.float32)
    stream = (residual.astype(jnp.float32) + projected).astype(jnp.bfloat16)
    stream_f = stream.astype(jnp.float32)
    scaled = stream_f * lax.rsqrt(lax.optimization_barrier(jnp.mean(stream_f * stream_f, axis=1, keepdims=True)) + 1e-06)
    normed = (scaled * norm_gain.astype(jnp.float32)).astype(jnp.bfloat16)
    gate_pre = jnp.dot(normed, gate_weight, preferred_element_type=jnp.float32).astype(jnp.bfloat16)
    value_pre = jnp.dot(normed, value_weight, preferred_element_type=jnp.float32).astype(jnp.bfloat16)
    reach = CONV // 2
    padded = jnp.pad(gate_pre, ((reach, reach), (0, 0)))
    mixed_gate = jnp.zeros(gate_pre.shape, jnp.float32)
    for tap in range(CONV):
        mixed_gate = mixed_gate + padded[tap:tap + tokens].astype(jnp.float32) * conv_weight[tap].astype(jnp.float32)
    active = (jax.nn.silu(mixed_gate) * value_pre.astype(jnp.float32)).astype(jnp.bfloat16)
    down = jnp.dot(active, down_weight, preferred_element_type=jnp.float32)
    return (stream.astype(jnp.float32) + down).astype(jnp.bfloat16)
```

```python
import functools
import math

import jax
import jax.numpy as jnp
from jax import lax
from jax.experimental import pallas as pl
from jax.experimental.pallas import tpu as pltpu
from jax.sharding import PartitionSpec as P

NOPE_A = 128
VAL_A = 128
NOPE_B = 64
VAL_B = 64
ROPE = 64


def padded_2(block, sides, width):
    for axis, dim in sides:
        count = lax.axis_size(axis)
        forward = [(i, i + 1) for i in range(count - 1)]
        backward = [(target, source) for source, target in forward]
        low = lax.ppermute(
            lax.slice_in_dim(block, block.shape[dim] - width, None, axis=dim), axis, forward
        )
        high = lax.ppermute(lax.slice_in_dim(block, 0, width, axis=dim), axis, backward)
        block = jnp.concatenate([low, block, high], axis=dim)
    return block


def tables(positions, width):
    half_width = width // 2
    frequency = 10000.0 ** (-jnp.arange(half_width, dtype=jnp.float32) / half_width)
    angles = positions.astype(jnp.float32)[:, None] * frequency[None, :]
    return (jnp.cos(angles), jnp.sin(angles))


def rotate(vectors, cos_table, sine_table):
    half_width = vectors.shape[-1] // 2
    first_half = vectors[:, :half_width].astype(jnp.float32)
    second_half = vectors[:, half_width:].astype(jnp.float32)
    turned = jnp.concatenate(
        [
            first_half * cos_table - second_half * sine_table,
            second_half * cos_table + first_half * sine_table,
        ],
        axis=1,
    )
    return turned.astype(jnp.bfloat16)


def normalize(stream, norm_gain):
    stream_f = stream.astype(jnp.float32)
    scaled = stream_f * lax.rsqrt(jnp.mean(stream_f * stream_f, axis=1, keepdims=True) + 1e-06)
    return (scaled * norm_gain.astype(jnp.float32)).astype(jnp.bfloat16)


def update(running, q_content, q_turned, k_content, k_turned, values, score_scale):
    row_max, row_sum, weighted = running
    scores = (
        jnp.einsum("qd,kd->qk", q_content, k_content, preferred_element_type=jnp.float32)
        + jnp.einsum("qd,kd->qk", q_turned, k_turned, preferred_element_type=jnp.float32)
    ) * score_scale
    new_max = jnp.maximum(row_max, jnp.max(scores, axis=1))
    weights = jnp.exp(scores - new_max[:, None])
    row_sum = jnp.sum(weights, axis=1)
    weighted = jnp.dot(weights.astype(jnp.bfloat16), values, preferred_element_type=jnp.float32)
    return (new_max, row_sum, weighted)


def body(
    queries,
    latents,
    shared_key,
    expand_weight,
    residual,
    out_weight,
    norm_gain,
    gate_weight,
    value_weight,
    conv_weight,
    down_weight,
):
    tok_rows = queries.shape[0]
    q_width = NOPE_A + NOPE_B + 2 * ROPE
    kv_width = NOPE_A + VAL_A + NOPE_B + VAL_B
    positions = lax.axis_index("sp") * tok_rows + jnp.arange(tok_rows, dtype=jnp.int32)
    cos_table, sine_table = tables(positions, ROPE)
    key_turned = rotate(shared_key, cos_table, sine_table)
    scale_wide = (NOPE_A + ROPE) ** (-0.5)
    scale_narrow = (NOPE_B + ROPE) ** (-0.5)
    initial = []
    pair_index = 0
    q_base = pair_index * q_width
    rotary_base = q_base + NOPE_A + NOPE_B
    wide_content = queries[:, q_base : q_base + NOPE_A]
    narrow_content = queries[:, q_base + NOPE_A : rotary_base]
    wide_turned = rotate(queries[:, rotary_base : rotary_base + ROPE], cos_table, sine_table)
    narrow_turned = rotate(
        queries[:, rotary_base + ROPE : rotary_base + 2 * ROPE], cos_table, sine_table
    )
    query_parts = [(wide_content, wide_turned, narrow_content, narrow_turned)]
    lowest = jnp.full((tok_rows,), -1e30, jnp.float32)
    empty_sum = jnp.zeros((tok_rows,), jnp.float32)
    initial += [
        lowest,
        empty_sum,
        jnp.zeros((tok_rows, VAL_A), jnp.float32),
        lowest,
        empty_sum,
        jnp.zeros((tok_rows, VAL_B), jnp.float32),
    ]
    initial = tuple(initial)
    pieces = (
        lax.all_gather(latents, "sp", axis=0, tiled=True),
        lax.all_gather(key_turned, "sp", axis=0, tiled=True),
    )
    expanded = jnp.dot(pieces[0], expand_weight, preferred_element_type=jnp.float32).astype(
        jnp.bfloat16
    )
    turned_keys = pieces[1]
    result = []
    pair_index = 0
    wide_content, wide_turned, narrow_content, narrow_turned = query_parts[pair_index]
    kv_base = pair_index * kv_width
    narrow_base = kv_base + NOPE_A + VAL_A
    wide_keys = expanded[:, kv_base : kv_base + NOPE_A]
    wide_values = expanded[:, kv_base + NOPE_A : narrow_base]
    narrow_keys = expanded[:, narrow_base : narrow_base + NOPE_B]
    narrow_values = expanded[:, narrow_base + NOPE_B : narrow_base + NOPE_B + VAL_B]
    absorb_offset = 6 * pair_index
    result += list(
        update(
            initial[absorb_offset : absorb_offset + 3],
            wide_content,
            wide_turned,
            wide_keys,
            turned_keys,
            wide_values,
            scale_wide,
        )
    )
    result += list(
        update(
            initial[absorb_offset + 3 : absorb_offset + 6],
            narrow_content,
            narrow_turned,
            narrow_keys,
            turned_keys,
            narrow_values,
            scale_narrow,
        )
    )
    running = tuple(result)
    outputs = []
    pair_index = 0
    for group_index in range(2):
        offset = 6 * pair_index + 3 * group_index
        outputs.append((running[offset + 2] / running[offset + 1][:, None]).astype(jnp.bfloat16))
    attended = jnp.concatenate(outputs, axis=1)
    share = tok_rows // lax.axis_size("tp")
    tp_index = lax.axis_index("tp")
    all_heads = lax.all_gather(attended, "tp", axis=1, tiled=True)
    projected = jnp.dot(all_heads, out_weight, preferred_element_type=jnp.float32)
    stream = (residual.astype(jnp.float32) + projected).astype(jnp.bfloat16)
    normed = normalize(stream, norm_gain)
    stream_own = lax.dynamic_slice_in_dim(stream, tp_index * share, share, 0)
    pieces = (
        lax.all_gather(gate_weight, "sp", axis=0, tiled=True),
        lax.all_gather(value_weight, "sp", axis=0, tiled=True),
    )
    gate_sum = jnp.dot(normed, pieces[0], preferred_element_type=jnp.float32)
    value_sum = jnp.dot(normed, pieces[1], preferred_element_type=jnp.float32)
    gate_pre = gate_sum.astype(jnp.bfloat16)
    value_pre = value_sum.astype(jnp.bfloat16)
    reach = conv_weight.shape[0] // 2
    padded = padded_2(gate_pre, (("sp", 0),), reach)
    mixed_gate = jnp.zeros(gate_pre.shape, jnp.float32)
    for tap in range(conv_weight.shape[0]):
        mixed_gate = mixed_gate + padded[tap : tap + tok_rows].astype(jnp.float32) * conv_weight[
            tap
        ].astype(jnp.float32)
    active = (jax.nn.silu(mixed_gate) * value_pre.astype(jnp.float32)).astype(jnp.bfloat16)
    partial_rows = jnp.dot(
        active,
        lax.all_gather(down_weight, "sp", axis=1, tiled=True),
        preferred_element_type=jnp.float32,
    )
    summed = lax.psum_scatter(
        partial_rows.astype(jnp.bfloat16), "tp", scatter_dimension=0, tiled=True
    ).astype(jnp.float32)
    return (stream_own.astype(jnp.float32) + summed).astype(jnp.bfloat16)


MESH = pl.DeviceIdType.MESH
KINDS = (
    "lz", "ly", "lx", "lxy", "lcz", "lcx", "lcy", "lcxy",
    "wz", "wy", "dz", "dy", "nz", "nx", "ncz", "ncx", "at", "pc", "px", "pz", "h",
)
SENDS = 96


def layer_kernel(
    zn,
    q_hbm,
    lat_hbm,
    key_hbm,
    conv_hbm,
    gain_hbm,
    expand_hbm,
    res_hbm,
    out_w_hbm,
    gate_hbm,
    value_hbm,
    down_hbm,
    out_ref,
    q_ref,
    lat_ref,
    key_ref,
    conv_ref,
    gain_ref,
    expand_ref,
    res_ref,
    out_w_ref,
    gate_ref,
    value_ref,
    down_ref,
    lat_all,
    att_send,
    att_recv,
    own_stream,
    nrm,
    stage,
    w_full,
    dn_full,
    hbuf,
    abuf,
    halo_send,
    halo_recv,
    part,
    c_send,
    c_recv,
    keep,
    x_send,
    x_recv,
    z_send,
    z_recv,
    in_s,
    send_s,
    recv_s,
):
    f32, bf16 = jnp.float32, jnp.bfloat16
    s, t = lax.axis_index("sp"), lax.axis_index("tp")
    z, y = s // 2, s % 2
    x, c = t // 2, t % 2
    yo, xo, co = 1 - y, 1 - x, 1 - c
    xt, ct, xct = 2 * xo + c, 2 * x + co, 2 * xo + co
    rows = lat_ref.shape[0]
    share = rows // 4
    packed = share // 2
    rank = lat_ref.shape[1]
    sub = down_ref.shape[0] // zn
    sp = 2 * zn

    inner = ((z + 1) // 2) % 2
    near = z + 1 - 2 * (z % 2)
    mid = (z + 2) % zn + inner * (zn - 1 - z - (z + 2) % zn)
    far = zn - 1 - z + inner * ((z + 2) % zn - (zn - 1 - z))
    arrivals = (near + inner * (mid - near), mid + inner * (far - mid), far + inner * (near - far))

    def to_z(zz):
        return {"sp": 2 * zz + y, "tp": t}

    y_dev = {"sp": 2 * z + yo, "tp": t}
    x_dev = {"sp": s, "tp": xt}
    c_dev = {"sp": s, "tp": ct}
    xc_dev = {"sp": s, "tp": xct}

    started = []
    used = [0]

    def copy_to(src, dst, dev, kind, i, slot):
        return pltpu.make_async_remote_copy(
            src_ref=src, dst_ref=dst, send_sem=send_s.at[slot],
            recv_sem=recv_s.at[KINDS.index(kind) * zn + i], device_id=dev, device_id_type=MESH,
        )

    def new_slot():
        used[0] += 1
        return used[0] - 1

    def send(ref, dev, kind, i, dst=None):
        copy = copy_to(ref, ref if dst is None else dst, dev, kind, i, new_slot())
        copy.start()
        started.append(copy)

    def arrived(dst, kind, i):
        with jax.named_scope("wait_" + kind):
            copy_to(dst, dst, c_dev, kind, i, 0).wait_recv()

    barrier = pltpu.get_barrier_semaphore()
    partners = [to_z(near), to_z(mid), to_z(far), y_dev, x_dev, c_dev, xc_dev]
    for dev in partners:
        pl.semaphore_signal(barrier, inc=1, device_id=dev, device_id_type=MESH)

    def res_rows(i):
        return res_hbm.at[pl.ds(pl.multiple_of((2 * i + c) * share, share), share), :]

    pairs = [
        (key_hbm, key_ref),
        (lat_hbm, lat_ref),
        (gate_hbm, gate_ref),
        (value_hbm, value_ref),
        (q_hbm, q_ref),
        (down_hbm, down_ref),
        (expand_hbm, expand_ref),
        (res_rows(0), res_ref.at[0]),
        (res_rows(1), res_ref.at[1]),
        (gain_hbm, gain_ref),
        (conv_hbm, conv_ref),
        (out_w_hbm, out_w_ref),
    ]
    loads = [pltpu.make_async_copy(src, dst, in_s.at[i]) for i, (src, dst) in enumerate(pairs)]
    for load in loads:
        load.start()

    h = ROPE // 2
    step = lax.broadcasted_iota(jnp.int32, (h, rows), 0).astype(f32) * (-math.log(10000.0) / h)
    spot = (s * rows + lax.broadcasted_iota(jnp.int32, (h, rows), 1)).astype(f32)
    angles = spot * jnp.exp(step)
    cos, sine = jnp.cos(angles), jnp.sin(angles)

    def turn(v):
        a, b = v[:h], v[h:]
        return jnp.concatenate([a * cos - b * sine, b * cos + a * sine], axis=0)

    loads[0].wait()
    turned = turn(key_ref[...].astype(f32))
    key_turned = jnp.concatenate([turned, jnp.zeros_like(turned)], axis=0).T.astype(bf16)[:, :ROPE]
    loads[1].wait()
    for i in range(4):
        for j in range(2):
            first = i * share + j * packed
            lat_all[s, i, :, j * rank : (j + 1) * rank] = lat_ref[first : first + packed, :]
        lat_all[s, i, :, 2 * rank :] = jnp.concatenate(
            [key_turned[i * share : i * share + packed], key_turned[i * share + packed : (i + 1) * share]], axis=1
        )
    loads[2].wait()
    loads[3].wait()
    for k in range(zn):
        stage[k, :, :sub] = gate_ref[:, k * sub : (k + 1) * sub]
        stage[k, :, sub:] = value_ref[:, k * sub : (k + 1) * sub]
    with jax.named_scope("barrier"):
        pl.semaphore_wait(barrier, len(partners))

    def lat(zz, yy, q):
        return lat_all.at[2 * zz + yy, q]

    for zz in (far, mid, near):
        send(lat(z, y, t), to_z(zz), "lz", z)
    send(lat(z, y, t), y_dev, "ly", z)
    send(lat(z, y, xt), y_dev, "lxy", z)
    for zz in (far, mid, near):
        send(stage.at[zz], to_z(zz), "wz", z, w_full.at[s])
    w_full[s] = stage[z]

    for zz in arrivals:
        arrived(lat(zz, y, t), "lz", zz)
        send(lat(zz, y, t), y_dev, "ly", zz)
        send(lat(zz, y, t), x_dev, "lx", zz)
        send(lat(zz, y, t), c_dev, "lcz", zz)
    send(w_full.at[s], y_dev, "wy", z)
    arrived(lat(z, yo, t), "ly", z)
    send(lat(z, yo, t), c_dev, "lcy", z)
    arrived(lat(z, yo, xt), "lxy", z)
    send(lat(z, yo, xt), c_dev, "lcxy", z)
    for i, zz in enumerate(arrivals):
        arrived(lat(zz, yo, t), "ly", zz)
        if i < 2:
            send(lat(zz, yo, t), x_dev, "lxy", zz)
        send(lat(zz, yo, t), c_dev, "lcy", zz)
        arrived(lat(zz, y, xt), "lx", zz)
        if i == 2:
            send(lat(zz, y, xt), y_dev, "lxy", zz)
        send(lat(zz, y, xt), c_dev, "lcx", zz)

    loads[4].wait()
    rot = NOPE_A + NOPE_B
    q = q_ref[...].astype(f32)
    q_wide = q[:NOPE_A].T.astype(bf16)
    pair = jnp.concatenate([q[NOPE_A:rot], turn(q[rot : rot + ROPE])], axis=0).T.astype(bf16)
    q_narrow, q_wide_t = pair[:, :NOPE_B], pair[:, NOPE_B:]
    turned = turn(q[rot + ROPE :])
    q_narrow_t = jnp.concatenate([turned, jnp.zeros_like(turned)], axis=0).T.astype(bf16)[:, :ROPE]
    loads[5].wait()
    dn_full[s] = down_ref[pl.ds(pl.multiple_of(z * sub, sub), sub), :]
    loads[6].wait()

    for zz in arrivals:
        arrived(lat(zz, yo, xt), "lxy", zz)
        send(lat(zz, yo, xt), c_dev, "lcxy", zz)
    for zz in arrivals:
        arrived(lat(zz, y, ct), "lcz", zz)
        arrived(lat(zz, y, xct), "lcx", zz)
    for zz in (z,) + arrivals:
        arrived(lat(zz, yo, ct), "lcy", zz)
        arrived(lat(zz, yo, xct), "lcxy", zz)

    whole = lat_all[...].reshape(sp * 4 * packed, lat_all.shape[3])
    expand_w = expand_ref[...]
    expanded = jnp.concatenate(
        [
            jnp.dot(whole[:, j * rank : (j + 1) * rank], expand_w, preferred_element_type=f32).astype(bf16)
            for j in range(2)
        ],
        axis=0,
    )
    keys_t = whole[:, 2 * rank :]
    empty = jnp.zeros((rows, ROPE), bf16)

    def attend(qc, qt, kc, v, scale):
        dims = (((1,), (1,)), ((), ()))
        turned_scores = [
            lax.dot_general(jnp.concatenate(two, axis=1), keys_t, dims, preferred_element_type=f32)
            for two in ([qt, empty], [empty, qt])
        ]
        scores = (
            lax.dot_general(qc, kc, dims, preferred_element_type=f32) + jnp.concatenate(turned_scores, axis=1)
        ) * scale
        w = jnp.exp(scores - jnp.max(scores, axis=1, keepdims=True))
        total = jnp.sum(w, axis=1, keepdims=True)
        return (jnp.dot(w.astype(bf16), v, preferred_element_type=f32) / total).astype(bf16)

    nb = NOPE_A + VAL_A
    wide = attend(q_wide, q_wide_t, expanded[:, :NOPE_A], expanded[:, NOPE_A:nb], (NOPE_A + ROPE) ** -0.5)
    narrow = attend(
        q_narrow, q_narrow_t, expanded[:, nb : nb + NOPE_B],
        expanded[:, nb + NOPE_B : nb + NOPE_B + VAL_B], (NOPE_B + ROPE) ** -0.5,
    )
    vals = VAL_A + VAL_B
    for i in range(4):
        att_send[i % 2, i // 2, :, :VAL_A] = wide[i * share : (i + 1) * share, :]
        att_send[i % 2, i // 2, :, VAL_A:vals] = narrow[i * share : (i + 1) * share, :]
    send(att_send.at[c], x_dev, "at", t, att_recv.at[t])
    send(att_send.at[co], xc_dev, "at", t, att_recv.at[t])
    send(att_send.at[co], c_dev, "at", t, att_recv.at[t])
    att_recv[t] = att_send[c]

    def forward_weights(zz):
        arrived(w_full.at[2 * zz + y], "wz", zz)
        send(w_full.at[2 * zz + y], y_dev, "wy", zz)

    for load in loads[7:]:
        load.wait()
    forward_weights(arrivals[0])
    for o in (ct, xt, xct):
        arrived(att_recv.at[o], "at", o)

    projected = None
    for i in range(4):
        term = jnp.dot(
            att_recv[i].reshape(2 * share, att_recv.shape[3])[:, :vals],
            out_w_ref[i * vals : (i + 1) * vals, :], preferred_element_type=f32,
        )
        projected = term if projected is None else projected + term
    stream = (res_ref[...].reshape(2 * share, res_ref.shape[2]).astype(f32) + projected).astype(bf16)
    stream_f = stream.astype(f32)
    scaled = stream_f * lax.rsqrt(jnp.mean(stream_f * stream_f, axis=1, keepdims=True) + 1e-06)
    normed = (scaled * gain_ref[...].astype(f32)).astype(bf16)
    for i in range(2):
        nrm[z, 2 * i + c] = normed[i * share : (i + 1) * share]
        own_stream[i] = stream[i * share : (i + 1) * share]

    own = nrm.at[z, t]
    send(own, to_z(mid), "nz", z)
    send(own, to_z(near), "nz", z)
    send(own, c_dev, "ncz", z)
    send(nrm.at[z, xt], c_dev, "ncx", z)

    def send_down(zz):
        piece = down_ref.at[pl.ds(pl.multiple_of(zz * sub, sub), sub), :]
        send(piece, to_z(zz), "dz", z, dn_full.at[s])

    send_down(far)
    send_down(mid)
    forward_weights(arrivals[1])
    passed = []
    for i, zz in enumerate(arrivals):
        blk = nrm.at[zz, t]
        arrived(blk, "nz", zz)
        if i < 2:
            on = copy_to(blk, blk, to_z(near), "nz", zz, new_slot())
            passed.append(on)

            @pl.when(inner == 1)
            def _():
                on.start()

        send(blk, x_dev, "nx", zz)
        send(blk, c_dev, "ncz", zz)
        if i == 0:
            forward_weights(arrivals[2])
    send_down(near)
    send(dn_full.at[s], y_dev, "dy", z)
    for zz in (z,) + arrivals:
        arrived(w_full.at[2 * zz + yo], "wy", zz)
    weights = w_full[...].reshape(sp * w_full.shape[1], 2 * sub)
    for i, zz in enumerate((z,) + arrivals):
        if i > 0:
            blk = nrm.at[zz, xt]
            arrived(blk, "nx", zz)
            send(blk, c_dev, "ncx", zz)
        arrived(nrm.at[zz, ct], "ncz", zz)
        arrived(nrm.at[zz, xct], "ncx", zz)
        block = nrm[zz].reshape(rows, nrm.shape[3])
        hbuf[zz] = jnp.dot(block, weights, preferred_element_type=f32).astype(bf16)

    wide_lanes = halo_send.shape[1]
    for k in range(zn):
        g = hbuf[k, :, :wide_lanes].astype(f32)
        halo_send[k : k + 1, :] = g[rows - 1 : rows, :]
        halo_send[zn + k : zn + k + 1, :] = g[0:1, :]
    send(halo_send, y_dev, "h", 0, halo_recv)

    def forward_down(zz):
        arrived(dn_full.at[2 * zz + y], "dz", zz)
        send(dn_full.at[2 * zz + y], y_dev, "dy", zz)

    for zz in arrivals:
        forward_down(zz)
    conv_all = conv_ref[...].astype(f32)
    pieces = [conv_all[:, k * sub : (k + 1) * sub] for k in range(zn)]
    taps = pieces[0]
    for k in range(1, zn):
        taps = jnp.where(z == k, pieces[k], taps)
    taps = jnp.concatenate([taps, jnp.zeros((taps.shape[0], wide_lanes - sub), f32)], axis=1)
    row_id = lax.broadcasted_iota(jnp.int32, (rows, wide_lanes), 0)
    arrived(halo_recv, "h", 0)
    nothing = jnp.zeros((1, wide_lanes), f32)
    for k in range(zn):
        before_low = halo_recv[k - 1 : k, :] if k > 0 else nothing
        before = jnp.where(y == 0, before_low, halo_recv[k : k + 1, :])
        after_high = halo_recv[zn + k + 1 : zn + k + 2, :] if k < zn - 1 else nothing
        after = jnp.where(y == 0, halo_recv[zn + k : zn + k + 1, :], after_high)
        g = hbuf[k, :, :wide_lanes].astype(f32)
        up = jnp.where(row_id == 0, before, pltpu.roll(g, 1, 0))
        down = jnp.where(row_id == rows - 1, after, pltpu.roll(g, rows - 1, 0))
        mixed = up * taps[0:1] + g * taps[1:2] + down * taps[2:3]
        mixed = mixed[:, :sub]
        v = hbuf[k].astype(f32)[:, sub:]
        abuf[k] = (mixed / (1.0 + jnp.exp(-mixed)) * v).astype(bf16)

    for zz in (z,) + arrivals:
        arrived(dn_full.at[2 * zz + yo], "dy", zz)
    order = (far, mid, near, z)
    depth = dn_full.shape[2]
    for d, zz in enumerate(order):
        a = abuf[zz]
        for k in range(sp):
            p = jnp.dot(a, dn_full[k], preferred_element_type=f32)
            part[d, :, :, k * depth : (k + 1) * depth] = p.reshape(4, share, depth)
        for i in range(2):
            c_send[d, i] = part[d, 2 * i + co].astype(bf16)
        send(c_send.at[d], c_dev, "pc", d, c_recv.at[d])
    for d, zz in enumerate(order):
        arrived(c_recv.at[d], "pc", d)
        x_send[d] = (part[d, xt] + c_recv[d, xo].astype(f32)).astype(bf16)
        send(x_send.at[d], x_dev, "px", d, x_recv.at[d])
        keep[d] = part[d, t] + c_recv[d, x].astype(f32)
    total = own_stream[x].astype(f32)
    for d, zz in enumerate(order):
        arrived(x_recv.at[d], "px", d)
        if d < zn - 1:
            z_send[d] = (keep[d] + x_recv[d].astype(f32)).astype(bf16)
            send(z_send.at[d], to_z(zz), "pz", z, z_recv.at[z])
        else:
            total += keep[d] + x_recv[d].astype(f32)
    for zz in arrivals:
        arrived(z_recv.at[zz], "pz", zz)
        total += z_recv[zz].astype(f32)
    out_ref[...] = total.astype(bf16)
    for copy in started:
        copy.wait_send()

    @pl.when(inner == 1)
    def _():
        for on in passed:
            on.wait_send()


def kernel_body(zn, *args):
    (queries, latents, shared_key, expand_weight, residual, out_weight, norm_gain,
     gate_weight, value_weight, conv_weight, down_weight) = args
    rows, width = residual.shape
    sub = down_weight.shape[0] // zn
    share = rows // 4
    d_own = gate_weight.shape[0]
    bf16, f32 = jnp.bfloat16, jnp.float32
    vals = VAL_A + VAL_B
    lanes = -(-vals // 128) * 128
    halo_lanes = -(-sub // 128) * 128
    V, DMA = pltpu.VMEM, pltpu.SemaphoreType.DMA
    return pl.pallas_call(
        functools.partial(layer_kernel, zn),
        out_shape=jax.ShapeDtypeStruct((share, width), bf16),
        in_specs=[pl.BlockSpec(memory_space=pl.ANY)] * 11,
        out_specs=pl.BlockSpec(memory_space=V),
        scratch_shapes=[
            V((queries.shape[1], rows), bf16),
            V(latents.shape, bf16),
            V((ROPE, rows), bf16),
            V(conv_weight.shape, bf16),
            V((1, width), bf16),
            V(expand_weight.shape, bf16),
            V((2, share, width), bf16),
            V(out_weight.shape, bf16),
            V(gate_weight.shape, bf16),
            V(value_weight.shape, bf16),
            V(down_weight.shape, bf16),
            V((2 * zn, 4, share // 2, 2 * latents.shape[1] + 2 * ROPE), bf16),
            V((2, 2, share, lanes), bf16),
            V((4, 2, share, lanes), bf16),
            V((2, share, width), bf16),
            V((zn, 4, share, width), bf16),
            V((zn, d_own, 2 * sub), bf16),
            V((2 * zn, d_own, 2 * sub), bf16),
            V((2 * zn, sub, down_weight.shape[1]), bf16),
            V((zn, rows, 2 * sub), bf16),
            V((zn, rows, sub), bf16),
            V((2 * zn, halo_lanes), f32),
            V((2 * zn, halo_lanes), f32),
            V((zn, 4, share, width), f32),
            V((zn, 2, share, width), bf16),
            V((zn, 2, share, width), bf16),
            V((zn, share, width), f32),
            V((zn, share, width), bf16),
            V((zn, share, width), bf16),
            V((zn, share, width), bf16),
            V((zn, share, width), bf16),
            DMA((12,)),
            DMA((SENDS,)),
            DMA((len(KINDS) * zn,)),
        ],
        compiler_params=pltpu.CompilerParams(collective_id=0, has_side_effects=True),
    )(queries.T, latents, shared_key.T, conv_weight, norm_gain.reshape(1, width), expand_weight, residual,
      out_weight, gate_weight, value_weight, down_weight)


def pick(*args):
    zn = lax.axis_size("sp") // 2
    hidden = args[10].shape[0]
    sub = hidden // zn
    fits = (
        lax.axis_size("sp") == 8
        and lax.axis_size("tp") == 4
        and hidden % zn == 0
        and sub % 64 == 0
        and args[7].shape[0] % 128 == 0
        and args[0].shape[0] % 128 == 0
        and args[4].shape[1] % args[0].shape[0] == 0
        and args[9].shape[0] == 3
    )
    return kernel_body(zn, *args) if fits else body(*args)


def solution(mesh):
    in_specs = (
        P("sp", "tp"),
        P("sp", None),
        P("sp", None),
        P(None, "tp"),
        P("sp", None),
        P(),
        P(),
        P("sp", "tp"),
        P("sp", "tp"),
        P(None, "tp"),
        P("tp", "sp"),
    )
    out_specs = P(("sp", "tp"), None)
    return jax.shard_map(pick, mesh=mesh, in_specs=in_specs, out_specs=out_specs, check_vma=False)
```

```python
import functools
import math

import jax
import jax.numpy as jnp
from jax import lax
from jax.experimental import pallas as pl
from jax.experimental.pallas import tpu as pltpu
from jax.sharding import PartitionSpec as P

NOPE_A = 128
VAL_A = 128
NOPE_B = 64
VAL_B = 64
ROPE = 64


def padded_2(block, sides, width):
    for axis, dim in sides:
        count = lax.axis_size(axis)
        forward = [(i, i + 1) for i in range(count - 1)]
        backward = [(target, source) for source, target in forward]
        low = lax.ppermute(
            lax.slice_in_dim(block, block.shape[dim] - width, None, axis=dim), axis, forward
        )
        high = lax.ppermute(lax.slice_in_dim(block, 0, width, axis=dim), axis, backward)
        block = jnp.concatenate([low, block, high], axis=dim)
    return block


def tables(positions, width):
    half_width = width // 2
    frequency = 10000.0 ** (-jnp.arange(half_width, dtype=jnp.float32) / half_width)
    angles = positions.astype(jnp.float32)[:, None] * frequency[None, :]
    return (jnp.cos(angles), jnp.sin(angles))


def rotate(vectors, cos_table, sine_table):
    half_width = vectors.shape[-1] // 2
    first_half = vectors[:, :half_width].astype(jnp.float32)
    second_half = vectors[:, half_width:].astype(jnp.float32)
    turned = jnp.concatenate(
        [
            first_half * cos_table - second_half * sine_table,
            second_half * cos_table + first_half * sine_table,
        ],
        axis=1,
    )
    return turned.astype(jnp.bfloat16)


def normalize(stream, norm_gain):
    stream_f = stream.astype(jnp.float32)
    scaled = stream_f * lax.rsqrt(jnp.mean(stream_f * stream_f, axis=1, keepdims=True) + 1e-06)
    return (scaled * norm_gain.astype(jnp.float32)).astype(jnp.bfloat16)


def update(running, q_content, q_turned, k_content, k_turned, values, score_scale):
    row_max, row_sum, weighted = running
    scores = (
        jnp.einsum("qd,kd->qk", q_content, k_content, preferred_element_type=jnp.float32)
        + jnp.einsum("qd,kd->qk", q_turned, k_turned, preferred_element_type=jnp.float32)
    ) * score_scale
    new_max = jnp.maximum(row_max, jnp.max(scores, axis=1))
    weights = jnp.exp(scores - new_max[:, None])
    row_sum = jnp.sum(weights, axis=1)
    weighted = jnp.dot(weights.astype(jnp.bfloat16), values, preferred_element_type=jnp.float32)
    return (new_max, row_sum, weighted)


def body(
    queries,
    latents,
    shared_key,
    expand_weight,
    residual,
    out_weight,
    norm_gain,
    gate_weight,
    value_weight,
    conv_weight,
    down_weight,
):
    tok_rows = queries.shape[0]
    q_width = NOPE_A + NOPE_B + 2 * ROPE
    kv_width = NOPE_A + VAL_A + NOPE_B + VAL_B
    positions = lax.axis_index("sp") * tok_rows + jnp.arange(tok_rows, dtype=jnp.int32)
    cos_table, sine_table = tables(positions, ROPE)
    key_turned = rotate(shared_key, cos_table, sine_table)
    scale_wide = (NOPE_A + ROPE) ** (-0.5)
    scale_narrow = (NOPE_B + ROPE) ** (-0.5)
    initial = []
    pair_index = 0
    q_base = pair_index * q_width
    rotary_base = q_base + NOPE_A + NOPE_B
    wide_content = queries[:, q_base : q_base + NOPE_A]
    narrow_content = queries[:, q_base + NOPE_A : rotary_base]
    wide_turned = rotate(queries[:, rotary_base : rotary_base + ROPE], cos_table, sine_table)
    narrow_turned = rotate(
        queries[:, rotary_base + ROPE : rotary_base + 2 * ROPE], cos_table, sine_table
    )
    query_parts = [(wide_content, wide_turned, narrow_content, narrow_turned)]
    lowest = jnp.full((tok_rows,), -1e30, jnp.float32)
    empty_sum = jnp.zeros((tok_rows,), jnp.float32)
    initial += [
        lowest,
        empty_sum,
        jnp.zeros((tok_rows, VAL_A), jnp.float32),
        lowest,
        empty_sum,
        jnp.zeros((tok_rows, VAL_B), jnp.float32),
    ]
    initial = tuple(initial)
    pieces = (
        lax.all_gather(latents, "sp", axis=0, tiled=True),
        lax.all_gather(key_turned, "sp", axis=0, tiled=True),
    )
    expanded = jnp.dot(pieces[0], expand_weight, preferred_element_type=jnp.float32).astype(
        jnp.bfloat16
    )
    turned_keys = pieces[1]
    result = []
    pair_index = 0
    wide_content, wide_turned, narrow_content, narrow_turned = query_parts[pair_index]
    kv_base = pair_index * kv_width
    narrow_base = kv_base + NOPE_A + VAL_A
    wide_keys = expanded[:, kv_base : kv_base + NOPE_A]
    wide_values = expanded[:, kv_base + NOPE_A : narrow_base]
    narrow_keys = expanded[:, narrow_base : narrow_base + NOPE_B]
    narrow_values = expanded[:, narrow_base + NOPE_B : narrow_base + NOPE_B + VAL_B]
    absorb_offset = 6 * pair_index
    result += list(
        update(
            initial[absorb_offset : absorb_offset + 3],
            wide_content,
            wide_turned,
            wide_keys,
            turned_keys,
            wide_values,
            scale_wide,
        )
    )
    result += list(
        update(
            initial[absorb_offset + 3 : absorb_offset + 6],
            narrow_content,
            narrow_turned,
            narrow_keys,
            turned_keys,
            narrow_values,
            scale_narrow,
        )
    )
    running = tuple(result)
    outputs = []
    pair_index = 0
    for group_index in range(2):
        offset = 6 * pair_index + 3 * group_index
        outputs.append((running[offset + 2] / running[offset + 1][:, None]).astype(jnp.bfloat16))
    attended = jnp.concatenate(outputs, axis=1)
    share = tok_rows // lax.axis_size("tp")
    tp_index = lax.axis_index("tp")
    all_heads = lax.all_gather(attended, "tp", axis=1, tiled=True)
    projected = jnp.dot(all_heads, out_weight, preferred_element_type=jnp.float32)
    stream = (residual.astype(jnp.float32) + projected).astype(jnp.bfloat16)
    normed = normalize(stream, norm_gain)
    stream_own = lax.dynamic_slice_in_dim(stream, tp_index * share, share, 0)
    pieces = (
        lax.all_gather(gate_weight, "sp", axis=0, tiled=True),
        lax.all_gather(value_weight, "sp", axis=0, tiled=True),
    )
    gate_sum = jnp.dot(normed, pieces[0], preferred_element_type=jnp.float32)
    value_sum = jnp.dot(normed, pieces[1], preferred_element_type=jnp.float32)
    gate_pre = gate_sum.astype(jnp.bfloat16)
    value_pre = value_sum.astype(jnp.bfloat16)
    reach = conv_weight.shape[0] // 2
    padded = padded_2(gate_pre, (("sp", 0),), reach)
    mixed_gate = jnp.zeros(gate_pre.shape, jnp.float32)
    for tap in range(conv_weight.shape[0]):
        mixed_gate = mixed_gate + padded[tap : tap + tok_rows].astype(jnp.float32) * conv_weight[
            tap
        ].astype(jnp.float32)
    active = (jax.nn.silu(mixed_gate) * value_pre.astype(jnp.float32)).astype(jnp.bfloat16)
    partial_rows = jnp.dot(
        active,
        lax.all_gather(down_weight, "sp", axis=1, tiled=True),
        preferred_element_type=jnp.float32,
    )
    summed = lax.psum_scatter(
        partial_rows.astype(jnp.bfloat16), "tp", scatter_dimension=0, tiled=True
    ).astype(jnp.float32)
    return (stream_own.astype(jnp.float32) + summed).astype(jnp.bfloat16)


MESH = pl.DeviceIdType.MESH
KINDS = (
    "lz", "ly", "lx", "lxy", "lcz", "lcx", "lcy", "lcxy",
    "wz", "", "wy", "", "dz", "dy", "nz", "", "nx", "", "ncz", "", "ncx", "",
    "at", "pc", "h", "px", "", "", "", "pz", "", "", "",
)
SENDS = 144


def layer_kernel(
    zn,
    q_hbm,
    lat_hbm,
    key_hbm,
    conv_hbm,
    gain_hbm,
    expand_hbm,
    res_hbm,
    out_w_hbm,
    gate_hbm,
    value_hbm,
    down_hbm,
    out_ref,
    q_ref,
    lat_ref,
    key_ref,
    conv_ref,
    gain_ref,
    expand_ref,
    res_ref,
    out_w_ref,
    gate_ref,
    value_ref,
    down_ref,
    lat_all,
    att_send,
    att_recv,
    own_stream,
    nrm,
    stage,
    w_full,
    dn_full,
    hbuf,
    abuf,
    halo_send,
    halo_recv,
    part,
    c_send,
    c_recv,
    keep,
    x_send,
    x_recv,
    z_send,
    z_recv,
    result,
    in_s,
    send_s,
    recv_s,
):
    f32, bf16 = jnp.float32, jnp.bfloat16
    s, t = lax.axis_index("sp"), lax.axis_index("tp")
    z, y = s // 2, s % 2
    x, c = t // 2, t % 2
    yo, xo, co = 1 - y, 1 - x, 1 - c
    xt, ct, xct = 2 * xo + c, 2 * x + co, 2 * xo + co
    rows = lat_ref.shape[0]
    share = rows // 4
    packed = share // 2
    rank = lat_ref.shape[1]
    sub = down_ref.shape[0] // zn
    sp = 2 * zn
    deep = gate_ref.shape[0] // 2

    inner = ((z + 1) // 2) % 2
    near = z + 1 - 2 * (z % 2)
    mid = (z + 2) % zn + inner * (zn - 1 - z - (z + 2) % zn)
    far = zn - 1 - z + inner * ((z + 2) % zn - (zn - 1 - z))
    arrivals = (near + inner * (mid - near), mid + inner * (far - mid), far + inner * (near - far))

    def to_z(zz):
        return {"sp": 2 * zz + y, "tp": t}

    y_dev = {"sp": 2 * z + yo, "tp": t}
    x_dev = {"sp": s, "tp": xt}
    c_dev = {"sp": s, "tp": ct}
    xc_dev = {"sp": s, "tp": xct}

    started = []
    used = [0]

    def copy_to(src, dst, dev, kind, i, slot):
        return pltpu.make_async_remote_copy(
            src_ref=src, dst_ref=dst, send_sem=send_s.at[slot],
            recv_sem=recv_s.at[KINDS.index(kind) * zn + i], device_id=dev, device_id_type=MESH,
        )

    def new_slot():
        used[0] += 1
        return used[0] - 1

    def send(ref, dev, kind, i, dst=None):
        copy = copy_to(ref, ref if dst is None else dst, dev, kind, i, new_slot())
        copy.start()
        started.append(copy)

    def send_in(*turns):
        slot = new_slot()

        def start(which, ref, dev, kind, i, dst=None, wait=None):
            @pl.when(turns[which])
            def _():
                if wait is not None:
                    arrived(ref, wait, i)
                copy_to(ref, ref if dst is None else dst, dev, kind, i, slot).start()

            if which == 0:
                started.append(copy_to(ref, ref if dst is None else dst, dev, kind, i, slot))

        return start

    def arrived(dst, kind, i):
        with jax.named_scope("wait_" + kind):
            copy_to(dst, dst, c_dev, kind, i, 0).wait_recv()

    barrier = pltpu.get_barrier_semaphore()
    partners = [to_z(near), to_z(mid), to_z(far), y_dev, x_dev, c_dev, xc_dev]
    for dev in partners:
        pl.semaphore_signal(barrier, inc=1, device_id=dev, device_id_type=MESH)

    def res_rows(i):
        return res_hbm.at[pl.ds(pl.multiple_of((2 * i + c) * share, share), share), :]

    pairs = [
        (key_hbm, key_ref),
        (lat_hbm, lat_ref),
        (gate_hbm, gate_ref),
        (value_hbm, value_ref),
        (q_hbm, q_ref),
        (down_hbm, down_ref),
        (expand_hbm, expand_ref),
        (res_rows(0), res_ref.at[0]),
        (res_rows(1), res_ref.at[1]),
        (gain_hbm, gain_ref),
        (conv_hbm, conv_ref),
        (out_w_hbm, out_w_ref),
    ]
    loads = [pltpu.make_async_copy(src, dst, in_s.at[i]) for i, (src, dst) in enumerate(pairs)]
    for load in loads:
        load.start()

    h = ROPE // 2
    step = lax.broadcasted_iota(jnp.int32, (h, rows), 0).astype(f32) * (-math.log(10000.0) / h)
    spot = (s * rows + lax.broadcasted_iota(jnp.int32, (h, rows), 1)).astype(f32)
    angles = spot * jnp.exp(step)
    cos, sine = jnp.cos(angles), jnp.sin(angles)

    def turn(v):
        a, b = v[:h], v[h:]
        return jnp.concatenate([a * cos - b * sine, b * cos + a * sine], axis=0)

    loads[0].wait()
    turned = turn(key_ref[...].astype(f32))
    key_turned = jnp.concatenate([turned, jnp.zeros_like(turned)], axis=0).T.astype(bf16)[:, :ROPE]
    loads[1].wait()
    for i in range(4):
        for j in range(2):
            first = i * share + j * packed
            lat_all[s, i, :, j * rank : (j + 1) * rank] = lat_ref[first : first + packed, :]
        lat_all[s, i, :, 2 * rank :] = jnp.concatenate(
            [key_turned[i * share : i * share + packed], key_turned[i * share + packed : (i + 1) * share]], axis=1
        )
    loads[2].wait()
    loads[3].wait()
    for k in range(zn):
        for i in range(2):
            stage[k, i, :, :sub] = gate_ref[i * deep : (i + 1) * deep, k * sub : (k + 1) * sub]
            stage[k, i, :, sub:] = value_ref[i * deep : (i + 1) * deep, k * sub : (k + 1) * sub]
    with jax.named_scope("barrier"):
        pl.semaphore_wait(barrier, len(partners))

    def lat(zz, yy, q):
        return lat_all.at[2 * zz + yy, q]

    for zz in (far, mid, near):
        send(lat(z, y, t), to_z(zz), "lz", z)
    send(lat(z, y, t), y_dev, "ly", z)
    send(lat(z, y, xt), y_dev, "lxy", z)
    send(stage.at[near], to_z(near), "wz", 2 * z, w_full.at[s])
    for zz, i in ((mid, 0), (mid, 1), (far, 0), (far, 1)):
        send(stage.at[zz, i], to_z(zz), "wz", 2 * z + i, w_full.at[s, i])
    w_full[s] = stage[z]

    for zz in arrivals:
        arrived(lat(zz, y, t), "lz", zz)
        send(lat(zz, y, t), y_dev, "ly", zz)
        send(lat(zz, y, t), x_dev, "lx", zz)
        send(lat(zz, y, t), c_dev, "lcz", zz)
    arrived(lat(z, yo, t), "ly", z)
    send(lat(z, yo, t), c_dev, "lcy", z)
    arrived(lat(z, yo, xt), "lxy", z)
    send(lat(z, yo, xt), c_dev, "lcxy", z)
    for i, zz in enumerate(arrivals):
        arrived(lat(zz, yo, t), "ly", zz)
        if i < 2:
            send(lat(zz, yo, t), x_dev, "lxy", zz)
        send(lat(zz, yo, t), c_dev, "lcy", zz)
        arrived(lat(zz, y, xt), "lx", zz)
        if i == 2:
            send(lat(zz, y, xt), y_dev, "lxy", zz)
        send(lat(zz, y, xt), c_dev, "lcx", zz)
    send(w_full.at[s], y_dev, "wy", 2 * z)

    loads[4].wait()
    rot = NOPE_A + NOPE_B
    q = q_ref[...].astype(f32)
    q_wide = q[:NOPE_A].T.astype(bf16)
    pair = jnp.concatenate([q[NOPE_A:rot], turn(q[rot : rot + ROPE])], axis=0).T.astype(bf16)
    q_narrow, q_wide_t = pair[:, :NOPE_B], pair[:, NOPE_B:]
    turned = turn(q[rot + ROPE :])
    q_narrow_t = jnp.concatenate([turned, jnp.zeros_like(turned)], axis=0).T.astype(bf16)[:, :ROPE]
    loads[5].wait()
    dn_full[s] = down_ref[pl.ds(pl.multiple_of(z * sub, sub), sub), :]
    loads[6].wait()

    for zz in arrivals:
        arrived(lat(zz, yo, xt), "lxy", zz)
        send(lat(zz, yo, xt), c_dev, "lcxy", zz)
    for zz in arrivals:
        arrived(lat(zz, y, ct), "lcz", zz)
        arrived(lat(zz, y, xct), "lcx", zz)
    for zz in (z,) + arrivals:
        arrived(lat(zz, yo, ct), "lcy", zz)
        arrived(lat(zz, yo, xct), "lcxy", zz)

    whole = lat_all[...].reshape(sp * 4 * packed, lat_all.shape[3])
    expand_w = expand_ref[...]
    expanded = jnp.concatenate(
        [
            jnp.dot(whole[:, j * rank : (j + 1) * rank], expand_w, preferred_element_type=f32).astype(bf16)
            for j in range(2)
        ],
        axis=0,
    )
    keys_t = whole[:, 2 * rank :]
    empty = jnp.zeros((rows, ROPE), bf16)

    def attend(qc, qt, kc, v, scale):
        dims = (((1,), (1,)), ((), ()))
        turned_scores = [
            lax.dot_general(jnp.concatenate(two, axis=1), keys_t, dims, preferred_element_type=f32)
            for two in ([qt, empty], [empty, qt])
        ]
        scores = (
            lax.dot_general(qc, kc, dims, preferred_element_type=f32) + jnp.concatenate(turned_scores, axis=1)
        ) * scale
        w = jnp.exp(scores - jnp.max(scores, axis=1, keepdims=True))
        total = jnp.sum(w, axis=1, keepdims=True)
        return (jnp.dot(w.astype(bf16), v, preferred_element_type=f32) / total).astype(bf16)

    nb = NOPE_A + VAL_A
    wide = attend(q_wide, q_wide_t, expanded[:, :NOPE_A], expanded[:, NOPE_A:nb], (NOPE_A + ROPE) ** -0.5)
    narrow = attend(
        q_narrow, q_narrow_t, expanded[:, nb : nb + NOPE_B],
        expanded[:, nb + NOPE_B : nb + NOPE_B + VAL_B], (NOPE_B + ROPE) ** -0.5,
    )
    vals = VAL_A + VAL_B
    for i in range(4):
        att_send[i % 2, i // 2, :, :VAL_A] = wide[i * share : (i + 1) * share, :]
        att_send[i % 2, i // 2, :, VAL_A:vals] = narrow[i * share : (i + 1) * share, :]
    send(att_send.at[c], x_dev, "at", t, att_recv.at[t])
    send(att_send.at[co], xc_dev, "at", t, att_recv.at[t])
    send(att_send.at[co], c_dev, "at", t, att_recv.at[t])
    att_recv[t] = att_send[c]

    arrived(w_full.at[2 * near + y], "wz", 2 * near)
    send(w_full.at[2 * near + y], y_dev, "wy", 2 * near)
    first_on = inner * c == 1
    weights_in = [
        (k, i, send_in(first_on, (1 - inner * c) * (1 - i + i * inner) == 1, i * (1 - inner) == 1))
        for k in (mid, far) for i in range(2)
    ]

    def forward_weights(which):
        for zz, i, pass_on in weights_in:
            if which < 2 or i == 1:
                pass_on(which, w_full.at[2 * zz + y, i], y_dev, "wy", 2 * zz + i, wait="wz")

    forward_weights(0)
    for load in loads[7:]:
        load.wait()
    for o in (ct, xt, xct):
        arrived(att_recv.at[o], "at", o)

    projected = None
    for i in range(4):
        term = jnp.dot(
            att_recv[i].reshape(2 * share, att_recv.shape[3])[:, :vals],
            out_w_ref[i * vals : (i + 1) * vals, :], preferred_element_type=f32,
        )
        projected = term if projected is None else projected + term
    stream = (res_ref[...].reshape(2 * share, res_ref.shape[2]).astype(f32) + projected).astype(bf16)
    stream_f = stream.astype(f32)
    scaled = stream_f * lax.rsqrt(jnp.mean(stream_f * stream_f, axis=1, keepdims=True) + 1e-06)
    normed = (scaled * gain_ref[...].astype(f32).reshape(1, scaled.shape[1])).astype(bf16)
    piece_rows = share // 2
    for i in range(2):
        for j in range(2):
            first = i * share + j * piece_rows
            nrm[z, 2 * i + c, j] = normed[first : first + piece_rows]
        own_stream[i] = stream[i * share : (i + 1) * share]

    for j in range(2):
        send(nrm.at[z, t, j], to_z(mid), "nz", 2 * z + j)
        send(nrm.at[z, t, j], to_z(near), "nz", 2 * z + j)
    send(nrm.at[z, t], c_dev, "ncz", 2 * z)
    send(nrm.at[z, xt], c_dev, "ncx", 2 * z)
    send(dn_full.at[s], y_dev, "dy", z)
    forward_weights(1)

    outer_turns = ((near, 0), (near, 1), (mid, 0), (far, 0), (mid, 1), (far, 1))
    inner_turns = ((mid, 0), (far, 0), (mid, 1), (far, 1), (near, 0), (near, 1))
    turns = [(a + inner * (b - a), i + inner * (j - i)) for (a, i), (b, j) in zip(outer_turns, inner_turns)]

    def from_x(n):
        zz, j = turns[n]
        arrived(nrm.at[zz, xt, j], "nx", 2 * zz + j)
        send(nrm.at[zz, xt, j], c_dev, "ncx", 2 * zz + j)

    passed = []
    for n, (zz, j) in enumerate(turns):
        blk = nrm.at[zz, t, j]
        arrived(blk, "nz", 2 * zz + j)
        if n < 4:
            on = copy_to(blk, blk, to_z(near), "nz", 2 * zz + j, new_slot())
            passed.append(on)

            @pl.when(inner == 1)
            def _():
                on.start()

        send(blk, x_dev, "nx", 2 * zz + j)
        send(blk, c_dev, "ncz", 2 * zz + j)
        if n == 1:
            forward_weights(2)
        if n > 1:
            from_x(n - 2)
    for zz in (near, mid, far):
        piece = down_ref.at[pl.ds(pl.multiple_of(zz * sub, sub), sub), :]
        send(piece, to_z(zz), "dz", z, dn_full.at[s])
    from_x(len(turns) - 2)
    from_x(len(turns) - 1)
    for zz in (z, near):
        arrived(w_full.at[2 * zz + yo], "wy", 2 * zz)
    for zz, i, _ in weights_in:
        arrived(w_full.at[2 * zz + yo, i], "wy", 2 * zz + i)
    weights = w_full[...].reshape(sp * 2 * deep, 2 * sub)
    def forward_down(zz):
        arrived(dn_full.at[2 * zz + y], "dz", zz)
        send(dn_full.at[2 * zz + y], y_dev, "dy", zz)

    for i, zz in enumerate((z,) + arrivals):
        if i == 0:
            arrived(nrm.at[zz, ct], "ncz", 2 * zz)
            arrived(nrm.at[zz, xct], "ncx", 2 * zz)
        else:
            for j in range(2):
                arrived(nrm.at[zz, ct, j], "ncz", 2 * zz + j)
                arrived(nrm.at[zz, xct, j], "ncx", 2 * zz + j)
        block = nrm[zz].reshape(rows, nrm.shape[4])
        hbuf[zz] = jnp.dot(block, weights, preferred_element_type=f32).astype(bf16)

    wide_lanes = halo_send.shape[1]
    for k in range(zn):
        g = hbuf[k, :, :wide_lanes].astype(f32)
        halo_send[k : k + 1, :] = g[rows - 1 : rows, :]
        halo_send[zn + k : zn + k + 1, :] = g[0:1, :]
    send(halo_send, y_dev, "h", 0, halo_recv)

    columns = (z, near, mid, far)
    forward_down(near)
    conv_all = conv_ref[...].astype(f32)
    pieces = [conv_all[:, k * sub : (k + 1) * sub] for k in range(zn)]
    taps = pieces[0]
    for k in range(1, zn):
        taps = jnp.where(z == k, pieces[k], taps)
    taps = jnp.concatenate([taps, jnp.zeros((taps.shape[0], wide_lanes - sub), f32)], axis=1)
    row_id = lax.broadcasted_iota(jnp.int32, (rows, wide_lanes), 0)
    arrived(halo_recv, "h", 0)
    nothing = jnp.zeros((1, wide_lanes), f32)
    for k in range(zn):
        before_low = halo_recv[k - 1 : k, :] if k > 0 else nothing
        before = jnp.where(y == 0, before_low, halo_recv[k : k + 1, :])
        after_high = halo_recv[zn + k + 1 : zn + k + 2, :] if k < zn - 1 else nothing
        after = jnp.where(y == 0, halo_recv[zn + k : zn + k + 1, :], after_high)
        g = hbuf[k, :, :wide_lanes].astype(f32)
        up = jnp.where(row_id == 0, before, pltpu.roll(g, 1, 0))
        down = jnp.where(row_id == rows - 1, after, pltpu.roll(g, rows - 1, 0))
        mixed = up * taps[0:1] + g * taps[1:2] + down * taps[2:3]
        mixed = mixed[:, :sub]
        v = hbuf[k].astype(f32)[:, sub:]
        abuf[k] = (mixed / (1.0 + jnp.exp(-mixed)) * v).astype(bf16)

    order = (far, mid, near, z)
    depth = dn_full.shape[2]
    two = 2 * depth

    def multiply(g):
        zz = columns[g]
        arrived(dn_full.at[2 * zz + yo], "dy", zz)
        down = jnp.concatenate([dn_full[2 * zz], dn_full[2 * zz + 1]], axis=1)
        for d, to in enumerate(order):
            p = jnp.dot(abuf[to], down, preferred_element_type=f32)
            part[g, d] = p.reshape(4, share, two)
            for i in range(2):
                c_send[g, d, i] = part[g, d, 2 * i + co].astype(bf16)
        send(c_send.at[g], c_dev, "pc", g, c_recv.at[g])

    def over_x(g):
        arrived(c_recv.at[g], "pc", g)
        for d in range(zn):
            x_send[g, d] = (part[g, d, xt] + c_recv[g, d, xo].astype(f32)).astype(bf16)
            send(x_send.at[g, d], x_dev, "px", g * zn + d, x_recv.at[g, d])
            keep[g, d] = part[g, d, t] + c_recv[g, d, x].astype(f32)

    def over_z(g):
        for d, to in enumerate(order):
            arrived(x_recv.at[g, d], "px", g * zn + d)
            both = keep[g, d] + x_recv[g, d].astype(f32)
            if d < zn - 1:
                z_send[g, d] = both.astype(bf16)
                send(z_send.at[g, d], to_z(to), "pz", columns[g] * zn + z, z_recv.at[columns[g], z])
            else:
                keep[g, d] = both

    multiply(0)
    forward_down(mid)
    over_x(0)
    multiply(1)
    over_x(1)
    over_z(0)
    forward_down(far)
    multiply(2)
    over_x(2)
    over_z(1)
    multiply(3)
    over_x(3)
    over_z(2)
    over_z(3)
    leaving = []
    for g, zz in enumerate(columns):
        total = keep[g, zn - 1]
        for frm in arrivals:
            arrived(z_recv.at[zz, frm], "pz", zz * zn + frm)
            total += z_recv[zz, frm].astype(f32)
        where = pl.ds(pl.multiple_of(zz * two, two), two)
        result[:, where] = (own_stream[x, :, where].astype(f32) + total).astype(bf16)
        leave = pltpu.make_async_copy(result.at[:, where], out_ref.at[:, where], in_s.at[len(pairs) + g])
        leave.start()
        leaving.append(leave)
    for copy in started:
        copy.wait_send()

    @pl.when(inner == 1)
    def _():
        for on in passed:
            on.wait_send()

    for leave in leaving:
        leave.wait()


def kernel_body(zn, *args):
    (queries, latents, shared_key, expand_weight, residual, out_weight, norm_gain,
     gate_weight, value_weight, conv_weight, down_weight) = args
    rows, width = residual.shape
    sub = down_weight.shape[0] // zn
    share = rows // 4
    d_own = gate_weight.shape[0]
    group = 2 * down_weight.shape[1]
    bf16, f32 = jnp.bfloat16, jnp.float32
    vals = VAL_A + VAL_B
    lanes = -(-vals // 128) * 128
    halo_lanes = -(-sub // 128) * 128
    V, DMA = pltpu.VMEM, pltpu.SemaphoreType.DMA
    return pl.pallas_call(
        functools.partial(layer_kernel, zn),
        out_shape=jax.ShapeDtypeStruct((share, width), bf16),
        in_specs=[pl.BlockSpec(memory_space=pl.ANY)] * 11,
        out_specs=pl.BlockSpec(memory_space=pl.ANY),
        scratch_shapes=[
            V((queries.shape[1], rows), bf16),
            V(latents.shape, bf16),
            V((ROPE, rows), bf16),
            V(conv_weight.shape, bf16),
            V((width,), bf16),
            V(expand_weight.shape, bf16),
            V((2, share, width), bf16),
            V(out_weight.shape, bf16),
            V(gate_weight.shape, bf16),
            V(value_weight.shape, bf16),
            V(down_weight.shape, bf16),
            V((2 * zn, 4, share // 2, 2 * latents.shape[1] + 2 * ROPE), bf16),
            V((2, 2, share, lanes), bf16),
            V((4, 2, share, lanes), bf16),
            V((2, share, width), bf16),
            V((zn, 4, 2, share // 2, width), bf16),
            V((zn, 2, d_own // 2, 2 * sub), bf16),
            V((2 * zn, 2, d_own // 2, 2 * sub), bf16),
            V((2 * zn, sub, down_weight.shape[1]), bf16),
            V((zn, rows, 2 * sub), bf16),
            V((zn, rows, sub), bf16),
            V((2 * zn, halo_lanes), f32),
            V((2 * zn, halo_lanes), f32),
            V((zn, zn, 4, share, group), f32),
            V((zn, zn, 2, share, group), bf16),
            V((zn, zn, 2, share, group), bf16),
            V((zn, zn, share, group), f32),
            V((zn, zn, share, group), bf16),
            V((zn, zn, share, group), bf16),
            V((zn, zn, share, group), bf16),
            V((zn, zn, share, group), bf16),
            V((share, width), bf16),
            DMA((12 + zn,)),
            DMA((SENDS,)),
            DMA((len(KINDS) * zn,)),
        ],
        compiler_params=pltpu.CompilerParams(collective_id=0, has_side_effects=True),
    )(queries.T, latents, shared_key.T, conv_weight, norm_gain, expand_weight, residual,
      out_weight, gate_weight, value_weight, down_weight)


def pick(*args):
    zn = lax.axis_size("sp") // 2
    hidden = args[10].shape[0]
    sub = hidden // zn
    fits = (
        lax.axis_size("sp") == 8
        and lax.axis_size("tp") == 4
        and hidden % zn == 0
        and sub % 64 == 0
        and args[7].shape[0] % 128 == 0
        and args[0].shape[0] % 128 == 0
        and args[4].shape[1] % args[0].shape[0] == 0
        and args[9].shape[0] == 3
    )
    return kernel_body(zn, *args) if fits else body(*args)


def solution(mesh):
    in_specs = (
        P("sp", "tp"),
        P("sp", None),
        P("sp", None),
        P(None, "tp"),
        P("sp", None),
        P(),
        P(),
        P("sp", "tp"),
        P("sp", "tp"),
        P(None, "tp"),
        P("tp", "sp"),
    )
    out_specs = P(("sp", "tp"), None)
    return jax.shard_map(pick, mesh=mesh, in_specs=in_specs, out_specs=out_specs, check_vma=False)
```

```python
import functools
import math

import jax
import jax.numpy as jnp
from jax import lax
from jax.experimental import pallas as pl
from jax.experimental.pallas import tpu as pltpu
from jax.sharding import PartitionSpec as P

NOPE_A = 128
VAL_A = 128
NOPE_B = 64
VAL_B = 64
ROPE = 64


def padded_2(block, sides, width):
    for axis, dim in sides:
        count = lax.axis_size(axis)
        forward = [(i, i + 1) for i in range(count - 1)]
        backward = [(target, source) for source, target in forward]
        low = lax.ppermute(
            lax.slice_in_dim(block, block.shape[dim] - width, None, axis=dim), axis, forward
        )
        high = lax.ppermute(lax.slice_in_dim(block, 0, width, axis=dim), axis, backward)
        block = jnp.concatenate([low, block, high], axis=dim)
    return block


def tables(positions, width):
    half_width = width // 2
    frequency = 10000.0 ** (-jnp.arange(half_width, dtype=jnp.float32) / half_width)
    angles = positions.astype(jnp.float32)[:, None] * frequency[None, :]
    return (jnp.cos(angles), jnp.sin(angles))


def rotate(vectors, cos_table, sine_table):
    half_width = vectors.shape[-1] // 2
    first_half = vectors[:, :half_width].astype(jnp.float32)
    second_half = vectors[:, half_width:].astype(jnp.float32)
    turned = jnp.concatenate(
        [
            first_half * cos_table - second_half * sine_table,
            second_half * cos_table + first_half * sine_table,
        ],
        axis=1,
    )
    return turned.astype(jnp.bfloat16)


def normalize(stream, norm_gain):
    stream_f = stream.astype(jnp.float32)
    scaled = stream_f * lax.rsqrt(jnp.mean(stream_f * stream_f, axis=1, keepdims=True) + 1e-06)
    return (scaled * norm_gain.astype(jnp.float32)).astype(jnp.bfloat16)


def update(running, q_content, q_turned, k_content, k_turned, values, score_scale):
    row_max, row_sum, weighted = running
    scores = (
        jnp.einsum("qd,kd->qk", q_content, k_content, preferred_element_type=jnp.float32)
        + jnp.einsum("qd,kd->qk", q_turned, k_turned, preferred_element_type=jnp.float32)
    ) * score_scale
    new_max = jnp.maximum(row_max, jnp.max(scores, axis=1))
    weights = jnp.exp(scores - new_max[:, None])
    row_sum = jnp.sum(weights, axis=1)
    weighted = jnp.dot(weights.astype(jnp.bfloat16), values, preferred_element_type=jnp.float32)
    return (new_max, row_sum, weighted)


def body(
    queries,
    latents,
    shared_key,
    expand_weight,
    residual,
    out_weight,
    norm_gain,
    gate_weight,
    value_weight,
    conv_weight,
    down_weight,
):
    tok_rows = queries.shape[0]
    q_width = NOPE_A + NOPE_B + 2 * ROPE
    kv_width = NOPE_A + VAL_A + NOPE_B + VAL_B
    positions = lax.axis_index("sp") * tok_rows + jnp.arange(tok_rows, dtype=jnp.int32)
    cos_table, sine_table = tables(positions, ROPE)
    key_turned = rotate(shared_key, cos_table, sine_table)
    scale_wide = (NOPE_A + ROPE) ** (-0.5)
    scale_narrow = (NOPE_B + ROPE) ** (-0.5)
    initial = []
    pair_index = 0
    q_base = pair_index * q_width
    rotary_base = q_base + NOPE_A + NOPE_B
    wide_content = queries[:, q_base : q_base + NOPE_A]
    narrow_content = queries[:, q_base + NOPE_A : rotary_base]
    wide_turned = rotate(queries[:, rotary_base : rotary_base + ROPE], cos_table, sine_table)
    narrow_turned = rotate(
        queries[:, rotary_base + ROPE : rotary_base + 2 * ROPE], cos_table, sine_table
    )
    query_parts = [(wide_content, wide_turned, narrow_content, narrow_turned)]
    lowest = jnp.full((tok_rows,), -1e30, jnp.float32)
    empty_sum = jnp.zeros((tok_rows,), jnp.float32)
    initial += [
        lowest,
        empty_sum,
        jnp.zeros((tok_rows, VAL_A), jnp.float32),
        lowest,
        empty_sum,
        jnp.zeros((tok_rows, VAL_B), jnp.float32),
    ]
    initial = tuple(initial)
    pieces = (
        lax.all_gather(latents, "sp", axis=0, tiled=True),
        lax.all_gather(key_turned, "sp", axis=0, tiled=True),
    )
    expanded = jnp.dot(pieces[0], expand_weight, preferred_element_type=jnp.float32).astype(
        jnp.bfloat16
    )
    turned_keys = pieces[1]
    result = []
    pair_index = 0
    wide_content, wide_turned, narrow_content, narrow_turned = query_parts[pair_index]
    kv_base = pair_index * kv_width
    narrow_base = kv_base + NOPE_A + VAL_A
    wide_keys = expanded[:, kv_base : kv_base + NOPE_A]
    wide_values = expanded[:, kv_base + NOPE_A : narrow_base]
    narrow_keys = expanded[:, narrow_base : narrow_base + NOPE_B]
    narrow_values = expanded[:, narrow_base + NOPE_B : narrow_base + NOPE_B + VAL_B]
    absorb_offset = 6 * pair_index
    result += list(
        update(
            initial[absorb_offset : absorb_offset + 3],
            wide_content,
            wide_turned,
            wide_keys,
            turned_keys,
            wide_values,
            scale_wide,
        )
    )
    result += list(
        update(
            initial[absorb_offset + 3 : absorb_offset + 6],
            narrow_content,
            narrow_turned,
            narrow_keys,
            turned_keys,
            narrow_values,
            scale_narrow,
        )
    )
    running = tuple(result)
    outputs = []
    pair_index = 0
    for group_index in range(2):
        offset = 6 * pair_index + 3 * group_index
        outputs.append((running[offset + 2] / running[offset + 1][:, None]).astype(jnp.bfloat16))
    attended = jnp.concatenate(outputs, axis=1)
    share = tok_rows // lax.axis_size("tp")
    tp_index = lax.axis_index("tp")
    all_heads = lax.all_gather(attended, "tp", axis=1, tiled=True)
    projected = jnp.dot(all_heads, out_weight, preferred_element_type=jnp.float32)
    stream = (residual.astype(jnp.float32) + projected).astype(jnp.bfloat16)
    normed = normalize(stream, norm_gain)
    stream_own = lax.dynamic_slice_in_dim(stream, tp_index * share, share, 0)
    pieces = (
        lax.all_gather(gate_weight, "sp", axis=0, tiled=True),
        lax.all_gather(value_weight, "sp", axis=0, tiled=True),
    )
    gate_sum = jnp.dot(normed, pieces[0], preferred_element_type=jnp.float32)
    value_sum = jnp.dot(normed, pieces[1], preferred_element_type=jnp.float32)
    gate_pre = gate_sum.astype(jnp.bfloat16)
    value_pre = value_sum.astype(jnp.bfloat16)
    reach = conv_weight.shape[0] // 2
    padded = padded_2(gate_pre, (("sp", 0),), reach)
    mixed_gate = jnp.zeros(gate_pre.shape, jnp.float32)
    for tap in range(conv_weight.shape[0]):
        mixed_gate = mixed_gate + padded[tap : tap + tok_rows].astype(jnp.float32) * conv_weight[
            tap
        ].astype(jnp.float32)
    active = (jax.nn.silu(mixed_gate) * value_pre.astype(jnp.float32)).astype(jnp.bfloat16)
    partial_rows = jnp.dot(
        active,
        lax.all_gather(down_weight, "sp", axis=1, tiled=True),
        preferred_element_type=jnp.float32,
    )
    summed = lax.psum_scatter(
        partial_rows.astype(jnp.bfloat16), "tp", scatter_dimension=0, tiled=True
    ).astype(jnp.float32)
    return (stream_own.astype(jnp.float32) + summed).astype(jnp.bfloat16)


MESH = pl.DeviceIdType.MESH
SINGLE = ("lc", "wy", "at", "h", "pz")
PER_Z = ("lz", "ly", "lx", "lxy", "dz", "dy", "nc", "pc")
PER_HALF = ("wz", "nz", "nx")
GROUPS = ("lat", "weights", "down", "own", "relay", "normed", "at", "h", "pc", "px", "pz")


def semaphore_places(zn):
    places, count = {}, 0
    for kinds, width in ((SINGLE, 1), (PER_Z, zn), (PER_HALF, 2 * zn), (("px",), zn * zn)):
        for kind in kinds:
            places[kind] = count
            count += width
    return places, count


def layer_kernel(
    zn,
    q_hbm,
    lat_hbm,
    key_hbm,
    conv_hbm,
    gain_hbm,
    expand_hbm,
    res_hbm,
    out_w_hbm,
    gate_hbm,
    value_hbm,
    down_hbm,
    out_ref,
    q_ref,
    lat_ref,
    key_ref,
    conv_ref,
    gain_ref,
    expand_ref,
    res_ref,
    out_w_ref,
    gate_ref,
    value_ref,
    down_ref,
    lat_all,
    att_send,
    att_recv,
    own_stream,
    nrm,
    stage,
    w_full,
    dn_full,
    hbuf,
    abuf,
    halo_send,
    halo_recv,
    part,
    c_send,
    c_recv,
    keep,
    x_send,
    x_recv,
    z_send,
    z_recv,
    result,
    in_s,
    send_s,
    recv_s,
):
    f32, bf16 = jnp.float32, jnp.bfloat16
    s, t = lax.axis_index("sp"), lax.axis_index("tp")
    z, y = s // 2, s % 2
    x, c = t // 2, t % 2
    yo, xo, co = 1 - y, 1 - x, 1 - c
    xt, ct, xct = 2 * xo + c, 2 * x + co, 2 * xo + co
    rows = lat_ref.shape[0]
    share = rows // 4
    packed = share // 2
    rank = lat_ref.shape[1]
    sub = down_ref.shape[0] // zn
    sp = 2 * zn
    deep = gate_ref.shape[0] // 2

    inner = ((z + 1) // 2) % 2
    near = z + 1 - 2 * (z % 2)
    mid = (z + 2) % zn + inner * (zn - 1 - z - (z + 2) % zn)
    far = zn - 1 - z + inner * ((z + 2) % zn - (zn - 1 - z))
    arrivals = (near + inner * (mid - near), mid + inner * (far - mid), far + inner * (near - far))

    def to_z(zz):
        return {"sp": 2 * zz + y, "tp": t}

    y_dev = {"sp": 2 * z + yo, "tp": t}
    x_dev = {"sp": s, "tp": xt}
    c_dev = {"sp": s, "tp": ct}
    xc_dev = {"sp": s, "tp": xct}

    places, _ = semaphore_places(zn)

    def copy_to(src, dst, dev, kind, i, group):
        return pltpu.make_async_remote_copy(
            src_ref=src, dst_ref=dst, send_sem=send_s.at[GROUPS.index(group)],
            recv_sem=recv_s.at[places[kind] + i], device_id=dev, device_id_type=MESH,
        )

    def send(ref, dev, kind, i, group, dst=None):
        copy_to(ref, ref if dst is None else dst, dev, kind, i, group).start()

    def send_if(condition, ref, dev, kind, i, group, dst=None, wait=None):
        @pl.when(condition)
        def _():
            if wait is not None:
                arrived(ref, wait, i)
            send(ref, dev, kind, i, group, dst)

    def arrived(dst, kind, i):
        with jax.named_scope("wait_" + kind):
            copy_to(dst, dst, c_dev, kind, i, "lat").wait_recv()

    def all_sent(ref, group):
        copy_to(ref, ref, c_dev, "lz", 0, group).wait_send()

    barrier = pltpu.get_barrier_semaphore()
    partners = [to_z(near), to_z(mid), to_z(far), y_dev, x_dev, c_dev, xc_dev]
    for dev in partners:
        pl.semaphore_signal(barrier, inc=1, device_id=dev, device_id_type=MESH)

    def res_rows(i):
        return res_hbm.at[pl.ds(pl.multiple_of((2 * i + c) * share, share), share), :]

    pairs = [
        (key_hbm, key_ref),
        (lat_hbm, lat_ref),
        (gate_hbm, gate_ref),
        (value_hbm, value_ref),
        (q_hbm, q_ref),
        (down_hbm, down_ref),
        (expand_hbm, expand_ref),
        (res_rows(0), res_ref.at[0]),
        (res_rows(1), res_ref.at[1]),
        (gain_hbm, gain_ref),
        (conv_hbm, conv_ref),
        (out_w_hbm, out_w_ref),
    ]
    loads = [pltpu.make_async_copy(src, dst, in_s.at[i]) for i, (src, dst) in enumerate(pairs)]
    for load in loads:
        load.start()

    h = ROPE // 2
    step = lax.broadcasted_iota(jnp.int32, (h, rows), 0).astype(f32) * (-math.log(10000.0) / h)
    spot = (s * rows + lax.broadcasted_iota(jnp.int32, (h, rows), 1)).astype(f32)
    angles = spot * jnp.exp(step)
    cos, sine = jnp.cos(angles), jnp.sin(angles)

    def turn(v):
        a, b = v[:h], v[h:]
        return jnp.concatenate([a * cos - b * sine, b * cos + a * sine], axis=0)

    loads[0].wait()
    turned = turn(key_ref[...].astype(f32))
    key_turned = jnp.concatenate([turned, jnp.zeros_like(turned)], axis=0).T.astype(bf16)[:, :ROPE]
    loads[1].wait()
    for i in range(4):
        for j in range(2):
            first = i * share + j * packed
            lat_all[s, i, :, j * rank : (j + 1) * rank] = lat_ref[first : first + packed, :]
        lat_all[s, i, :, 2 * rank :] = jnp.concatenate(
            [key_turned[i * share : i * share + packed], key_turned[i * share + packed : (i + 1) * share]], axis=1
        )
    with jax.named_scope("barrier"):
        pl.semaphore_wait(barrier, len(partners))

    def lat(zz, yy, q):
        return lat_all.at[2 * zz + yy, q]

    for zz in (far, mid, near):
        send(lat(z, y, t), to_z(zz), "lz", z, "lat")
    send(lat(z, y, t), y_dev, "ly", z, "lat")
    send(lat(z, y, xt), y_dev, "lxy", z, "lat")
    loads[2].wait()
    loads[3].wait()
    for k in range(zn):
        for i in range(2):
            stage[k, i, :, :sub] = gate_ref[i * deep : (i + 1) * deep, k * sub : (k + 1) * sub]
            stage[k, i, :, sub:] = value_ref[i * deep : (i + 1) * deep, k * sub : (k + 1) * sub]
    send(stage.at[near], to_z(near), "wz", 2 * z, "weights", w_full.at[s])
    for zz, i in ((mid, 0), (mid, 1), (far, 0), (far, 1)):
        send(stage.at[zz, i], to_z(zz), "wz", 2 * z + i, "weights", w_full.at[s, i])
    w_full[s] = stage[z]

    for zz in arrivals:
        arrived(lat(zz, y, t), "lz", zz)
        send(lat(zz, y, t), y_dev, "ly", zz, "lat")
        send(lat(zz, y, t), x_dev, "lx", zz, "lat")
        send(lat(zz, y, t), c_dev, "lc", 0, "lat")
    arrived(lat(z, yo, t), "ly", z)
    send(lat(z, yo, t), c_dev, "lc", 0, "lat")
    arrived(lat(z, yo, xt), "lxy", z)
    send(lat(z, yo, xt), c_dev, "lc", 0, "lat")
    for i, zz in enumerate(arrivals):
        arrived(lat(zz, yo, t), "ly", zz)
        if i < 2:
            send(lat(zz, yo, t), x_dev, "lxy", zz, "lat")
        send(lat(zz, yo, t), c_dev, "lc", 0, "lat")
        arrived(lat(zz, y, xt), "lx", zz)
        if i == 2:
            send(lat(zz, y, xt), y_dev, "lxy", zz, "lat")
        send(lat(zz, y, xt), c_dev, "lc", 0, "lat")
    send(w_full.at[s], y_dev, "wy", 0, "weights")

    loads[4].wait()
    rot = NOPE_A + NOPE_B
    q = q_ref[...].astype(f32)
    q_wide = q[:NOPE_A].T.astype(bf16)
    pair = jnp.concatenate([q[NOPE_A:rot], turn(q[rot : rot + ROPE])], axis=0).T.astype(bf16)
    q_narrow, q_wide_t = pair[:, :NOPE_B], pair[:, NOPE_B:]
    turned = turn(q[rot + ROPE :])
    q_narrow_t = jnp.concatenate([turned, jnp.zeros_like(turned)], axis=0).T.astype(bf16)[:, :ROPE]
    loads[5].wait()
    dn_full[s] = down_ref[pl.ds(pl.multiple_of(z * sub, sub), sub), :]
    loads[6].wait()

    for zz in arrivals:
        arrived(lat(zz, yo, xt), "lxy", zz)
        send(lat(zz, yo, xt), c_dev, "lc", 0, "lat")
    arrived(lat_all.at[pl.ds(0, sp - 1), pl.ds(0, 2)], "lc", 0)

    whole = lat_all[...].reshape(sp * 4 * packed, lat_all.shape[3])
    expand_w = expand_ref[...]
    expanded = jnp.concatenate(
        [
            jnp.dot(whole[:, j * rank : (j + 1) * rank], expand_w, preferred_element_type=f32).astype(bf16)
            for j in range(2)
        ],
        axis=0,
    )
    keys_t = whole[:, 2 * rank :]
    empty = jnp.zeros((rows, ROPE), bf16)

    def attend(qc, qt, kc, v, scale):
        dims = (((1,), (1,)), ((), ()))
        turned_scores = [
            lax.dot_general(jnp.concatenate(two, axis=1), keys_t, dims, preferred_element_type=f32)
            for two in ([qt, empty], [empty, qt])
        ]
        scores = (
            lax.dot_general(qc, kc, dims, preferred_element_type=f32) + jnp.concatenate(turned_scores, axis=1)
        ) * scale
        w = jnp.exp(scores - jnp.max(scores, axis=1, keepdims=True))
        total = jnp.sum(w, axis=1, keepdims=True)
        return (jnp.dot(w.astype(bf16), v, preferred_element_type=f32) / total).astype(bf16)

    nb = NOPE_A + VAL_A
    wide = attend(q_wide, q_wide_t, expanded[:, :NOPE_A], expanded[:, NOPE_A:nb], (NOPE_A + ROPE) ** -0.5)
    narrow = attend(
        q_narrow, q_narrow_t, expanded[:, nb : nb + NOPE_B],
        expanded[:, nb + NOPE_B : nb + NOPE_B + VAL_B], (NOPE_B + ROPE) ** -0.5,
    )
    vals = VAL_A + VAL_B
    for i in range(4):
        att_send[i % 2, i // 2, :, :VAL_A] = wide[i * share : (i + 1) * share, :]
        att_send[i % 2, i // 2, :, VAL_A:vals] = narrow[i * share : (i + 1) * share, :]
    send(att_send.at[c], x_dev, "at", 0, "at", att_recv.at[t])
    send(att_send.at[co], xc_dev, "at", 0, "at", att_recv.at[t])
    send(att_send.at[co], c_dev, "at", 0, "at", att_recv.at[t])
    att_recv[t] = att_send[c]

    arrived(w_full.at[2 * near + y], "wz", 2 * near)
    send(w_full.at[2 * near + y], y_dev, "wy", 0, "weights")

    def forward_weights(turn):
        for zz in (mid, far):
            for i in range(2):
                turns = (inner * c, (1 - inner * c) * (1 - i + i * inner), i * (1 - inner))
                if turn == 2 and i == 0:
                    continue

                @pl.when(turns[turn] == 1)
                def _():
                    arrived(w_full.at[2 * zz + y, i], "wz", 2 * zz + i)
                    send(w_full.at[2 * zz + y, i], y_dev, "wy", 0, "weights")

    forward_weights(0)
    for load in loads[7:]:
        load.wait()
    arrived(att_recv.at[pl.ds(0, 3)], "at", 0)

    projected = None
    for i in range(4):
        term = jnp.dot(
            att_recv[i].reshape(2 * share, att_recv.shape[3])[:, :vals],
            out_w_ref[i * vals : (i + 1) * vals, :], preferred_element_type=f32,
        )
        projected = term if projected is None else projected + term
    stream = (res_ref[...].reshape(2 * share, res_ref.shape[2]).astype(f32) + projected).astype(bf16)
    stream_f = stream.astype(f32)
    scaled = stream_f * lax.rsqrt(jnp.mean(stream_f * stream_f, axis=1, keepdims=True) + 1e-06)
    normed = (scaled * gain_ref[...].astype(f32).reshape(1, scaled.shape[1])).astype(bf16)
    piece_rows = share // 2
    for i in range(2):
        for j in range(2):
            first = i * share + j * piece_rows
            nrm[z, 2 * i + c, j] = normed[first : first + piece_rows]
        own_stream[i] = stream[i * share : (i + 1) * share]

    for j in range(2):
        send(nrm.at[z, t, j], to_z(mid), "nz", 2 * z + j, "own")
        send(nrm.at[z, t, j], to_z(near), "nz", 2 * z + j, "own")
    send(nrm.at[z, t], c_dev, "nc", z, "own")
    send(nrm.at[z, xt], c_dev, "nc", z, "own")
    send(dn_full.at[s], y_dev, "dy", z, "down")
    forward_weights(1)

    outer_turns = ((near, 0), (near, 1), (mid, 0), (far, 0), (mid, 1), (far, 1))
    inner_turns = ((mid, 0), (far, 0), (mid, 1), (far, 1), (near, 0), (near, 1))
    turns = [(a + inner * (b - a), i + inner * (j - i)) for (a, i), (b, j) in zip(outer_turns, inner_turns)]

    def from_x(n):
        zz, j = turns[n]
        arrived(nrm.at[zz, xt, j], "nx", 2 * zz + j)
        send(nrm.at[zz, xt, j], c_dev, "nc", zz, "normed")

    def send_down(zz):
        piece = down_ref.at[pl.ds(pl.multiple_of(zz * sub, sub), sub), :]
        send(piece, to_z(zz), "dz", z, "down", dn_full.at[s])

    for n, (zz, j) in enumerate(turns):
        blk = nrm.at[zz, t, j]
        arrived(blk, "nz", 2 * zz + j)
        if n < 4:
            send_if(inner == 1, blk, to_z(near), "nz", 2 * zz + j, "relay")
        send(blk, x_dev, "nx", 2 * zz + j, "normed")
        send(blk, c_dev, "nc", zz, "normed")
        if n == 1:
            forward_weights(2)
        if n > 1:
            from_x(n - 2)
    for to in (near, mid, far):
        send_down(to)
    arrived(w_full.at[pl.ds(0, zn)], "wy", 0)
    weights = w_full[...].reshape(sp * 2 * deep, 2 * sub)

    def forward_down(zz):
        arrived(dn_full.at[2 * zz + y], "dz", zz)
        send(dn_full.at[2 * zz + y], y_dev, "dy", zz, "down")

    def mix(zz):
        hbuf[zz] = jnp.dot(
            nrm[zz].reshape(rows, nrm.shape[4]), weights, preferred_element_type=f32
        ).astype(bf16)

    def block_here(zz):
        arrived(nrm.at[zz, pl.ds(0, 2)], "nc", zz)

    columns = (z, near + inner * (mid - near), mid + inner * (near - mid), far)
    block_here(z)
    mix(z)
    for i, zz in enumerate(arrivals):
        if i > 0:
            from_x(len(turns) - 3 + i)
        block_here(zz)
        mix(zz)

    wide_lanes = halo_send.shape[1]
    for k in range(zn):
        g = hbuf[k, :, :wide_lanes].astype(f32)
        halo_send[k : k + 1, :] = g[rows - 1 : rows, :]
        halo_send[zn + k : zn + k + 1, :] = g[0:1, :]
    send(halo_send, y_dev, "h", 0, "h", halo_recv)

    forward_down(columns[1])
    conv_all = conv_ref[...].astype(f32)
    pieces = [conv_all[:, k * sub : (k + 1) * sub] for k in range(zn)]
    taps = pieces[0]
    for k in range(1, zn):
        taps = jnp.where(z == k, pieces[k], taps)
    taps = jnp.concatenate([taps, jnp.zeros((taps.shape[0], wide_lanes - sub), f32)], axis=1)
    row_id = lax.broadcasted_iota(jnp.int32, (rows, wide_lanes), 0)
    arrived(halo_recv, "h", 0)
    forward_down(columns[2])
    nothing = jnp.zeros((1, wide_lanes), f32)
    for k in range(zn):
        before_low = halo_recv[k - 1 : k, :] if k > 0 else nothing
        before = jnp.where(y == 0, before_low, halo_recv[k : k + 1, :])
        after_high = halo_recv[zn + k + 1 : zn + k + 2, :] if k < zn - 1 else nothing
        after = jnp.where(y == 0, halo_recv[zn + k : zn + k + 1, :], after_high)
        g = hbuf[k, :, :wide_lanes].astype(f32)
        up = jnp.where(row_id == 0, before, pltpu.roll(g, 1, 0))
        down = jnp.where(row_id == rows - 1, after, pltpu.roll(g, rows - 1, 0))
        mixed = up * taps[0:1] + g * taps[1:2] + down * taps[2:3]
        mixed = mixed[:, :sub]
        v = hbuf[k].astype(f32)[:, sub:]
        abuf[k] = (mixed / (1.0 + jnp.exp(-mixed)) * v).astype(bf16)

    order = (far, mid, near, z)
    depth = dn_full.shape[2]
    two = 2 * depth

    def multiply(g):
        zz = columns[g]
        arrived(dn_full.at[2 * zz + yo], "dy", zz)
        down = jnp.concatenate([dn_full[2 * zz], dn_full[2 * zz + 1]], axis=1)
        for d, to in enumerate(order):
            p = jnp.dot(abuf[to], down, preferred_element_type=f32)
            part[g, d] = p.reshape(4, share, two)
            for i in range(2):
                c_send[g, d, i] = part[g, d, 2 * i + co].astype(bf16)
        send(c_send.at[g], c_dev, "pc", g, "pc", c_recv.at[g])

    def over_x(g, turns):
        for d in turns:
            x_send[g, d] = (part[g, d, xt] + c_recv[g, d, xo].astype(f32)).astype(bf16)
            send(x_send.at[g, d], x_dev, "px", g * zn + d, "px", x_recv.at[g, d])
            keep[g, d] = part[g, d, t] + c_recv[g, d, x].astype(f32)

    def over_z(g, turns):
        for d in turns:
            arrived(x_recv.at[g, d], "px", g * zn + d)
            both = keep[g, d] + x_recv[g, d].astype(f32)
            if d < zn - 1:
                z_send[g, d] = both.astype(bf16)
                send(z_send.at[g, d], to_z(order[d]), "pz", 0, "pz", z_recv.at[columns[g], z])
            else:
                keep[g, d] = both

    away, stay = range(zn - 1), range(zn - 1, zn)
    for g in range(zn):
        multiply(g)
        if g == 0:
            forward_down(far)
        arrived(c_recv.at[g], "pc", g)
        over_x(g, away)
        if g > 0:
            over_z(g - 1, away)
    for g in range(zn):
        over_x(g, stay)
    over_z(zn - 1, away)
    for g in range(zn):
        over_z(g, stay)
    leaving = []
    arrived(z_recv.at[:, pl.ds(0, zn - 1)], "pz", 0)
    for g, zz in enumerate(columns):
        total = keep[g, zn - 1]
        for frm in arrivals:
            total += z_recv[zz, frm].astype(f32)
        where = pl.ds(pl.multiple_of(zz * two, two), two)
        result[:, where] = (own_stream[x, :, where].astype(f32) + total).astype(bf16)
        leave = pltpu.make_async_copy(result.at[:, where], out_ref.at[:, where], in_s.at[len(pairs) + g])
        leave.start()
        leaving.append(leave)
    all_sent(lat_all.at[pl.ds(0, sp - 1)], "lat")
    all_sent(w_full.at[pl.ds(0, sp - 1)], "weights")
    all_sent(dn_full.at[pl.ds(0, sp - 1)], "down")
    all_sent(nrm.at[0], "own")
    all_sent(nrm.at[pl.ds(0, zn - 1), pl.ds(0, 3)], "normed")
    all_sent(att_recv.at[pl.ds(0, 3)], "at")
    all_sent(halo_send, "h")
    all_sent(c_send, "pc")
    all_sent(x_send, "px")
    all_sent(z_send.at[:, pl.ds(0, zn - 1)], "pz")

    @pl.when(inner == 1)
    def _():
        all_sent(nrm.at[0, pl.ds(0, 2)], "relay")

    with jax.named_scope("leave"):
        for leave in leaving:
            leave.wait()


def kernel_body(zn, *args):
    (queries, latents, shared_key, expand_weight, residual, out_weight, norm_gain,
     gate_weight, value_weight, conv_weight, down_weight) = args
    rows, width = residual.shape
    sub = down_weight.shape[0] // zn
    share = rows // 4
    d_own = gate_weight.shape[0]
    group = 2 * down_weight.shape[1]
    bf16, f32 = jnp.bfloat16, jnp.float32
    vals = VAL_A + VAL_B
    lanes = -(-vals // 128) * 128
    halo_lanes = -(-sub // 128) * 128
    V, DMA = pltpu.VMEM, pltpu.SemaphoreType.DMA
    return pl.pallas_call(
        functools.partial(layer_kernel, zn),
        out_shape=jax.ShapeDtypeStruct((share, width), bf16),
        in_specs=[pl.BlockSpec(memory_space=pl.ANY)] * 11,
        out_specs=pl.BlockSpec(memory_space=pl.ANY),
        scratch_shapes=[
            V((queries.shape[1], rows), bf16),
            V(latents.shape, bf16),
            V((ROPE, rows), bf16),
            V(conv_weight.shape, bf16),
            V((width,), bf16),
            V(expand_weight.shape, bf16),
            V((2, share, width), bf16),
            V(out_weight.shape, bf16),
            V(gate_weight.shape, bf16),
            V(value_weight.shape, bf16),
            V(down_weight.shape, bf16),
            V((2 * zn, 4, share // 2, 2 * latents.shape[1] + 2 * ROPE), bf16),
            V((2, 2, share, lanes), bf16),
            V((4, 2, share, lanes), bf16),
            V((2, share, width), bf16),
            V((zn, 4, 2, share // 2, width), bf16),
            V((zn, 2, d_own // 2, 2 * sub), bf16),
            V((2 * zn, 2, d_own // 2, 2 * sub), bf16),
            V((2 * zn, sub, down_weight.shape[1]), bf16),
            V((zn, rows, 2 * sub), bf16),
            V((zn, rows, sub), bf16),
            V((2 * zn, halo_lanes), f32),
            V((2 * zn, halo_lanes), f32),
            V((zn, zn, 4, share, group), f32),
            V((zn, zn, 2, share, group), bf16),
            V((zn, zn, 2, share, group), bf16),
            V((zn, zn, share, group), f32),
            V((zn, zn, share, group), bf16),
            V((zn, zn, share, group), bf16),
            V((zn, zn, share, group), bf16),
            V((zn, zn, share, group), bf16),
            V((share, width), bf16),
            DMA((12 + zn,)),
            DMA((len(GROUPS),)),
            DMA((semaphore_places(zn)[1],)),
        ],
        compiler_params=pltpu.CompilerParams(collective_id=0, has_side_effects=True),
    )(queries.T, latents, shared_key.T, conv_weight, norm_gain, expand_weight, residual,
      out_weight, gate_weight, value_weight, down_weight)


def pick(*args):
    zn = lax.axis_size("sp") // 2
    hidden = args[10].shape[0]
    sub = hidden // zn
    fits = (
        lax.axis_size("sp") == 8
        and lax.axis_size("tp") == 4
        and hidden % zn == 0
        and sub % 64 == 0
        and args[7].shape[0] % 128 == 0
        and args[0].shape[0] % 128 == 0
        and args[4].shape[1] % args[0].shape[0] == 0
        and args[9].shape[0] == 3
    )
    return kernel_body(zn, *args) if fits else body(*args)


def solution(mesh):
    in_specs = (
        P("sp", "tp"),
        P("sp", None),
        P("sp", None),
        P(None, "tp"),
        P("sp", None),
        P(),
        P(),
        P("sp", "tp"),
        P("sp", "tp"),
        P(None, "tp"),
        P("tp", "sp"),
    )
    out_specs = P(("sp", "tp"), None)
    return jax.shard_map(pick, mesh=mesh, in_specs=in_specs, out_specs=out_specs, check_vma=False)
```

```python
import functools
import math

import jax
import jax.numpy as jnp
from jax import lax
from jax.experimental import pallas as pl
from jax.experimental.pallas import tpu as pltpu
from jax.sharding import PartitionSpec as P

NOPE_A = 128
VAL_A = 128
NOPE_B = 64
VAL_B = 64
ROPE = 64


def padded_2(block, sides, width):
    for axis, dim in sides:
        count = lax.axis_size(axis)
        forward = [(i, i + 1) for i in range(count - 1)]
        backward = [(target, source) for source, target in forward]
        low = lax.ppermute(
            lax.slice_in_dim(block, block.shape[dim] - width, None, axis=dim), axis, forward
        )
        high = lax.ppermute(lax.slice_in_dim(block, 0, width, axis=dim), axis, backward)
        block = jnp.concatenate([low, block, high], axis=dim)
    return block


def tables(positions, width):
    half_width = width // 2
    frequency = 10000.0 ** (-jnp.arange(half_width, dtype=jnp.float32) / half_width)
    angles = positions.astype(jnp.float32)[:, None] * frequency[None, :]
    return (jnp.cos(angles), jnp.sin(angles))


def rotate(vectors, cos_table, sine_table):
    half_width = vectors.shape[-1] // 2
    first_half = vectors[:, :half_width].astype(jnp.float32)
    second_half = vectors[:, half_width:].astype(jnp.float32)
    turned = jnp.concatenate(
        [
            first_half * cos_table - second_half * sine_table,
            second_half * cos_table + first_half * sine_table,
        ],
        axis=1,
    )
    return turned.astype(jnp.bfloat16)


def normalize(stream, norm_gain):
    stream_f = stream.astype(jnp.float32)
    scaled = stream_f * lax.rsqrt(jnp.mean(stream_f * stream_f, axis=1, keepdims=True) + 1e-06)
    return (scaled * norm_gain.astype(jnp.float32)).astype(jnp.bfloat16)


def update(running, q_content, q_turned, k_content, k_turned, values, score_scale):
    row_max, row_sum, weighted = running
    scores = (
        jnp.einsum("qd,kd->qk", q_content, k_content, preferred_element_type=jnp.float32)
        + jnp.einsum("qd,kd->qk", q_turned, k_turned, preferred_element_type=jnp.float32)
    ) * score_scale
    new_max = jnp.maximum(row_max, jnp.max(scores, axis=1))
    weights = jnp.exp(scores - new_max[:, None])
    row_sum = jnp.sum(weights, axis=1)
    weighted = jnp.dot(weights.astype(jnp.bfloat16), values, preferred_element_type=jnp.float32)
    return (new_max, row_sum, weighted)


def body(
    queries,
    latents,
    shared_key,
    expand_weight,
    residual,
    out_weight,
    norm_gain,
    gate_weight,
    value_weight,
    conv_weight,
    down_weight,
):
    tok_rows = queries.shape[0]
    q_width = NOPE_A + NOPE_B + 2 * ROPE
    kv_width = NOPE_A + VAL_A + NOPE_B + VAL_B
    positions = lax.axis_index("sp") * tok_rows + jnp.arange(tok_rows, dtype=jnp.int32)
    cos_table, sine_table = tables(positions, ROPE)
    key_turned = rotate(shared_key, cos_table, sine_table)
    scale_wide = (NOPE_A + ROPE) ** (-0.5)
    scale_narrow = (NOPE_B + ROPE) ** (-0.5)
    initial = []
    pair_index = 0
    q_base = pair_index * q_width
    rotary_base = q_base + NOPE_A + NOPE_B
    wide_content = queries[:, q_base : q_base + NOPE_A]
    narrow_content = queries[:, q_base + NOPE_A : rotary_base]
    wide_turned = rotate(queries[:, rotary_base : rotary_base + ROPE], cos_table, sine_table)
    narrow_turned = rotate(
        queries[:, rotary_base + ROPE : rotary_base + 2 * ROPE], cos_table, sine_table
    )
    query_parts = [(wide_content, wide_turned, narrow_content, narrow_turned)]
    lowest = jnp.full((tok_rows,), -1e30, jnp.float32)
    empty_sum = jnp.zeros((tok_rows,), jnp.float32)
    initial += [
        lowest,
        empty_sum,
        jnp.zeros((tok_rows, VAL_A), jnp.float32),
        lowest,
        empty_sum,
        jnp.zeros((tok_rows, VAL_B), jnp.float32),
    ]
    initial = tuple(initial)
    pieces = (
        lax.all_gather(latents, "sp", axis=0, tiled=True),
        lax.all_gather(key_turned, "sp", axis=0, tiled=True),
    )
    expanded = jnp.dot(pieces[0], expand_weight, preferred_element_type=jnp.float32).astype(
        jnp.bfloat16
    )
    turned_keys = pieces[1]
    result = []
    pair_index = 0
    wide_content, wide_turned, narrow_content, narrow_turned = query_parts[pair_index]
    kv_base = pair_index * kv_width
    narrow_base = kv_base + NOPE_A + VAL_A
    wide_keys = expanded[:, kv_base : kv_base + NOPE_A]
    wide_values = expanded[:, kv_base + NOPE_A : narrow_base]
    narrow_keys = expanded[:, narrow_base : narrow_base + NOPE_B]
    narrow_values = expanded[:, narrow_base + NOPE_B : narrow_base + NOPE_B + VAL_B]
    absorb_offset = 6 * pair_index
    result += list(
        update(
            initial[absorb_offset : absorb_offset + 3],
            wide_content,
            wide_turned,
            wide_keys,
            turned_keys,
            wide_values,
            scale_wide,
        )
    )
    result += list(
        update(
            initial[absorb_offset + 3 : absorb_offset + 6],
            narrow_content,
            narrow_turned,
            narrow_keys,
            turned_keys,
            narrow_values,
            scale_narrow,
        )
    )
    running = tuple(result)
    outputs = []
    pair_index = 0
    for group_index in range(2):
        offset = 6 * pair_index + 3 * group_index
        outputs.append((running[offset + 2] / running[offset + 1][:, None]).astype(jnp.bfloat16))
    attended = jnp.concatenate(outputs, axis=1)
    share = tok_rows // lax.axis_size("tp")
    tp_index = lax.axis_index("tp")
    all_heads = lax.all_gather(attended, "tp", axis=1, tiled=True)
    projected = jnp.dot(all_heads, out_weight, preferred_element_type=jnp.float32)
    stream = (residual.astype(jnp.float32) + projected).astype(jnp.bfloat16)
    normed = normalize(stream, norm_gain)
    stream_own = lax.dynamic_slice_in_dim(stream, tp_index * share, share, 0)
    pieces = (
        lax.all_gather(gate_weight, "sp", axis=0, tiled=True),
        lax.all_gather(value_weight, "sp", axis=0, tiled=True),
    )
    gate_sum = jnp.dot(normed, pieces[0], preferred_element_type=jnp.float32)
    value_sum = jnp.dot(normed, pieces[1], preferred_element_type=jnp.float32)
    gate_pre = gate_sum.astype(jnp.bfloat16)
    value_pre = value_sum.astype(jnp.bfloat16)
    reach = conv_weight.shape[0] // 2
    padded = padded_2(gate_pre, (("sp", 0),), reach)
    mixed_gate = jnp.zeros(gate_pre.shape, jnp.float32)
    for tap in range(conv_weight.shape[0]):
        mixed_gate = mixed_gate + padded[tap : tap + tok_rows].astype(jnp.float32) * conv_weight[
            tap
        ].astype(jnp.float32)
    active = (jax.nn.silu(mixed_gate) * value_pre.astype(jnp.float32)).astype(jnp.bfloat16)
    partial_rows = jnp.dot(
        active,
        lax.all_gather(down_weight, "sp", axis=1, tiled=True),
        preferred_element_type=jnp.float32,
    )
    summed = lax.psum_scatter(
        partial_rows.astype(jnp.bfloat16), "tp", scatter_dimension=0, tiled=True
    ).astype(jnp.float32)
    return (stream_own.astype(jnp.float32) + summed).astype(jnp.bfloat16)


MESH = pl.DeviceIdType.MESH
SINGLE = ("lc", "wy", "at", "h", "pz")
PER_Z = ("lz", "ly", "lx", "lxy", "dz", "dy", "nc")
PER_HALF = ("wz", "nz", "nx", "pc")
GROUPS = ("lat", "weights", "down", "own", "relay", "normed", "at", "h", "pc", "px", "pz")


def semaphore_places(zn):
    places, count = {}, 0
    for kinds, width in ((SINGLE, 1), (PER_Z, zn), (PER_HALF, 2 * zn), (("px",), zn * zn)):
        for kind in kinds:
            places[kind] = count
            count += width
    return places, count


def layer_kernel(
    zn,
    q_hbm,
    lat_hbm,
    key_hbm,
    conv_hbm,
    gain_hbm,
    expand_hbm,
    res_hbm,
    out_w_hbm,
    gate_hbm,
    value_hbm,
    down_hbm,
    out_ref,
    q_ref,
    lat_ref,
    key_ref,
    conv_ref,
    gain_ref,
    expand_ref,
    res_ref,
    out_w_ref,
    gate_ref,
    value_ref,
    down_ref,
    lat_all,
    att_send,
    att_recv,
    own_stream,
    nrm,
    stage,
    w_full,
    dn_full,
    hbuf,
    abuf,
    halo_send,
    halo_recv,
    part,
    c_send,
    c_recv,
    keep,
    x_send,
    x_recv,
    z_send,
    z_recv,
    result,
    in_s,
    send_s,
    recv_s,
):
    f32, bf16 = jnp.float32, jnp.bfloat16
    s, t = lax.axis_index("sp"), lax.axis_index("tp")
    z, y = s // 2, s % 2
    x, c = t // 2, t % 2
    yo, xo, co = 1 - y, 1 - x, 1 - c
    xt, ct, xct = 2 * xo + c, 2 * x + co, 2 * xo + co
    rows = lat_ref.shape[0]
    share = rows // 4
    packed = share // 2
    rank = lat_ref.shape[1]
    sub = down_ref.shape[0] // zn
    sp = 2 * zn
    deep = gate_ref.shape[0] // 2

    inner = ((z + 1) // 2) % 2
    near = z + 1 - 2 * (z % 2)
    mid = (z + 2) % zn + inner * (zn - 1 - z - (z + 2) % zn)
    far = zn - 1 - z + inner * ((z + 2) % zn - (zn - 1 - z))
    arrivals = (near + inner * (mid - near), mid + inner * (far - mid), far + inner * (near - far))

    def to_z(zz):
        return {"sp": 2 * zz + y, "tp": t}

    y_dev = {"sp": 2 * z + yo, "tp": t}
    x_dev = {"sp": s, "tp": xt}
    c_dev = {"sp": s, "tp": ct}
    xc_dev = {"sp": s, "tp": xct}

    places, _ = semaphore_places(zn)

    def copy_to(src, dst, dev, kind, i, group):
        return pltpu.make_async_remote_copy(
            src_ref=src, dst_ref=dst, send_sem=send_s.at[GROUPS.index(group)],
            recv_sem=recv_s.at[places[kind] + i], device_id=dev, device_id_type=MESH,
        )

    def send(ref, dev, kind, i, group, dst=None):
        copy_to(ref, ref if dst is None else dst, dev, kind, i, group).start()

    def send_if(condition, ref, dev, kind, i, group, dst=None, wait=None):
        @pl.when(condition)
        def _():
            if wait is not None:
                arrived(ref, wait, i)
            send(ref, dev, kind, i, group, dst)

    def arrived(dst, kind, i):
        with jax.named_scope("wait_" + kind):
            copy_to(dst, dst, c_dev, kind, i, "lat").wait_recv()

    def all_sent(ref, group):
        copy_to(ref, ref, c_dev, "lz", 0, group).wait_send()

    barrier = pltpu.get_barrier_semaphore()
    partners = [to_z(near), to_z(mid), to_z(far), y_dev, x_dev, c_dev, xc_dev]
    for dev in partners:
        pl.semaphore_signal(barrier, inc=1, device_id=dev, device_id_type=MESH)

    def res_rows(i):
        return res_hbm.at[pl.ds(pl.multiple_of((2 * i + c) * share, share), share), :]

    pairs = [
        (key_hbm, key_ref),
        (lat_hbm, lat_ref),
        (gate_hbm, gate_ref),
        (value_hbm, value_ref),
        (q_hbm, q_ref),
        (down_hbm, down_ref),
        (expand_hbm, expand_ref),
        (res_rows(0), res_ref.at[0]),
        (res_rows(1), res_ref.at[1]),
        (gain_hbm, gain_ref),
        (conv_hbm, conv_ref),
        (out_w_hbm, out_w_ref),
    ]
    loads = [pltpu.make_async_copy(src, dst, in_s.at[i]) for i, (src, dst) in enumerate(pairs)]
    for load in loads:
        load.start()

    h = ROPE // 2
    step = lax.broadcasted_iota(jnp.int32, (h, rows), 0).astype(f32) * (-math.log(10000.0) / h)
    spot = (s * rows + lax.broadcasted_iota(jnp.int32, (h, rows), 1)).astype(f32)
    angles = spot * jnp.exp(step)
    cos, sine = jnp.cos(angles), jnp.sin(angles)

    def turn(v):
        a, b = v[:h], v[h:]
        return jnp.concatenate([a * cos - b * sine, b * cos + a * sine], axis=0)

    loads[0].wait()
    turned = turn(key_ref[...].astype(f32))
    key_turned = jnp.concatenate([turned, jnp.zeros_like(turned)], axis=0).T.astype(bf16)[:, :ROPE]
    loads[1].wait()
    for i in range(4):
        for j in range(2):
            first = i * share + j * packed
            lat_all[s, i, :, j * rank : (j + 1) * rank] = lat_ref[first : first + packed, :]
        lat_all[s, i, :, 2 * rank :] = jnp.concatenate(
            [key_turned[i * share : i * share + packed], key_turned[i * share + packed : (i + 1) * share]], axis=1
        )
    with jax.named_scope("barrier"):
        pl.semaphore_wait(barrier, len(partners))

    def lat(zz, yy, q):
        return lat_all.at[2 * zz + yy, q]

    for zz in (far, mid, near):
        send(lat(z, y, t), to_z(zz), "lz", z, "lat")
    send(lat(z, y, t), y_dev, "ly", z, "lat")
    send(lat(z, y, xt), y_dev, "lxy", z, "lat")
    loads[2].wait()
    loads[3].wait()
    for k in range(zn):
        for i in range(2):
            stage[k, i, :, :sub] = gate_ref[i * deep : (i + 1) * deep, k * sub : (k + 1) * sub]
            stage[k, i, :, sub:] = value_ref[i * deep : (i + 1) * deep, k * sub : (k + 1) * sub]
    send(stage.at[near], to_z(near), "wz", 2 * z, "weights", w_full.at[s])
    for zz, i in ((mid, 0), (mid, 1), (far, 0), (far, 1)):
        send(stage.at[zz, i], to_z(zz), "wz", 2 * z + i, "weights", w_full.at[s, i])
    w_full[s] = stage[z]

    for zz in arrivals:
        arrived(lat(zz, y, t), "lz", zz)
        send(lat(zz, y, t), y_dev, "ly", zz, "lat")
        send(lat(zz, y, t), x_dev, "lx", zz, "lat")
        send(lat(zz, y, t), c_dev, "lc", 0, "lat")
    arrived(lat(z, yo, t), "ly", z)
    send(lat(z, yo, t), c_dev, "lc", 0, "lat")
    arrived(lat(z, yo, xt), "lxy", z)
    send(lat(z, yo, xt), c_dev, "lc", 0, "lat")
    for i, zz in enumerate(arrivals):
        arrived(lat(zz, yo, t), "ly", zz)
        if i < 2:
            send(lat(zz, yo, t), x_dev, "lxy", zz, "lat")
        send(lat(zz, yo, t), c_dev, "lc", 0, "lat")
        arrived(lat(zz, y, xt), "lx", zz)
        if i == 2:
            send(lat(zz, y, xt), y_dev, "lxy", zz, "lat")
        send(lat(zz, y, xt), c_dev, "lc", 0, "lat")
    send(w_full.at[s], y_dev, "wy", 0, "weights")

    loads[4].wait()
    rot = NOPE_A + NOPE_B
    q = q_ref[...].astype(f32)
    q_wide = q[:NOPE_A].T.astype(bf16)
    pair = jnp.concatenate([q[NOPE_A:rot], turn(q[rot : rot + ROPE])], axis=0).T.astype(bf16)
    q_narrow, q_wide_t = pair[:, :NOPE_B], pair[:, NOPE_B:]
    turned = turn(q[rot + ROPE :])
    q_narrow_t = jnp.concatenate([turned, jnp.zeros_like(turned)], axis=0).T.astype(bf16)[:, :ROPE]
    loads[5].wait()
    dn_full[s] = down_ref[pl.ds(pl.multiple_of(z * sub, sub), sub), :]
    loads[6].wait()

    for zz in arrivals:
        arrived(lat(zz, yo, xt), "lxy", zz)
        send(lat(zz, yo, xt), c_dev, "lc", 0, "lat")
    arrived(lat_all.at[pl.ds(0, sp - 1), pl.ds(0, 2)], "lc", 0)

    whole = lat_all[...].reshape(sp * 4 * packed, lat_all.shape[3])
    expand_w = expand_ref[...]
    expanded = jnp.concatenate(
        [
            jnp.dot(whole[:, j * rank : (j + 1) * rank], expand_w, preferred_element_type=f32).astype(bf16)
            for j in range(2)
        ],
        axis=0,
    )
    keys_t = whole[:, 2 * rank :]
    empty = jnp.zeros((rows, ROPE), bf16)

    def attend(qc, qt, kc, v, scale):
        dims = (((1,), (1,)), ((), ()))
        turned_scores = [
            lax.dot_general(jnp.concatenate(two, axis=1), keys_t, dims, preferred_element_type=f32)
            for two in ([qt, empty], [empty, qt])
        ]
        scores = (
            lax.dot_general(qc, kc, dims, preferred_element_type=f32) + jnp.concatenate(turned_scores, axis=1)
        ) * scale
        w = jnp.exp(scores - jnp.max(scores, axis=1, keepdims=True))
        total = jnp.sum(w, axis=1, keepdims=True)
        return (jnp.dot(w.astype(bf16), v, preferred_element_type=f32) / total).astype(bf16)

    nb = NOPE_A + VAL_A
    wide = attend(q_wide, q_wide_t, expanded[:, :NOPE_A], expanded[:, NOPE_A:nb], (NOPE_A + ROPE) ** -0.5)
    narrow = attend(
        q_narrow, q_narrow_t, expanded[:, nb : nb + NOPE_B],
        expanded[:, nb + NOPE_B : nb + NOPE_B + VAL_B], (NOPE_B + ROPE) ** -0.5,
    )
    vals = VAL_A + VAL_B
    for i in range(4):
        att_send[i % 2, i // 2, :, :VAL_A] = wide[i * share : (i + 1) * share, :]
        att_send[i % 2, i // 2, :, VAL_A:vals] = narrow[i * share : (i + 1) * share, :]
    send(att_send.at[c], x_dev, "at", 0, "at", att_recv.at[t])
    send(att_send.at[co], xc_dev, "at", 0, "at", att_recv.at[t])
    send(att_send.at[co], c_dev, "at", 0, "at", att_recv.at[t])
    att_recv[t] = att_send[c]

    arrived(w_full.at[2 * near + y], "wz", 2 * near)
    send(w_full.at[2 * near + y], y_dev, "wy", 0, "weights")

    def forward_weights(turn):
        for zz in (mid, far):
            for i in range(2):
                turns = (inner * c, (1 - inner * c) * (1 - i + i * inner), i * (1 - inner))
                if turn == 2 and i == 0:
                    continue

                @pl.when(turns[turn] == 1)
                def _():
                    arrived(w_full.at[2 * zz + y, i], "wz", 2 * zz + i)
                    send(w_full.at[2 * zz + y, i], y_dev, "wy", 0, "weights")

    forward_weights(0)
    for load in loads[7:]:
        load.wait()
    arrived(att_recv.at[pl.ds(0, 3)], "at", 0)

    projected = None
    for i in range(4):
        term = jnp.dot(
            att_recv[i].reshape(2 * share, att_recv.shape[3])[:, :vals],
            out_w_ref[i * vals : (i + 1) * vals, :], preferred_element_type=f32,
        )
        projected = term if projected is None else projected + term
    stream = (res_ref[...].reshape(2 * share, res_ref.shape[2]).astype(f32) + projected).astype(bf16)
    stream_f = stream.astype(f32)
    scaled = stream_f * lax.rsqrt(jnp.mean(stream_f * stream_f, axis=1, keepdims=True) + 1e-06)
    normed = (scaled * gain_ref[...].astype(f32).reshape(1, scaled.shape[1])).astype(bf16)
    piece_rows = share // 2
    for i in range(2):
        for j in range(2):
            first = i * share + j * piece_rows
            nrm[z, 2 * i + c, j] = normed[first : first + piece_rows]
        own_stream[i] = stream[i * share : (i + 1) * share]

    for j in range(2):
        send(nrm.at[z, t, j], to_z(mid), "nz", 2 * z + j, "own")
        send(nrm.at[z, t, j], to_z(near), "nz", 2 * z + j, "own")
    send(nrm.at[z, t], c_dev, "nc", z, "own")
    send(nrm.at[z, xt], c_dev, "nc", z, "own")
    send(dn_full.at[s], y_dev, "dy", z, "down")
    forward_weights(1)

    outer_turns = ((near, 0), (near, 1), (mid, 0), (far, 0), (mid, 1), (far, 1))
    inner_turns = ((mid, 0), (far, 0), (mid, 1), (far, 1), (near, 0), (near, 1))
    turns = [(a + inner * (b - a), i + inner * (j - i)) for (a, i), (b, j) in zip(outer_turns, inner_turns)]

    def from_x(n):
        zz, j = turns[n]
        arrived(nrm.at[zz, xt, j], "nx", 2 * zz + j)
        send(nrm.at[zz, xt, j], c_dev, "nc", zz, "normed")

    def send_down(zz, cond):
        piece = down_ref.at[pl.ds(pl.multiple_of(zz * sub, sub), sub), :]
        if cond is None:
            send(piece, to_z(zz), "dz", z, "down", dn_full.at[s])
        else:
            send_if(cond, piece, to_z(zz), "dz", z, "down", dn_full.at[s])

    for n, (zz, j) in enumerate(turns):
        blk = nrm.at[zz, t, j]
        arrived(blk, "nz", 2 * zz + j)
        if n < 4:
            send_if(inner == 1, blk, to_z(near), "nz", 2 * zz + j, "relay")
        send(blk, x_dev, "nx", 2 * zz + j, "normed")
        send(blk, c_dev, "nc", zz, "normed")
        if n == 1:
            forward_weights(2)
        if n == 3:
            send_down(mid, ((1 - inner) * c) == 1)
        if n > 1:
            from_x(n - 2)
    send_down(near, None)
    send_down(mid, ((1 - inner) * c) == 0)
    send_down(far, None)
    arrived(w_full.at[pl.ds(0, zn)], "wy", 0)
    weights = w_full[...].reshape(sp * 2 * deep, 2 * sub)

    def forward_down(zz):
        arrived(dn_full.at[2 * zz + y], "dz", zz)
        send(dn_full.at[2 * zz + y], y_dev, "dy", zz, "down")

    def mix(zz):
        hbuf[zz] = jnp.dot(
            nrm[zz].reshape(rows, nrm.shape[4]), weights, preferred_element_type=f32
        ).astype(bf16)

    def block_here(zz):
        arrived(nrm.at[zz, pl.ds(0, 2)], "nc", zz)

    columns = (z, near + inner * (mid - near), mid + inner * (near - mid), far)
    block_here(z)
    mix(z)
    for i, zz in enumerate(arrivals):
        if i > 0:
            from_x(len(turns) - 3 + i)
        block_here(zz)
        mix(zz)

    wide_lanes = halo_send.shape[1]
    for k in range(zn):
        g = hbuf[k, :, :wide_lanes].astype(f32)
        halo_send[k : k + 1, :] = g[rows - 1 : rows, :]
        halo_send[zn + k : zn + k + 1, :] = g[0:1, :]
    send(halo_send, y_dev, "h", 0, "h", halo_recv)

    forward_down(columns[1])
    conv_all = conv_ref[...].astype(f32)
    pieces = [conv_all[:, k * sub : (k + 1) * sub] for k in range(zn)]
    taps = pieces[0]
    for k in range(1, zn):
        taps = jnp.where(z == k, pieces[k], taps)
    taps = jnp.concatenate([taps, jnp.zeros((taps.shape[0], wide_lanes - sub), f32)], axis=1)

    def activate(k, first, count, before=None, after=None):
        g = hbuf[k, first : first + count, :wide_lanes].astype(f32)
        row_id = lax.broadcasted_iota(jnp.int32, (count, wide_lanes), 0)
        up, down = pltpu.roll(g, 1, 0), pltpu.roll(g, count - 1, 0)
        if before is not None:
            up = jnp.where(row_id == 0, before, up)
        if after is not None:
            down = jnp.where(row_id == count - 1, after, down)
        mixed = up * taps[0:1] + g * taps[1:2] + down * taps[2:3]
        mixed = mixed[:, :sub]
        v = hbuf[k, first : first + count].astype(f32)[:, sub:]
        return (mixed / (1.0 + jnp.exp(-mixed)) * v).astype(bf16)

    edge = rows // 8
    for k in range(zn):
        abuf[k] = activate(k, 0, rows)
    arrived(halo_recv, "h", 0)
    forward_down(columns[2])
    nothing = jnp.zeros((1, wide_lanes), f32)
    for k in range(zn):
        before_low = halo_recv[k - 1 : k, :] if k > 0 else nothing
        before = jnp.where(y == 0, before_low, halo_recv[k : k + 1, :])
        after_high = halo_recv[zn + k + 1 : zn + k + 2, :] if k < zn - 1 else nothing
        after = jnp.where(y == 0, halo_recv[zn + k : zn + k + 1, :], after_high)
        abuf[k, :edge] = activate(k, 0, 2 * edge, before=before)[:edge]
        abuf[k, rows - edge :] = activate(k, rows - 2 * edge, 2 * edge, after=after)[edge:]

    order = (far, mid, near, z)
    depth = dn_full.shape[2]
    two = 2 * depth

    def multiply(g):
        zz = columns[g]
        arrived(dn_full.at[2 * zz + yo], "dy", zz)
        down = jnp.concatenate([dn_full[2 * zz], dn_full[2 * zz + 1]], axis=1)
        for d, to in enumerate(order):
            p = jnp.dot(abuf[to], down, preferred_element_type=f32)
            part[g, d] = p.reshape(4, share, two)
            for i in range(2):
                c_send[g, d, i] = part[g, d, 2 * i + co].astype(bf16)
            if d % 2 == 1:
                ready = pl.ds(d - 1, 2)
                send(c_send.at[g, ready], c_dev, "pc", 2 * g + d // 2, "pc", c_recv.at[g, ready])

    def over_x(g, turns):
        for d in turns:
            if d % 2 == 0:
                arrived(c_recv.at[g, pl.ds(d, 2)], "pc", 2 * g + d // 2)
            x_send[g, d] = (part[g, d, xt] + c_recv[g, d, xo].astype(f32)).astype(bf16)
            send(x_send.at[g, d], x_dev, "px", g * zn + d, "px", x_recv.at[g, d])
            keep[g, d] = part[g, d, t] + c_recv[g, d, x].astype(f32)

    def over_z(g, turns):
        for d in turns:
            arrived(x_recv.at[g, d], "px", g * zn + d)
            both = keep[g, d] + x_recv[g, d].astype(f32)
            if d < zn - 1:
                z_send[g, d] = both.astype(bf16)
                send(z_send.at[g, d], to_z(order[d]), "pz", 0, "pz", z_recv.at[columns[g], z])
            else:
                keep[g, d] = both

    away, stay = range(zn - 1), range(zn - 1, zn)
    for g in range(zn):
        multiply(g)
        if g == 0:
            forward_down(far)
        over_x(g, away)
        if g > 0:
            over_z(g - 1, away)
    for g in range(zn):
        over_x(g, stay)
    over_z(zn - 1, away)
    for g in range(zn):
        over_z(g, stay)
    leaving = []
    arrived(z_recv.at[:, pl.ds(0, zn - 1)], "pz", 0)
    for g, zz in enumerate(columns):
        total = keep[g, zn - 1]
        for frm in arrivals:
            total += z_recv[zz, frm].astype(f32)
        where = pl.ds(pl.multiple_of(zz * two, two), two)
        result[:, where] = (own_stream[x, :, where].astype(f32) + total).astype(bf16)
        leave = pltpu.make_async_copy(result.at[:, where], out_ref.at[:, where], in_s.at[len(pairs) + g])
        leave.start()
        leaving.append(leave)
    all_sent(lat_all.at[pl.ds(0, sp - 1)], "lat")
    all_sent(w_full.at[pl.ds(0, sp - 1)], "weights")
    all_sent(dn_full.at[pl.ds(0, sp - 1)], "down")
    all_sent(nrm.at[0], "own")
    all_sent(nrm.at[pl.ds(0, zn - 1), pl.ds(0, 3)], "normed")
    all_sent(att_recv.at[pl.ds(0, 3)], "at")
    all_sent(halo_send, "h")
    all_sent(c_send, "pc")
    all_sent(x_send, "px")
    all_sent(z_send.at[:, pl.ds(0, zn - 1)], "pz")

    @pl.when(inner == 1)
    def _():
        all_sent(nrm.at[0, pl.ds(0, 2)], "relay")

    with jax.named_scope("leave"):
        for leave in leaving:
            leave.wait()


def kernel_body(zn, *args):
    (queries, latents, shared_key, expand_weight, residual, out_weight, norm_gain,
     gate_weight, value_weight, conv_weight, down_weight) = args
    rows, width = residual.shape
    sub = down_weight.shape[0] // zn
    share = rows // 4
    d_own = gate_weight.shape[0]
    group = 2 * down_weight.shape[1]
    bf16, f32 = jnp.bfloat16, jnp.float32
    vals = VAL_A + VAL_B
    lanes = -(-vals // 128) * 128
    halo_lanes = -(-sub // 128) * 128
    V, DMA = pltpu.VMEM, pltpu.SemaphoreType.DMA
    return pl.pallas_call(
        functools.partial(layer_kernel, zn),
        out_shape=jax.ShapeDtypeStruct((share, width), bf16),
        in_specs=[pl.BlockSpec(memory_space=pl.ANY)] * 11,
        out_specs=pl.BlockSpec(memory_space=pl.ANY),
        scratch_shapes=[
            V((queries.shape[1], rows), bf16),
            V(latents.shape, bf16),
            V((ROPE, rows), bf16),
            V(conv_weight.shape, bf16),
            V((width,), bf16),
            V(expand_weight.shape, bf16),
            V((2, share, width), bf16),
            V(out_weight.shape, bf16),
            V(gate_weight.shape, bf16),
            V(value_weight.shape, bf16),
            V(down_weight.shape, bf16),
            V((2 * zn, 4, share // 2, 2 * latents.shape[1] + 2 * ROPE), bf16),
            V((2, 2, share, lanes), bf16),
            V((4, 2, share, lanes), bf16),
            V((2, share, width), bf16),
            V((zn, 4, 2, share // 2, width), bf16),
            V((zn, 2, d_own // 2, 2 * sub), bf16),
            V((2 * zn, 2, d_own // 2, 2 * sub), bf16),
            V((2 * zn, sub, down_weight.shape[1]), bf16),
            V((zn, rows, 2 * sub), bf16),
            V((zn, rows, sub), bf16),
            V((2 * zn, halo_lanes), f32),
            V((2 * zn, halo_lanes), f32),
            V((zn, zn, 4, share, group), f32),
            V((zn, zn, 2, share, group), bf16),
            V((zn, zn, 2, share, group), bf16),
            V((zn, zn, share, group), f32),
            V((zn, zn, share, group), bf16),
            V((zn, zn, share, group), bf16),
            V((zn, zn, share, group), bf16),
            V((zn, zn, share, group), bf16),
            V((share, width), bf16),
            DMA((12 + zn,)),
            DMA((len(GROUPS),)),
            DMA((semaphore_places(zn)[1],)),
        ],
        compiler_params=pltpu.CompilerParams(collective_id=0, has_side_effects=True),
    )(queries.T, latents, shared_key.T, conv_weight, norm_gain, expand_weight, residual,
      out_weight, gate_weight, value_weight, down_weight)


def pick(*args):
    zn = lax.axis_size("sp") // 2
    hidden = args[10].shape[0]
    sub = hidden // zn
    fits = (
        lax.axis_size("sp") == 8
        and lax.axis_size("tp") == 4
        and hidden % zn == 0
        and sub % 64 == 0
        and args[7].shape[0] % 128 == 0
        and args[0].shape[0] % 128 == 0
        and args[4].shape[1] % args[0].shape[0] == 0
        and args[9].shape[0] == 3
    )
    return kernel_body(zn, *args) if fits else body(*args)


def solution(mesh):
    in_specs = (
        P("sp", "tp"),
        P("sp", None),
        P("sp", None),
        P(None, "tp"),
        P("sp", None),
        P(),
        P(),
        P("sp", "tp"),
        P("sp", "tp"),
        P(None, "tp"),
        P("tp", "sp"),
    )
    out_specs = P(("sp", "tp"), None)
    return jax.shard_map(pick, mesh=mesh, in_specs=in_specs, out_specs=out_specs, check_vma=False)
```

```python
import functools
import math

import jax
import jax.numpy as jnp
from jax import lax
from jax.experimental import pallas as pl
from jax.experimental.pallas import tpu as pltpu
from jax.sharding import PartitionSpec as P

NOPE_A = 128
VAL_A = 128
NOPE_B = 64
VAL_B = 64
ROPE = 64


def padded_2(block, sides, width):
    for axis, dim in sides:
        count = lax.axis_size(axis)
        forward = [(i, i + 1) for i in range(count - 1)]
        backward = [(target, source) for source, target in forward]
        low = lax.ppermute(
            lax.slice_in_dim(block, block.shape[dim] - width, None, axis=dim), axis, forward
        )
        high = lax.ppermute(lax.slice_in_dim(block, 0, width, axis=dim), axis, backward)
        block = jnp.concatenate([low, block, high], axis=dim)
    return block


def tables(positions, width):
    half_width = width // 2
    frequency = 10000.0 ** (-jnp.arange(half_width, dtype=jnp.float32) / half_width)
    angles = positions.astype(jnp.float32)[:, None] * frequency[None, :]
    return (jnp.cos(angles), jnp.sin(angles))


def rotate(vectors, cos_table, sine_table):
    half_width = vectors.shape[-1] // 2
    first_half = vectors[:, :half_width].astype(jnp.float32)
    second_half = vectors[:, half_width:].astype(jnp.float32)
    turned = jnp.concatenate(
        [
            first_half * cos_table - second_half * sine_table,
            second_half * cos_table + first_half * sine_table,
        ],
        axis=1,
    )
    return turned.astype(jnp.bfloat16)


def normalize(stream, norm_gain):
    stream_f = stream.astype(jnp.float32)
    scaled = stream_f * lax.rsqrt(jnp.mean(stream_f * stream_f, axis=1, keepdims=True) + 1e-06)
    return (scaled * norm_gain.astype(jnp.float32)).astype(jnp.bfloat16)


def update(running, q_content, q_turned, k_content, k_turned, values, score_scale):
    row_max, row_sum, weighted = running
    scores = (
        jnp.einsum("qd,kd->qk", q_content, k_content, preferred_element_type=jnp.float32)
        + jnp.einsum("qd,kd->qk", q_turned, k_turned, preferred_element_type=jnp.float32)
    ) * score_scale
    new_max = jnp.maximum(row_max, jnp.max(scores, axis=1))
    weights = jnp.exp(scores - new_max[:, None])
    row_sum = jnp.sum(weights, axis=1)
    weighted = jnp.dot(weights.astype(jnp.bfloat16), values, preferred_element_type=jnp.float32)
    return (new_max, row_sum, weighted)


def body(
    queries,
    latents,
    shared_key,
    expand_weight,
    residual,
    out_weight,
    norm_gain,
    gate_weight,
    value_weight,
    conv_weight,
    down_weight,
):
    tok_rows = queries.shape[0]
    q_width = NOPE_A + NOPE_B + 2 * ROPE
    kv_width = NOPE_A + VAL_A + NOPE_B + VAL_B
    positions = lax.axis_index("sp") * tok_rows + jnp.arange(tok_rows, dtype=jnp.int32)
    cos_table, sine_table = tables(positions, ROPE)
    key_turned = rotate(shared_key, cos_table, sine_table)
    scale_wide = (NOPE_A + ROPE) ** (-0.5)
    scale_narrow = (NOPE_B + ROPE) ** (-0.5)
    initial = []
    pair_index = 0
    q_base = pair_index * q_width
    rotary_base = q_base + NOPE_A + NOPE_B
    wide_content = queries[:, q_base : q_base + NOPE_A]
    narrow_content = queries[:, q_base + NOPE_A : rotary_base]
    wide_turned = rotate(queries[:, rotary_base : rotary_base + ROPE], cos_table, sine_table)
    narrow_turned = rotate(
        queries[:, rotary_base + ROPE : rotary_base + 2 * ROPE], cos_table, sine_table
    )
    query_parts = [(wide_content, wide_turned, narrow_content, narrow_turned)]
    lowest = jnp.full((tok_rows,), -1e30, jnp.float32)
    empty_sum = jnp.zeros((tok_rows,), jnp.float32)
    initial += [
        lowest,
        empty_sum,
        jnp.zeros((tok_rows, VAL_A), jnp.float32),
        lowest,
        empty_sum,
        jnp.zeros((tok_rows, VAL_B), jnp.float32),
    ]
    initial = tuple(initial)
    pieces = (
        lax.all_gather(latents, "sp", axis=0, tiled=True),
        lax.all_gather(key_turned, "sp", axis=0, tiled=True),
    )
    expanded = jnp.dot(pieces[0], expand_weight, preferred_element_type=jnp.float32).astype(
        jnp.bfloat16
    )
    turned_keys = pieces[1]
    result = []
    pair_index = 0
    wide_content, wide_turned, narrow_content, narrow_turned = query_parts[pair_index]
    kv_base = pair_index * kv_width
    narrow_base = kv_base + NOPE_A + VAL_A
    wide_keys = expanded[:, kv_base : kv_base + NOPE_A]
    wide_values = expanded[:, kv_base + NOPE_A : narrow_base]
    narrow_keys = expanded[:, narrow_base : narrow_base + NOPE_B]
    narrow_values = expanded[:, narrow_base + NOPE_B : narrow_base + NOPE_B + VAL_B]
    absorb_offset = 6 * pair_index
    result += list(
        update(
            initial[absorb_offset : absorb_offset + 3],
            wide_content,
            wide_turned,
            wide_keys,
            turned_keys,
            wide_values,
            scale_wide,
        )
    )
    result += list(
        update(
            initial[absorb_offset + 3 : absorb_offset + 6],
            narrow_content,
            narrow_turned,
            narrow_keys,
            turned_keys,
            narrow_values,
            scale_narrow,
        )
    )
    running = tuple(result)
    outputs = []
    pair_index = 0
    for group_index in range(2):
        offset = 6 * pair_index + 3 * group_index
        outputs.append((running[offset + 2] / running[offset + 1][:, None]).astype(jnp.bfloat16))
    attended = jnp.concatenate(outputs, axis=1)
    share = tok_rows // lax.axis_size("tp")
    tp_index = lax.axis_index("tp")
    all_heads = lax.all_gather(attended, "tp", axis=1, tiled=True)
    projected = jnp.dot(all_heads, out_weight, preferred_element_type=jnp.float32)
    stream = (residual.astype(jnp.float32) + projected).astype(jnp.bfloat16)
    normed = normalize(stream, norm_gain)
    stream_own = lax.dynamic_slice_in_dim(stream, tp_index * share, share, 0)
    pieces = (
        lax.all_gather(gate_weight, "sp", axis=0, tiled=True),
        lax.all_gather(value_weight, "sp", axis=0, tiled=True),
    )
    gate_sum = jnp.dot(normed, pieces[0], preferred_element_type=jnp.float32)
    value_sum = jnp.dot(normed, pieces[1], preferred_element_type=jnp.float32)
    gate_pre = gate_sum.astype(jnp.bfloat16)
    value_pre = value_sum.astype(jnp.bfloat16)
    reach = conv_weight.shape[0] // 2
    padded = padded_2(gate_pre, (("sp", 0),), reach)
    mixed_gate = jnp.zeros(gate_pre.shape, jnp.float32)
    for tap in range(conv_weight.shape[0]):
        mixed_gate = mixed_gate + padded[tap : tap + tok_rows].astype(jnp.float32) * conv_weight[
            tap
        ].astype(jnp.float32)
    active = (jax.nn.silu(mixed_gate) * value_pre.astype(jnp.float32)).astype(jnp.bfloat16)
    partial_rows = jnp.dot(
        active,
        lax.all_gather(down_weight, "sp", axis=1, tiled=True),
        preferred_element_type=jnp.float32,
    )
    summed = lax.psum_scatter(
        partial_rows.astype(jnp.bfloat16), "tp", scatter_dimension=0, tiled=True
    ).astype(jnp.float32)
    return (stream_own.astype(jnp.float32) + summed).astype(jnp.bfloat16)


MESH = pl.DeviceIdType.MESH
SINGLE = ("lc", "lco", "wy", "at", "an", "h", "pz")
PER_Z = ("lz", "ly", "lx", "lxy", "dz", "dy", "nc")
PER_HALF = ("wz", "nz", "nx", "pc")
GROUPS = ("lat", "lat_o", "weights", "down", "own", "relay", "normed", "at", "an", "h", "pc", "px", "pz")


def semaphore_places(zn):
    places, count = {}, 0
    for kinds, width in ((SINGLE, 1), (PER_Z, zn), (PER_HALF, 2 * zn), (("px",), zn * zn)):
        for kind in kinds:
            places[kind] = count
            count += width
    return places, count


def layer_kernel(
    zn,
    q_hbm,
    lat_hbm,
    key_hbm,
    conv_hbm,
    gain_hbm,
    expand_hbm,
    res_hbm,
    out_w_hbm,
    gate_hbm,
    value_hbm,
    down_hbm,
    out_ref,
    q_ref,
    lat_ref,
    key_ref,
    conv_ref,
    gain_ref,
    expand_ref,
    res_ref,
    out_w_ref,
    gate_ref,
    value_ref,
    down_ref,
    lat_all,
    att_send,
    att_recv,
    nar_send,
    nar_recv,
    own_stream,
    nrm,
    stage,
    w_full,
    dn_full,
    hbuf,
    abuf,
    halo_send,
    halo_recv,
    part,
    c_send,
    c_recv,
    keep,
    x_send,
    x_recv,
    z_send,
    z_recv,
    result,
    in_s,
    send_s,
    recv_s,
):
    f32, bf16 = jnp.float32, jnp.bfloat16
    s, t = lax.axis_index("sp"), lax.axis_index("tp")
    z, y = s // 2, s % 2
    x, c = t // 2, t % 2
    yo, xo, co = 1 - y, 1 - x, 1 - c
    xt, ct, xct = 2 * xo + c, 2 * x + co, 2 * xo + co
    rows = lat_ref.shape[0]
    share = rows // 4
    packed = share // 2
    rank = lat_ref.shape[1]
    sub = down_ref.shape[0] // zn
    sp = 2 * zn
    deep = gate_ref.shape[0] // 2

    inner = ((z + 1) // 2) % 2
    near = z + 1 - 2 * (z % 2)
    mid = (z + 2) % zn + inner * (zn - 1 - z - (z + 2) % zn)
    far = zn - 1 - z + inner * ((z + 2) % zn - (zn - 1 - z))
    arrivals = (near + inner * (mid - near), mid + inner * (far - mid), far + inner * (near - far))

    def to_z(zz):
        return {"sp": 2 * zz + y, "tp": t}

    y_dev = {"sp": 2 * z + yo, "tp": t}
    x_dev = {"sp": s, "tp": xt}
    c_dev = {"sp": s, "tp": ct}
    xc_dev = {"sp": s, "tp": xct}

    places, _ = semaphore_places(zn)

    def copy_to(src, dst, dev, kind, i, group):
        return pltpu.make_async_remote_copy(
            src_ref=src, dst_ref=dst, send_sem=send_s.at[GROUPS.index(group)],
            recv_sem=recv_s.at[places[kind] + i], device_id=dev, device_id_type=MESH,
        )

    def send(ref, dev, kind, i, group, dst=None):
        copy_to(ref, ref if dst is None else dst, dev, kind, i, group).start()

    def send_if(condition, ref, dev, kind, i, group, dst=None, wait=None):
        @pl.when(condition)
        def _():
            if wait is not None:
                arrived(ref, wait, i)
            send(ref, dev, kind, i, group, dst)

    def arrived(dst, kind, i):
        with jax.named_scope("wait_" + kind):
            copy_to(dst, dst, c_dev, kind, i, "lat").wait_recv()

    def all_sent(ref, group):
        copy_to(ref, ref, c_dev, "lz", 0, group).wait_send()

    barrier = pltpu.get_barrier_semaphore()
    partners = [to_z(near), to_z(mid), to_z(far), y_dev, x_dev, c_dev, xc_dev]
    for dev in partners:
        pl.semaphore_signal(barrier, inc=1, device_id=dev, device_id_type=MESH)

    def res_rows(i):
        return res_hbm.at[pl.ds(pl.multiple_of((2 * i + c) * share, share), share), :]

    pairs = [
        (key_hbm, key_ref),
        (lat_hbm, lat_ref),
        (gate_hbm, gate_ref),
        (value_hbm, value_ref),
        (q_hbm, q_ref),
        (down_hbm, down_ref),
        (expand_hbm, expand_ref),
        (res_rows(0), res_ref.at[0]),
        (res_rows(1), res_ref.at[1]),
        (gain_hbm, gain_ref),
        (conv_hbm, conv_ref),
        (out_w_hbm, out_w_ref),
    ]
    loads = [pltpu.make_async_copy(src, dst, in_s.at[i]) for i, (src, dst) in enumerate(pairs)]
    for load in loads:
        load.start()

    h = ROPE // 2
    step = lax.broadcasted_iota(jnp.int32, (h, rows), 0).astype(f32) * (-math.log(10000.0) / h)
    spot = (s * rows + lax.broadcasted_iota(jnp.int32, (h, rows), 1)).astype(f32)
    angles = spot * jnp.exp(step)
    cos, sine = jnp.cos(angles), jnp.sin(angles)

    def turn(v):
        a, b = v[:h], v[h:]
        return jnp.concatenate([a * cos - b * sine, b * cos + a * sine], axis=0)

    loads[0].wait()
    turned = turn(key_ref[...].astype(f32))
    key_turned = jnp.concatenate([turned, jnp.zeros_like(turned)], axis=0).T.astype(bf16)[:, :ROPE]
    loads[1].wait()
    for i in range(4):
        for j in range(2):
            first = i * share + j * packed
            lat_all[z, y, i, :, j * rank : (j + 1) * rank] = lat_ref[first : first + packed, :]
        lat_all[z, y, i, :, 2 * rank :] = jnp.concatenate(
            [key_turned[i * share : i * share + packed], key_turned[i * share + packed : (i + 1) * share]], axis=1
        )
    with jax.named_scope("barrier"):
        pl.semaphore_wait(barrier, len(partners))

    def lat(zz, yy, q):
        return lat_all.at[zz, yy, q]

    for zz in (far, mid, near):
        send(lat(z, y, t), to_z(zz), "lz", z, "lat")
    send(lat(z, y, t), y_dev, "ly", z, "lat_o")
    send(lat(z, y, xt), y_dev, "lxy", z, "lat_o")
    loads[2].wait()
    loads[3].wait()
    for k in range(zn):
        for i in range(2):
            stage[k, i, :, :sub] = gate_ref[i * deep : (i + 1) * deep, k * sub : (k + 1) * sub]
            stage[k, i, :, sub:] = value_ref[i * deep : (i + 1) * deep, k * sub : (k + 1) * sub]
    send(stage.at[near], to_z(near), "wz", 2 * z, "weights", w_full.at[s])
    for zz, i in ((mid, 0), (mid, 1), (far, 0), (far, 1)):
        send(stage.at[zz, i], to_z(zz), "wz", 2 * z + i, "weights", w_full.at[s, i])
    w_full[s] = stage[z]

    for zz in arrivals:
        arrived(lat(zz, y, t), "lz", zz)
        send(lat(zz, y, t), y_dev, "ly", zz, "lat_o")
        send(lat(zz, y, t), x_dev, "lx", zz, "lat")
        send(lat(zz, y, t), c_dev, "lc", 0, "lat")
    arrived(lat(z, yo, t), "ly", z)
    send(lat(z, yo, t), c_dev, "lco", 0, "lat_o")
    arrived(lat(z, yo, xt), "lxy", z)
    send(lat(z, yo, xt), c_dev, "lco", 0, "lat_o")
    for i, zz in enumerate(arrivals):
        arrived(lat(zz, yo, t), "ly", zz)
        if i < 2:
            send(lat(zz, yo, t), x_dev, "lxy", zz, "lat_o")
        send(lat(zz, yo, t), c_dev, "lco", 0, "lat_o")
        arrived(lat(zz, y, xt), "lx", zz)
        if i == 2:
            send(lat(zz, y, xt), y_dev, "lxy", zz, "lat_o")
        send(lat(zz, y, xt), c_dev, "lc", 0, "lat")
    send(w_full.at[s], y_dev, "wy", 0, "weights")

    loads[4].wait()
    rot = NOPE_A + NOPE_B
    q = q_ref[...].astype(f32)
    q_wide = q[:NOPE_A].T.astype(bf16)
    pair = jnp.concatenate([q[NOPE_A:rot], turn(q[rot : rot + ROPE])], axis=0).T.astype(bf16)
    q_narrow, q_wide_t = pair[:, :NOPE_B], pair[:, NOPE_B:]
    turned = turn(q[rot + ROPE :])
    q_narrow_t = jnp.concatenate([turned, jnp.zeros_like(turned)], axis=0).T.astype(bf16)[:, :ROPE]
    loads[5].wait()
    dn_full[s] = down_ref[pl.ds(pl.multiple_of(z * sub, sub), sub), :]
    loads[6].wait()

    def pass_far(zz):
        arrived(lat(zz, yo, xt), "lxy", zz)
        send(lat(zz, yo, xt), c_dev, "lco", 0, "lat_o")

    expand_w = expand_ref[...]
    empty = jnp.zeros((rows, ROPE), bf16)
    nb = NOPE_A + VAL_A
    dims = (((1,), (1,)), ((), ()))

    def score(qc, qt, kc, keys_t, scale):
        turned_scores = [
            lax.dot_general(jnp.concatenate(two, axis=1), keys_t, dims, preferred_element_type=f32)
            for two in ([qt, empty], [empty, qt])
        ]
        return (
            lax.dot_general(qc, kc, dims, preferred_element_type=f32) + jnp.concatenate(turned_scores, axis=1)
        ) * scale

    def scored(yy):
        whole = lat_all[:, yy].reshape(zn * 4 * packed, lat_all.shape[4])
        expanded = jnp.concatenate(
            [
                jnp.dot(whole[:, j * rank : (j + 1) * rank], expand_w, preferred_element_type=f32).astype(bf16)
                for j in range(2)
            ],
            axis=0,
        )
        keys_t = whole[:, 2 * rank :]
        return (
            score(q_wide, q_wide_t, expanded[:, :NOPE_A], keys_t, (NOPE_A + ROPE) ** -0.5),
            expanded[:, NOPE_A:nb],
            score(q_narrow, q_narrow_t, expanded[:, nb : nb + NOPE_B], keys_t, (NOPE_B + ROPE) ** -0.5),
            expanded[:, nb + NOPE_B : nb + NOPE_B + VAL_B],
        )

    pass_far(arrivals[0])

    @pl.when(c == 1)
    def _():
        pass_far(arrivals[1])
        pass_far(arrivals[2])

    arrived(lat_all.at[pl.ds(0, zn - 1), 0, pl.ds(0, 2)], "lc", 0)
    here = scored(y)

    @pl.when(c == 0)
    def _():
        pass_far(arrivals[1])
        pass_far(arrivals[2])

    arrived(lat_all.at[:, 0, pl.ds(0, 2)], "lco", 0)
    there = scored(yo)

    def attend(head):
        scores = jnp.concatenate([here[2 * head], there[2 * head]], axis=1)
        v = jnp.concatenate([here[2 * head + 1], there[2 * head + 1]], axis=0)
        w = jnp.exp(scores - jnp.max(scores, axis=1, keepdims=True))
        total = jnp.sum(w, axis=1, keepdims=True)
        return (jnp.dot(w.astype(bf16), v, preferred_element_type=f32) / total).astype(bf16)

    def to_heads(sent, received, kind):
        send(sent.at[c], x_dev, kind, 0, kind, received.at[t])
        send(sent.at[co], xc_dev, kind, 0, kind, received.at[t])
        send(sent.at[co], c_dev, kind, 0, kind, received.at[t])
        received[t] = sent[c]

    vals = VAL_A + VAL_B
    wide = attend(0)
    for i in range(4):
        att_send[i % 2, i // 2] = wide[i * share : (i + 1) * share, :]
    to_heads(att_send, att_recv, "at")
    narrow = attend(1)
    for i in range(4):
        part_rows = narrow[i * share : (i + 1) * share, :]
        nar_send[i % 2, i // 2] = jnp.concatenate([part_rows[:packed], part_rows[packed:]], axis=1)
    to_heads(nar_send, nar_recv, "an")

    arrived(w_full.at[2 * near + y], "wz", 2 * near)
    send(w_full.at[2 * near + y], y_dev, "wy", 0, "weights")

    def forward_weights(turn):
        for zz in (mid, far):
            for i in range(2):
                turns = (inner * c, (1 - inner * c) * (1 - i + i * inner), i * (1 - inner))
                if turn == 2 and i == 0:
                    continue

                @pl.when(turns[turn] == 1)
                def _():
                    arrived(w_full.at[2 * zz + y, i], "wz", 2 * zz + i)
                    send(w_full.at[2 * zz + y, i], y_dev, "wy", 0, "weights")

    forward_weights(0)
    for load in loads[7:]:
        load.wait()
    arrived(att_recv.at[pl.ds(0, 3)], "at", 0)
    arrived(nar_recv.at[pl.ds(0, 3)], "an", 0)

    projected = None
    for i in range(4):
        narrow = [nar_recv[i, j, :, k * VAL_B : (k + 1) * VAL_B] for j in range(2) for k in range(2)]
        term = jnp.dot(
            jnp.concatenate([att_recv[i].reshape(2 * share, VAL_A), jnp.concatenate(narrow, axis=0)], axis=1),
            out_w_ref[i * vals : (i + 1) * vals, :], preferred_element_type=f32,
        )
        projected = term if projected is None else projected + term
    stream = (res_ref[...].reshape(2 * share, res_ref.shape[2]).astype(f32) + projected).astype(bf16)
    stream_f = stream.astype(f32)
    scaled = stream_f * lax.rsqrt(jnp.mean(stream_f * stream_f, axis=1, keepdims=True) + 1e-06)
    normed = (scaled * gain_ref[...].astype(f32).reshape(1, scaled.shape[1])).astype(bf16)
    piece_rows = share // 2
    for i in range(2):
        for j in range(2):
            first = i * share + j * piece_rows
            nrm[z, 2 * i + c, j] = normed[first : first + piece_rows]
        own_stream[i] = stream[i * share : (i + 1) * share]

    for j in range(2):
        send(nrm.at[z, t, j], to_z(mid), "nz", 2 * z + j, "own")
        send(nrm.at[z, t, j], to_z(near), "nz", 2 * z + j, "own")
    send_if(inner == 1, nrm.at[z, t, 0], to_z(far), "nz", 2 * z + 0, "relay")
    send(nrm.at[z, t], c_dev, "nc", z, "own")
    send(nrm.at[z, xt], c_dev, "nc", z, "own")
    send(dn_full.at[s], y_dev, "dy", z, "down")
    forward_weights(1)

    outer_turns = ((near, 0), (near, 1), (mid, 0), (far, 0), (mid, 1), (far, 1))
    inner_turns = ((mid, 0), (far, 0), (mid, 1), (far, 1), (near, 0), (near, 1))
    turns = [(a + inner * (b - a), i + inner * (j - i)) for (a, i), (b, j) in zip(outer_turns, inner_turns)]

    def from_x(n):
        zz, j = turns[n]
        arrived(nrm.at[zz, xt, j], "nx", 2 * zz + j)
        send(nrm.at[zz, xt, j], c_dev, "nc", zz, "normed")

    def send_down(zz, cond):
        piece = down_ref.at[pl.ds(pl.multiple_of(zz * sub, sub), sub), :]
        if cond is None:
            send(piece, to_z(zz), "dz", z, "down", dn_full.at[s])
        else:
            send_if(cond, piece, to_z(zz), "dz", z, "down", dn_full.at[s])

    for n, (zz, j) in enumerate(turns):
        blk = nrm.at[zz, t, j]
        arrived(blk, "nz", 2 * zz + j)
        if 0 < n < 4:
            send_if(inner == 1, blk, to_z(near), "nz", 2 * zz + j, "relay")
        send(blk, x_dev, "nx", 2 * zz + j, "normed")
        send(blk, c_dev, "nc", zz, "normed")
        if n == 1:
            forward_weights(2)
        if n == 2:
            send_down(mid, ((1 - inner) * c) == 1)
        if n > 1:
            from_x(n - 2)
    send_down(near, None)
    send_down(mid, ((1 - inner) * c) == 0)
    send_down(far, None)
    arrived(w_full.at[pl.ds(0, zn)], "wy", 0)
    weights = w_full[...].reshape(sp * 2 * deep, 2 * sub)

    def forward_down(zz):
        arrived(dn_full.at[2 * zz + y], "dz", zz)
        send(dn_full.at[2 * zz + y], y_dev, "dy", zz, "down")

    def mix(zz):
        hbuf[zz] = jnp.dot(
            nrm[zz].reshape(rows, nrm.shape[4]), weights, preferred_element_type=f32
        ).astype(bf16)

    def block_here(zz):
        arrived(nrm.at[zz, pl.ds(0, 2)], "nc", zz)

    columns = (z, near + inner * (mid - near), mid + inner * (near - mid), far)
    block_here(z)
    mix(z)
    for i, zz in enumerate(arrivals):
        if i > 0:
            from_x(len(turns) - 3 + i)
        block_here(zz)
        mix(zz)

    wide_lanes = halo_send.shape[1]
    for k in range(zn):
        g = hbuf[k, :, :wide_lanes].astype(f32)
        halo_send[k : k + 1, :] = g[rows - 1 : rows, :]
        halo_send[zn + k : zn + k + 1, :] = g[0:1, :]
    send(halo_send, y_dev, "h", 0, "h", halo_recv)

    forward_down(columns[1])
    conv_all = conv_ref[...].astype(f32)
    pieces = [conv_all[:, k * sub : (k + 1) * sub] for k in range(zn)]
    taps = pieces[0]
    for k in range(1, zn):
        taps = jnp.where(z == k, pieces[k], taps)
    taps = jnp.concatenate([taps, jnp.zeros((taps.shape[0], wide_lanes - sub), f32)], axis=1)

    def activate(k, first, count, before=None, after=None):
        g = hbuf[k, first : first + count, :wide_lanes].astype(f32)
        row_id = lax.broadcasted_iota(jnp.int32, (count, wide_lanes), 0)
        up, down = pltpu.roll(g, 1, 0), pltpu.roll(g, count - 1, 0)
        if before is not None:
            up = jnp.where(row_id == 0, before, up)
        if after is not None:
            down = jnp.where(row_id == count - 1, after, down)
        mixed = up * taps[0:1] + g * taps[1:2] + down * taps[2:3]
        mixed = mixed[:, :sub]
        v = hbuf[k, first : first + count].astype(f32)[:, sub:]
        return (mixed / (1.0 + jnp.exp(-mixed)) * v).astype(bf16)

    edge = rows // 8
    for k in range(zn):
        abuf[k] = activate(k, 0, rows)
    arrived(halo_recv, "h", 0)
    forward_down(columns[2])
    nothing = jnp.zeros((1, wide_lanes), f32)
    for k in range(zn):
        before_low = halo_recv[k - 1 : k, :] if k > 0 else nothing
        before = jnp.where(y == 0, before_low, halo_recv[k : k + 1, :])
        after_high = halo_recv[zn + k + 1 : zn + k + 2, :] if k < zn - 1 else nothing
        after = jnp.where(y == 0, halo_recv[zn + k : zn + k + 1, :], after_high)
        abuf[k, :edge] = activate(k, 0, 2 * edge, before=before)[:edge]
        abuf[k, rows - edge :] = activate(k, rows - 2 * edge, 2 * edge, after=after)[edge:]

    order = (far, mid, near, z)
    depth = dn_full.shape[2]
    two = 2 * depth

    def multiply(g):
        zz = columns[g]
        arrived(dn_full.at[2 * zz + yo], "dy", zz)
        down = jnp.concatenate([dn_full[2 * zz], dn_full[2 * zz + 1]], axis=1)
        for d, to in enumerate(order):
            p = jnp.dot(abuf[to], down, preferred_element_type=f32)
            part[g, d] = p.reshape(4, share, two)
            for i in range(2):
                c_send[g, d, i] = part[g, d, 2 * i + co].astype(bf16)
            if d % 2 == 1:
                ready = pl.ds(d - 1, 2)
                send(c_send.at[g, ready], c_dev, "pc", 2 * g + d // 2, "pc", c_recv.at[g, ready])

    def over_x(g, turns):
        for d in turns:
            if d % 2 == 0:
                arrived(c_recv.at[g, pl.ds(d, 2)], "pc", 2 * g + d // 2)
            x_send[g, d] = (part[g, d, xt] + c_recv[g, d, xo].astype(f32)).astype(bf16)
            send(x_send.at[g, d], x_dev, "px", g * zn + d, "px", x_recv.at[g, d])
            keep[g, d] = part[g, d, t] + c_recv[g, d, x].astype(f32)

    def over_z(g, turns):
        for d in turns:
            arrived(x_recv.at[g, d], "px", g * zn + d)
            both = keep[g, d] + x_recv[g, d].astype(f32)
            if d < zn - 1:
                z_send[g, d] = both.astype(bf16)
                send(z_send.at[g, d], to_z(order[d]), "pz", 0, "pz", z_recv.at[columns[g], z])
            else:
                keep[g, d] = both

    away, stay = range(zn - 1), range(zn - 1, zn)
    for g in range(zn):
        multiply(g)
        if g == 0:
            forward_down(far)
        over_x(g, away)
        if g > 0:
            over_z(g - 1, away)
    for g in range(zn):
        over_x(g, stay)
    over_z(zn - 1, away)
    for g in range(zn):
        over_z(g, stay)
    leaving = []
    arrived(z_recv.at[:, pl.ds(0, zn - 1)], "pz", 0)
    for g, zz in enumerate(columns):
        total = keep[g, zn - 1]
        for frm in arrivals:
            total += z_recv[zz, frm].astype(f32)
        where = pl.ds(pl.multiple_of(zz * two, two), two)
        result[:, where] = (own_stream[x, :, where].astype(f32) + total).astype(bf16)
        leave = pltpu.make_async_copy(result.at[:, where], out_ref.at[:, where], in_s.at[len(pairs) + g])
        leave.start()
        leaving.append(leave)
    all_sent(lat_all.at[pl.ds(0, zn - 1), 0], "lat")
    all_sent(lat_all.at[:, 0], "lat_o")
    all_sent(w_full.at[pl.ds(0, sp - 1)], "weights")
    all_sent(dn_full.at[pl.ds(0, sp - 1)], "down")
    all_sent(nrm.at[0], "own")
    all_sent(nrm.at[pl.ds(0, zn - 1), pl.ds(0, 3)], "normed")
    all_sent(att_recv.at[pl.ds(0, 3)], "at")
    all_sent(nar_recv.at[pl.ds(0, 3)], "an")
    all_sent(halo_send, "h")
    all_sent(c_send, "pc")
    all_sent(x_send, "px")
    all_sent(z_send.at[:, pl.ds(0, zn - 1)], "pz")

    @pl.when(inner == 1)
    def _():
        all_sent(nrm.at[0, pl.ds(0, 2)], "relay")

    with jax.named_scope("leave"):
        for leave in leaving:
            leave.wait()


def kernel_body(zn, *args):
    (queries, latents, shared_key, expand_weight, residual, out_weight, norm_gain,
     gate_weight, value_weight, conv_weight, down_weight) = args
    rows, width = residual.shape
    sub = down_weight.shape[0] // zn
    share = rows // 4
    d_own = gate_weight.shape[0]
    group = 2 * down_weight.shape[1]
    bf16, f32 = jnp.bfloat16, jnp.float32
    halo_lanes = -(-sub // 128) * 128
    V, DMA = pltpu.VMEM, pltpu.SemaphoreType.DMA
    return pl.pallas_call(
        functools.partial(layer_kernel, zn),
        out_shape=jax.ShapeDtypeStruct((share, width), bf16),
        in_specs=[pl.BlockSpec(memory_space=pl.ANY)] * 11,
        out_specs=pl.BlockSpec(memory_space=pl.ANY),
        scratch_shapes=[
            V((queries.shape[1], rows), bf16),
            V(latents.shape, bf16),
            V((ROPE, rows), bf16),
            V(conv_weight.shape, bf16),
            V((width,), bf16),
            V(expand_weight.shape, bf16),
            V((2, share, width), bf16),
            V(out_weight.shape, bf16),
            V(gate_weight.shape, bf16),
            V(value_weight.shape, bf16),
            V(down_weight.shape, bf16),
            V((zn, 2, 4, share // 2, 2 * latents.shape[1] + 2 * ROPE), bf16),
            V((2, 2, share, VAL_A), bf16),
            V((4, 2, share, VAL_A), bf16),
            V((2, 2, share // 2, 2 * VAL_B), bf16),
            V((4, 2, share // 2, 2 * VAL_B), bf16),
            V((2, share, width), bf16),
            V((zn, 4, 2, share // 2, width), bf16),
            V((zn, 2, d_own // 2, 2 * sub), bf16),
            V((2 * zn, 2, d_own // 2, 2 * sub), bf16),
            V((2 * zn, sub, down_weight.shape[1]), bf16),
            V((zn, rows, 2 * sub), bf16),
            V((zn, rows, sub), bf16),
            V((2 * zn, halo_lanes), f32),
            V((2 * zn, halo_lanes), f32),
            V((zn, zn, 4, share, group), f32),
            V((zn, zn, 2, share, group), bf16),
            V((zn, zn, 2, share, group), bf16),
            V((zn, zn, share, group), f32),
            V((zn, zn, share, group), bf16),
            V((zn, zn, share, group), bf16),
            V((zn, zn, share, group), bf16),
            V((zn, zn, share, group), bf16),
            V((share, width), bf16),
            DMA((12 + zn,)),
            DMA((len(GROUPS),)),
            DMA((semaphore_places(zn)[1],)),
        ],
        compiler_params=pltpu.CompilerParams(collective_id=0, has_side_effects=True),
    )(queries.T, latents, shared_key.T, conv_weight, norm_gain, expand_weight, residual,
      out_weight, gate_weight, value_weight, down_weight)


def pick(*args):
    zn = lax.axis_size("sp") // 2
    hidden = args[10].shape[0]
    sub = hidden // zn
    fits = (
        lax.axis_size("sp") == 8
        and lax.axis_size("tp") == 4
        and hidden % zn == 0
        and sub % 64 == 0
        and args[7].shape[0] % 128 == 0
        and args[0].shape[0] % 128 == 0
        and args[4].shape[1] % args[0].shape[0] == 0
        and args[9].shape[0] == 3
    )
    return kernel_body(zn, *args) if fits else body(*args)


def solution(mesh):
    in_specs = (
        P("sp", "tp"),
        P("sp", None),
        P("sp", None),
        P(None, "tp"),
        P("sp", None),
        P(),
        P(),
        P("sp", "tp"),
        P("sp", "tp"),
        P(None, "tp"),
        P("tp", "sp"),
    )
    out_specs = P(("sp", "tp"), None)
    return jax.shard_map(pick, mesh=mesh, in_specs=in_specs, out_specs=out_specs, check_vma=False)
```

```python
import functools
import math

import jax
import jax.numpy as jnp
from jax import lax
from jax.experimental import pallas as pl
from jax.experimental.pallas import tpu as pltpu
from jax.sharding import PartitionSpec as P

NOPE_A = 128
VAL_A = 128
NOPE_B = 64
VAL_B = 64
ROPE = 64


def padded_2(block, sides, width):
    for axis, dim in sides:
        count = lax.axis_size(axis)
        forward = [(i, i + 1) for i in range(count - 1)]
        backward = [(target, source) for source, target in forward]
        low = lax.ppermute(
            lax.slice_in_dim(block, block.shape[dim] - width, None, axis=dim), axis, forward
        )
        high = lax.ppermute(lax.slice_in_dim(block, 0, width, axis=dim), axis, backward)
        block = jnp.concatenate([low, block, high], axis=dim)
    return block


def tables(positions, width):
    half_width = width // 2
    frequency = 10000.0 ** (-jnp.arange(half_width, dtype=jnp.float32) / half_width)
    angles = positions.astype(jnp.float32)[:, None] * frequency[None, :]
    return (jnp.cos(angles), jnp.sin(angles))


def rotate(vectors, cos_table, sine_table):
    half_width = vectors.shape[-1] // 2
    first_half = vectors[:, :half_width].astype(jnp.float32)
    second_half = vectors[:, half_width:].astype(jnp.float32)
    turned = jnp.concatenate(
        [
            first_half * cos_table - second_half * sine_table,
            second_half * cos_table + first_half * sine_table,
        ],
        axis=1,
    )
    return turned.astype(jnp.bfloat16)


def normalize(stream, norm_gain):
    stream_f = stream.astype(jnp.float32)
    scaled = stream_f * lax.rsqrt(jnp.mean(stream_f * stream_f, axis=1, keepdims=True) + 1e-06)
    return (scaled * norm_gain.astype(jnp.float32)).astype(jnp.bfloat16)


def update(running, q_content, q_turned, k_content, k_turned, values, score_scale):
    row_max, row_sum, weighted = running
    scores = (
        jnp.einsum("qd,kd->qk", q_content, k_content, preferred_element_type=jnp.float32)
        + jnp.einsum("qd,kd->qk", q_turned, k_turned, preferred_element_type=jnp.float32)
    ) * score_scale
    new_max = jnp.maximum(row_max, jnp.max(scores, axis=1))
    weights = jnp.exp(scores - new_max[:, None])
    row_sum = jnp.sum(weights, axis=1)
    weighted = jnp.dot(weights.astype(jnp.bfloat16), values, preferred_element_type=jnp.float32)
    return (new_max, row_sum, weighted)


def body(
    queries,
    latents,
    shared_key,
    expand_weight,
    residual,
    out_weight,
    norm_gain,
    gate_weight,
    value_weight,
    conv_weight,
    down_weight,
):
    tok_rows = queries.shape[0]
    q_width = NOPE_A + NOPE_B + 2 * ROPE
    kv_width = NOPE_A + VAL_A + NOPE_B + VAL_B
    positions = lax.axis_index("sp") * tok_rows + jnp.arange(tok_rows, dtype=jnp.int32)
    cos_table, sine_table = tables(positions, ROPE)
    key_turned = rotate(shared_key, cos_table, sine_table)
    scale_wide = (NOPE_A + ROPE) ** (-0.5)
    scale_narrow = (NOPE_B + ROPE) ** (-0.5)
    initial = []
    pair_index = 0
    q_base = pair_index * q_width
    rotary_base = q_base + NOPE_A + NOPE_B
    wide_content = queries[:, q_base : q_base + NOPE_A]
    narrow_content = queries[:, q_base + NOPE_A : rotary_base]
    wide_turned = rotate(queries[:, rotary_base : rotary_base + ROPE], cos_table, sine_table)
    narrow_turned = rotate(
        queries[:, rotary_base + ROPE : rotary_base + 2 * ROPE], cos_table, sine_table
    )
    query_parts = [(wide_content, wide_turned, narrow_content, narrow_turned)]
    lowest = jnp.full((tok_rows,), -1e30, jnp.float32)
    empty_sum = jnp.zeros((tok_rows,), jnp.float32)
    initial += [
        lowest,
        empty_sum,
        jnp.zeros((tok_rows, VAL_A), jnp.float32),
        lowest,
        empty_sum,
        jnp.zeros((tok_rows, VAL_B), jnp.float32),
    ]
    initial = tuple(initial)
    pieces = (
        lax.all_gather(latents, "sp", axis=0, tiled=True),
        lax.all_gather(key_turned, "sp", axis=0, tiled=True),
    )
    expanded = jnp.dot(pieces[0], expand_weight, preferred_element_type=jnp.float32).astype(
        jnp.bfloat16
    )
    turned_keys = pieces[1]
    result = []
    pair_index = 0
    wide_content, wide_turned, narrow_content, narrow_turned = query_parts[pair_index]
    kv_base = pair_index * kv_width
    narrow_base = kv_base + NOPE_A + VAL_A
    wide_keys = expanded[:, kv_base : kv_base + NOPE_A]
    wide_values = expanded[:, kv_base + NOPE_A : narrow_base]
    narrow_keys = expanded[:, narrow_base : narrow_base + NOPE_B]
    narrow_values = expanded[:, narrow_base + NOPE_B : narrow_base + NOPE_B + VAL_B]
    absorb_offset = 6 * pair_index
    result += list(
        update(
            initial[absorb_offset : absorb_offset + 3],
            wide_content,
            wide_turned,
            wide_keys,
            turned_keys,
            wide_values,
            scale_wide,
        )
    )
    result += list(
        update(
            initial[absorb_offset + 3 : absorb_offset + 6],
            narrow_content,
            narrow_turned,
            narrow_keys,
            turned_keys,
            narrow_values,
            scale_narrow,
        )
    )
    running = tuple(result)
    outputs = []
    pair_index = 0
    for group_index in range(2):
        offset = 6 * pair_index + 3 * group_index
        outputs.append((running[offset + 2] / running[offset + 1][:, None]).astype(jnp.bfloat16))
    attended = jnp.concatenate(outputs, axis=1)
    share = tok_rows // lax.axis_size("tp")
    tp_index = lax.axis_index("tp")
    all_heads = lax.all_gather(attended, "tp", axis=1, tiled=True)
    projected = jnp.dot(all_heads, out_weight, preferred_element_type=jnp.float32)
    stream = (residual.astype(jnp.float32) + projected).astype(jnp.bfloat16)
    normed = normalize(stream, norm_gain)
    stream_own = lax.dynamic_slice_in_dim(stream, tp_index * share, share, 0)
    pieces = (
        lax.all_gather(gate_weight, "sp", axis=0, tiled=True),
        lax.all_gather(value_weight, "sp", axis=0, tiled=True),
    )
    gate_sum = jnp.dot(normed, pieces[0], preferred_element_type=jnp.float32)
    value_sum = jnp.dot(normed, pieces[1], preferred_element_type=jnp.float32)
    gate_pre = gate_sum.astype(jnp.bfloat16)
    value_pre = value_sum.astype(jnp.bfloat16)
    reach = conv_weight.shape[0] // 2
    padded = padded_2(gate_pre, (("sp", 0),), reach)
    mixed_gate = jnp.zeros(gate_pre.shape, jnp.float32)
    for tap in range(conv_weight.shape[0]):
        mixed_gate = mixed_gate + padded[tap : tap + tok_rows].astype(jnp.float32) * conv_weight[
            tap
        ].astype(jnp.float32)
    active = (jax.nn.silu(mixed_gate) * value_pre.astype(jnp.float32)).astype(jnp.bfloat16)
    partial_rows = jnp.dot(
        active,
        lax.all_gather(down_weight, "sp", axis=1, tiled=True),
        preferred_element_type=jnp.float32,
    )
    summed = lax.psum_scatter(
        partial_rows.astype(jnp.bfloat16), "tp", scatter_dimension=0, tiled=True
    ).astype(jnp.float32)
    return (stream_own.astype(jnp.float32) + summed).astype(jnp.bfloat16)


MESH = pl.DeviceIdType.MESH
SINGLE = ("lc", "lco", "wy", "at", "an", "h", "pz")
PER_Z = ("lz", "ly", "lx", "lxy", "dz", "dy", "nc")
PER_HALF = ("wz", "nz", "nx", "pc")
GROUPS = ("lat", "lat_o", "weights", "down", "own", "relay", "normed", "at", "an", "h", "pc", "px", "pz")


def semaphore_places(zn):
    places, count = {}, 0
    for kinds, width in ((SINGLE, 1), (PER_Z, zn), (PER_HALF, 2 * zn), (("px",), zn * zn)):
        for kind in kinds:
            places[kind] = count
            count += width
    return places, count


def layer_kernel(
    zn,
    q_hbm,
    lat_hbm,
    key_hbm,
    conv_hbm,
    gain_hbm,
    expand_hbm,
    res_hbm,
    out_w_hbm,
    gate_hbm,
    value_hbm,
    down_hbm,
    out_ref,
    q_ref,
    lat_ref,
    key_ref,
    conv_ref,
    gain_ref,
    expand_ref,
    res_ref,
    out_w_ref,
    gate_ref,
    value_ref,
    down_ref,
    lat_all,
    att_send,
    att_recv,
    nar_send,
    nar_recv,
    own_stream,
    nrm,
    stage,
    w_full,
    dn_full,
    hbuf,
    abuf,
    halo_send,
    halo_recv,
    part,
    c_send,
    c_recv,
    keep,
    x_send,
    x_recv,
    z_send,
    z_recv,
    result,
    in_s,
    send_s,
    recv_s,
):
    f32, bf16 = jnp.float32, jnp.bfloat16
    s, t = lax.axis_index("sp"), lax.axis_index("tp")
    z, y = s // 2, s % 2
    x, c = t // 2, t % 2
    yo, xo, co = 1 - y, 1 - x, 1 - c
    xt, ct, xct = 2 * xo + c, 2 * x + co, 2 * xo + co
    rows = lat_ref.shape[0]
    share = rows // 4
    packed = share // 2
    rank = lat_ref.shape[1]
    sub = down_ref.shape[0] // zn
    sp = 2 * zn
    deep = gate_ref.shape[0] // 2

    inner = ((z + 1) // 2) % 2
    near = z + 1 - 2 * (z % 2)
    mid = (z + 2) % zn + inner * (zn - 1 - z - (z + 2) % zn)
    far = zn - 1 - z + inner * ((z + 2) % zn - (zn - 1 - z))
    arrivals = (near + inner * (mid - near), mid + inner * (far - mid), far + inner * (near - far))

    def to_z(zz):
        return {"sp": 2 * zz + y, "tp": t}

    y_dev = {"sp": 2 * z + yo, "tp": t}
    x_dev = {"sp": s, "tp": xt}
    c_dev = {"sp": s, "tp": ct}
    xc_dev = {"sp": s, "tp": xct}

    places, _ = semaphore_places(zn)

    def copy_to(src, dst, dev, kind, i, group):
        return pltpu.make_async_remote_copy(
            src_ref=src, dst_ref=dst, send_sem=send_s.at[GROUPS.index(group)],
            recv_sem=recv_s.at[places[kind] + i], device_id=dev, device_id_type=MESH,
        )

    def send(ref, dev, kind, i, group, dst=None):
        copy_to(ref, ref if dst is None else dst, dev, kind, i, group).start()

    def send_if(condition, ref, dev, kind, i, group, dst=None, wait=None):
        @pl.when(condition)
        def _():
            if wait is not None:
                arrived(ref, wait, i)
            send(ref, dev, kind, i, group, dst)

    def arrived(dst, kind, i):
        with jax.named_scope("wait_" + kind):
            copy_to(dst, dst, c_dev, kind, i, "lat").wait_recv()

    def all_sent(ref, group):
        copy_to(ref, ref, c_dev, "lz", 0, group).wait_send()

    barrier = pltpu.get_barrier_semaphore()
    partners = [to_z(near), to_z(mid), to_z(far), y_dev, x_dev, c_dev, xc_dev]
    for dev in partners:
        pl.semaphore_signal(barrier, inc=1, device_id=dev, device_id_type=MESH)

    def res_rows(i):
        return res_hbm.at[pl.ds(pl.multiple_of((2 * i + c) * share, share), share), :]

    pairs = [
        (key_hbm, key_ref),
        (lat_hbm, lat_ref),
        (gate_hbm, gate_ref),
        (value_hbm, value_ref),
        (q_hbm, q_ref),
        (down_hbm, down_ref),
        (expand_hbm, expand_ref),
        (res_rows(0), res_ref.at[0]),
        (res_rows(1), res_ref.at[1]),
        (gain_hbm, gain_ref),
        (conv_hbm, conv_ref),
        (out_w_hbm, out_w_ref),
    ]
    loads = [pltpu.make_async_copy(src, dst, in_s.at[i]) for i, (src, dst) in enumerate(pairs)]
    for load in loads:
        load.start()

    h = ROPE // 2
    step = lax.broadcasted_iota(jnp.int32, (h, rows), 0).astype(f32) * (-math.log(10000.0) / h)
    spot = (s * rows + lax.broadcasted_iota(jnp.int32, (h, rows), 1)).astype(f32)
    angles = spot * jnp.exp(step)
    cos, sine = jnp.cos(angles), jnp.sin(angles)

    def turn(v):
        a, b = v[:h], v[h:]
        return jnp.concatenate([a * cos - b * sine, b * cos + a * sine], axis=0)

    loads[0].wait()
    turned = turn(key_ref[...].astype(f32))
    key_turned = jnp.concatenate([turned, jnp.zeros_like(turned)], axis=0).T.astype(bf16)[:, :ROPE]
    loads[1].wait()
    for i in range(4):
        for j in range(2):
            first = i * share + j * packed
            lat_all[z, y, i, :, j * rank : (j + 1) * rank] = lat_ref[first : first + packed, :]
        lat_all[z, y, i, :, 2 * rank :] = jnp.concatenate(
            [key_turned[i * share : i * share + packed], key_turned[i * share + packed : (i + 1) * share]], axis=1
        )
    with jax.named_scope("barrier"):
        pl.semaphore_wait(barrier, len(partners))

    def lat(zz, yy, q):
        return lat_all.at[zz, yy, q]

    for zz in (far, mid, near):
        send(lat(z, y, t), to_z(zz), "lz", z, "lat")
    send(lat(z, y, t), y_dev, "ly", z, "lat_o")
    send(lat(z, y, xt), y_dev, "lxy", z, "lat_o")
    loads[2].wait()
    loads[3].wait()
    for k in range(zn):
        for i in range(2):
            stage[k, i, :, :sub] = gate_ref[i * deep : (i + 1) * deep, k * sub : (k + 1) * sub]
            stage[k, i, :, sub:] = value_ref[i * deep : (i + 1) * deep, k * sub : (k + 1) * sub]
    send(stage.at[near], to_z(near), "wz", 2 * z, "weights", w_full.at[s])
    for zz, i in ((mid, 0), (mid, 1), (far, 0), (far, 1)):
        send(stage.at[zz, i], to_z(zz), "wz", 2 * z + i, "weights", w_full.at[s, i])
    w_full[s] = stage[z]

    for zz in arrivals:
        arrived(lat(zz, y, t), "lz", zz)
        send(lat(zz, y, t), y_dev, "ly", zz, "lat_o")
        send(lat(zz, y, t), x_dev, "lx", zz, "lat")
        send(lat(zz, y, t), c_dev, "lc", 0, "lat")
    arrived(lat(z, yo, t), "ly", z)
    send(lat(z, yo, t), c_dev, "lco", 0, "lat_o")
    arrived(lat(z, yo, xt), "lxy", z)
    send(lat(z, yo, xt), c_dev, "lco", 0, "lat_o")
    for i, zz in enumerate(arrivals):
        arrived(lat(zz, yo, t), "ly", zz)
        if i < 2:
            send(lat(zz, yo, t), x_dev, "lxy", zz, "lat_o")
        send(lat(zz, yo, t), c_dev, "lco", 0, "lat_o")
        arrived(lat(zz, y, xt), "lx", zz)
        if i == 2:
            send(lat(zz, y, xt), y_dev, "lxy", zz, "lat_o")
        send(lat(zz, y, xt), c_dev, "lc", 0, "lat")
    send(w_full.at[s], y_dev, "wy", 0, "weights")

    loads[4].wait()
    rot = NOPE_A + NOPE_B
    q = q_ref[...].astype(f32)
    q_wide = q[:NOPE_A].T.astype(bf16)
    pair = jnp.concatenate([q[NOPE_A:rot], turn(q[rot : rot + ROPE])], axis=0).T.astype(bf16)
    q_narrow, q_wide_t = pair[:, :NOPE_B], pair[:, NOPE_B:]
    turned = turn(q[rot + ROPE :])
    q_narrow_t = jnp.concatenate([turned, jnp.zeros_like(turned)], axis=0).T.astype(bf16)[:, :ROPE]
    loads[5].wait()
    dn_full[s] = down_ref[pl.ds(pl.multiple_of(z * sub, sub), sub), :]
    loads[6].wait()

    def pass_far(zz):
        arrived(lat(zz, yo, xt), "lxy", zz)
        send(lat(zz, yo, xt), c_dev, "lco", 0, "lat_o")

    expand_w = expand_ref[...]
    empty = jnp.zeros((rows, ROPE), bf16)
    nb = NOPE_A + VAL_A
    dims = (((1,), (1,)), ((), ()))

    def score(qc, qt, kc, keys_t, scale):
        turned_scores = [
            lax.dot_general(jnp.concatenate(two, axis=1), keys_t, dims, preferred_element_type=f32)
            for two in ([qt, empty], [empty, qt])
        ]
        return (
            lax.dot_general(qc, kc, dims, preferred_element_type=f32) + jnp.concatenate(turned_scores, axis=1)
        ) * scale

    def scored(yy):
        whole = lat_all[:, yy].reshape(zn * 4 * packed, lat_all.shape[4])
        expanded = jnp.concatenate(
            [
                jnp.dot(whole[:, j * rank : (j + 1) * rank], expand_w, preferred_element_type=f32).astype(bf16)
                for j in range(2)
            ],
            axis=0,
        )
        keys_t = whole[:, 2 * rank :]
        return (
            score(q_wide, q_wide_t, expanded[:, :NOPE_A], keys_t, (NOPE_A + ROPE) ** -0.5),
            expanded[:, NOPE_A:nb],
            score(q_narrow, q_narrow_t, expanded[:, nb : nb + NOPE_B], keys_t, (NOPE_B + ROPE) ** -0.5),
            expanded[:, nb + NOPE_B : nb + NOPE_B + VAL_B],
        )

    pass_far(arrivals[0])

    @pl.when(c == 1)
    def _():
        pass_far(arrivals[1])
        pass_far(arrivals[2])

    arrived(lat_all.at[pl.ds(0, zn - 1), 0, pl.ds(0, 2)], "lc", 0)
    here = scored(y)

    @pl.when(c == 0)
    def _():
        pass_far(arrivals[1])
        pass_far(arrivals[2])

    arrived(lat_all.at[:, 0, pl.ds(0, 2)], "lco", 0)
    there = scored(yo)

    def attend(head):
        scores = jnp.concatenate([here[2 * head], there[2 * head]], axis=1)
        v = jnp.concatenate([here[2 * head + 1], there[2 * head + 1]], axis=0)
        w = jnp.exp(scores - jnp.max(scores, axis=1, keepdims=True))
        total = jnp.sum(w, axis=1, keepdims=True)
        return (jnp.dot(w.astype(bf16), v, preferred_element_type=f32) / total).astype(bf16)

    def to_heads(sent, received, kind):
        send(sent.at[c], x_dev, kind, 0, kind, received.at[t])
        send(sent.at[co], xc_dev, kind, 0, kind, received.at[t])
        send(sent.at[co], c_dev, kind, 0, kind, received.at[t])
        received[t] = sent[c]

    vals = VAL_A + VAL_B
    wide = attend(0)
    for i in range(4):
        att_send[i % 2, i // 2] = wide[i * share : (i + 1) * share, :]
    to_heads(att_send, att_recv, "at")
    narrow = attend(1)
    for i in range(4):
        part_rows = narrow[i * share : (i + 1) * share, :]
        nar_send[i % 2, i // 2] = jnp.concatenate([part_rows[:packed], part_rows[packed:]], axis=1)
    to_heads(nar_send, nar_recv, "an")

    arrived(w_full.at[2 * near + y], "wz", 2 * near)
    send(w_full.at[2 * near + y], y_dev, "wy", 0, "weights")

    def forward_weights(turn):
        for zz in (mid, far):
            for i in range(2):
                turns = (inner * c, (1 - inner * c) * (1 - i + i * inner), i * (1 - inner))
                if turn == 2 and i == 0:
                    continue

                @pl.when(turns[turn] == 1)
                def _():
                    arrived(w_full.at[2 * zz + y, i], "wz", 2 * zz + i)
                    send(w_full.at[2 * zz + y, i], y_dev, "wy", 0, "weights")

    forward_weights(0)
    for load in loads[7:]:
        load.wait()
    arrived(att_recv.at[pl.ds(0, 3)], "at", 0)
    arrived(nar_recv.at[pl.ds(0, 3)], "an", 0)

    projected = None
    for i in range(4):
        narrow = [nar_recv[i, j, :, k * VAL_B : (k + 1) * VAL_B] for j in range(2) for k in range(2)]
        term = jnp.dot(
            jnp.concatenate([att_recv[i].reshape(2 * share, VAL_A), jnp.concatenate(narrow, axis=0)], axis=1),
            out_w_ref[i * vals : (i + 1) * vals, :], preferred_element_type=f32,
        )
        projected = term if projected is None else projected + term
    stream = (res_ref[...].reshape(2 * share, res_ref.shape[2]).astype(f32) + projected).astype(bf16)
    stream_f = stream.astype(f32)
    scaled = stream_f * lax.rsqrt(jnp.mean(stream_f * stream_f, axis=1, keepdims=True) + 1e-06)
    normed = (scaled * gain_ref[...].astype(f32).reshape(1, scaled.shape[1])).astype(bf16)
    piece_rows = share // 2
    for i in range(2):
        for j in range(2):
            first = i * share + j * piece_rows
            nrm[z, 2 * i + c, j] = normed[first : first + piece_rows]
        own_stream[i] = stream[i * share : (i + 1) * share]

    for j in range(2):
        send(nrm.at[z, t, j], to_z(mid), "nz", 2 * z + j, "own")
        send(nrm.at[z, t, j], to_z(near), "nz", 2 * z + j, "own")
    send_if(inner == 1, nrm.at[z, t, 0], to_z(far), "nz", 2 * z + 0, "relay")
    send(nrm.at[z, t], c_dev, "nc", z, "own")
    send(nrm.at[z, xt], c_dev, "nc", z, "own")
    send(dn_full.at[s], y_dev, "dy", z, "down")
    forward_weights(1)

    outer_turns = ((near, 0), (near, 1), (mid, 0), (far, 0), (mid, 1), (far, 1))
    inner_turns = ((mid, 0), (far, 0), (mid, 1), (far, 1), (near, 0), (near, 1))
    turns = [(a + inner * (b - a), i + inner * (j - i)) for (a, i), (b, j) in zip(outer_turns, inner_turns)]

    def from_x(n):
        zz, j = turns[n]
        arrived(nrm.at[zz, xt, j], "nx", 2 * zz + j)
        send(nrm.at[zz, xt, j], c_dev, "nc", zz, "normed")

    def send_down(zz, cond):
        piece = down_ref.at[pl.ds(pl.multiple_of(zz * sub, sub), sub), :]
        if cond is None:
            send(piece, to_z(zz), "dz", z, "down", dn_full.at[s])
        else:
            send_if(cond, piece, to_z(zz), "dz", z, "down", dn_full.at[s])

    for n, (zz, j) in enumerate(turns):
        blk = nrm.at[zz, t, j]
        arrived(blk, "nz", 2 * zz + j)
        if 0 < n < 4:
            send_if(inner == 1, blk, to_z(near), "nz", 2 * zz + j, "relay")
        send(blk, x_dev, "nx", 2 * zz + j, "normed")
        send(blk, c_dev, "nc", zz, "normed")
        if n == 0:
            forward_weights(2)
        if n == 2:
            send_down(mid, ((1 - inner) * c) == 1)
        if n > 1:
            from_x(n - 2)
    send_down(near, None)
    send_down(mid, ((1 - inner) * c) == 0)
    send_down(far, None)
    arrived(w_full.at[pl.ds(0, zn)], "wy", 0)
    weights = w_full[...].reshape(sp * 2 * deep, 2 * sub)

    def forward_down(zz):
        arrived(dn_full.at[2 * zz + y], "dz", zz)
        send(dn_full.at[2 * zz + y], y_dev, "dy", zz, "down")

    def mix(zz):
        hbuf[zz] = jnp.dot(
            nrm[zz].reshape(rows, nrm.shape[4]), weights, preferred_element_type=f32
        ).astype(bf16)

    def block_here(zz):
        arrived(nrm.at[zz, pl.ds(0, 2)], "nc", zz)

    columns = (z, near + inner * (mid - near), mid + inner * (near - mid), far)
    block_here(z)
    mix(z)
    for i, zz in enumerate(arrivals):
        if i > 0:
            from_x(len(turns) - 3 + i)
        block_here(zz)
        mix(zz)

    wide_lanes = halo_send.shape[1]
    for k in range(zn):
        g = hbuf[k, :, :wide_lanes].astype(f32)
        halo_send[k : k + 1, :] = g[rows - 1 : rows, :]
        halo_send[zn + k : zn + k + 1, :] = g[0:1, :]
    send(halo_send, y_dev, "h", 0, "h", halo_recv)

    forward_down(columns[1])
    conv_all = conv_ref[...].astype(f32)
    pieces = [conv_all[:, k * sub : (k + 1) * sub] for k in range(zn)]
    taps = pieces[0]
    for k in range(1, zn):
        taps = jnp.where(z == k, pieces[k], taps)
    taps = jnp.concatenate([taps, jnp.zeros((taps.shape[0], wide_lanes - sub), f32)], axis=1)

    def activate(k, first, count, before=None, after=None):
        g = hbuf[k, first : first + count, :wide_lanes].astype(f32)
        row_id = lax.broadcasted_iota(jnp.int32, (count, wide_lanes), 0)
        up, down = pltpu.roll(g, 1, 0), pltpu.roll(g, count - 1, 0)
        if before is not None:
            up = jnp.where(row_id == 0, before, up)
        if after is not None:
            down = jnp.where(row_id == count - 1, after, down)
        mixed = up * taps[0:1] + g * taps[1:2] + down * taps[2:3]
        mixed = mixed[:, :sub]
        v = hbuf[k, first : first + count].astype(f32)[:, sub:]
        return (mixed / (1.0 + jnp.exp(-mixed)) * v).astype(bf16)

    edge = rows // 8
    for k in range(zn):
        abuf[k] = activate(k, 0, rows)
    arrived(halo_recv, "h", 0)
    forward_down(columns[2])
    nothing = jnp.zeros((1, wide_lanes), f32)
    for k in range(zn):
        before_low = halo_recv[k - 1 : k, :] if k > 0 else nothing
        before = jnp.where(y == 0, before_low, halo_recv[k : k + 1, :])
        after_high = halo_recv[zn + k + 1 : zn + k + 2, :] if k < zn - 1 else nothing
        after = jnp.where(y == 0, halo_recv[zn + k : zn + k + 1, :], after_high)
        abuf[k, :edge] = activate(k, 0, 2 * edge, before=before)[:edge]
        abuf[k, rows - edge :] = activate(k, rows - 2 * edge, 2 * edge, after=after)[edge:]

    order = (far, mid, near, z)
    depth = dn_full.shape[2]
    two = 2 * depth

    def multiply(g):
        zz = columns[g]
        arrived(dn_full.at[2 * zz + yo], "dy", zz)
        down = jnp.concatenate([dn_full[2 * zz], dn_full[2 * zz + 1]], axis=1)
        for d, to in enumerate(order):
            p = jnp.dot(abuf[to], down, preferred_element_type=f32)
            part[g, d] = p.reshape(4, share, two)
            for i in range(2):
                c_send[g, d, i] = part[g, d, 2 * i + co].astype(bf16)
            if d % 2 == 1:
                ready = pl.ds(d - 1, 2)
                send(c_send.at[g, ready], c_dev, "pc", 2 * g + d // 2, "pc", c_recv.at[g, ready])

    def over_x(g, turns):
        for d in turns:
            if d % 2 == 0:
                arrived(c_recv.at[g, pl.ds(d, 2)], "pc", 2 * g + d // 2)
            x_send[g, d] = (part[g, d, xt] + c_recv[g, d, xo].astype(f32)).astype(bf16)
            send(x_send.at[g, d], x_dev, "px", g * zn + d, "px", x_recv.at[g, d])
            keep[g, d] = part[g, d, t] + c_recv[g, d, x].astype(f32)

    def over_z(g, turns):
        for d in turns:
            arrived(x_recv.at[g, d], "px", g * zn + d)
            both = keep[g, d] + x_recv[g, d].astype(f32)
            if d < zn - 1:
                z_send[g, d] = both.astype(bf16)
                send(z_send.at[g, d], to_z(order[d]), "pz", 0, "pz", z_recv.at[columns[g], z])
            else:
                keep[g, d] = both

    away, stay = range(zn - 1), range(zn - 1, zn)
    for g in range(zn):
        multiply(g)
        if g == 0:
            forward_down(far)
        over_x(g, away)
        if g > 0:
            over_z(g - 1, away)
    for g in range(zn):
        over_x(g, stay)
    over_z(zn - 1, away)
    for g in range(zn):
        over_z(g, stay)
    leaving = []
    arrived(z_recv.at[:, pl.ds(0, zn - 1)], "pz", 0)
    for g, zz in enumerate(columns):
        total = keep[g, zn - 1]
        for frm in arrivals:
            total += z_recv[zz, frm].astype(f32)
        where = pl.ds(pl.multiple_of(zz * two, two), two)
        result[:, where] = (own_stream[x, :, where].astype(f32) + total).astype(bf16)
        leave = pltpu.make_async_copy(result.at[:, where], out_ref.at[:, where], in_s.at[g])
        leave.start()
        leaving.append(leave)
    all_sent(lat_all.at[pl.ds(0, zn - 1), 0], "lat")
    all_sent(lat_all.at[:, 0], "lat_o")
    all_sent(w_full.at[pl.ds(0, sp - 1)], "weights")
    all_sent(dn_full.at[pl.ds(0, sp - 1)], "down")
    all_sent(nrm.at[0], "own")
    all_sent(nrm.at[pl.ds(0, zn - 1), pl.ds(0, 3)], "normed")
    all_sent(att_recv.at[pl.ds(0, 3)], "at")
    all_sent(nar_recv.at[pl.ds(0, 3)], "an")
    all_sent(halo_send, "h")
    all_sent(c_send, "pc")
    all_sent(x_send, "px")
    all_sent(z_send.at[:, pl.ds(0, zn - 1)], "pz")

    @pl.when(inner == 1)
    def _():
        all_sent(nrm.at[0, pl.ds(0, 2)], "relay")

    with jax.named_scope("leave"):
        for leave in leaving:
            leave.wait()


def kernel_body(zn, *args):
    (queries, latents, shared_key, expand_weight, residual, out_weight, norm_gain,
     gate_weight, value_weight, conv_weight, down_weight) = args
    rows, width = residual.shape
    sub = down_weight.shape[0] // zn
    share = rows // 4
    d_own = gate_weight.shape[0]
    group = 2 * down_weight.shape[1]
    bf16, f32 = jnp.bfloat16, jnp.float32
    halo_lanes = -(-sub // 128) * 128
    V, DMA = pltpu.VMEM, pltpu.SemaphoreType.DMA
    return pl.pallas_call(
        functools.partial(layer_kernel, zn),
        out_shape=jax.ShapeDtypeStruct((share, width), bf16),
        in_specs=[pl.BlockSpec(memory_space=pl.ANY)] * 11,
        out_specs=pl.BlockSpec(memory_space=pl.ANY),
        scratch_shapes=[
            V((queries.shape[1], rows), bf16),
            V(latents.shape, bf16),
            V((ROPE, rows), bf16),
            V(conv_weight.shape, bf16),
            V((width,), bf16),
            V(expand_weight.shape, bf16),
            V((2, share, width), bf16),
            V(out_weight.shape, bf16),
            V(gate_weight.shape, bf16),
            V(value_weight.shape, bf16),
            V(down_weight.shape, bf16),
            V((zn, 2, 4, share // 2, 2 * latents.shape[1] + 2 * ROPE), bf16),
            V((2, 2, share, VAL_A), bf16),
            V((4, 2, share, VAL_A), bf16),
            V((2, 2, share // 2, 2 * VAL_B), bf16),
            V((4, 2, share // 2, 2 * VAL_B), bf16),
            V((2, share, width), bf16),
            V((zn, 4, 2, share // 2, width), bf16),
            V((zn, 2, d_own // 2, 2 * sub), bf16),
            V((2 * zn, 2, d_own // 2, 2 * sub), bf16),
            V((2 * zn, sub, down_weight.shape[1]), bf16),
            V((zn, rows, 2 * sub), bf16),
            V((zn, rows, sub), bf16),
            V((2 * zn, halo_lanes), f32),
            V((2 * zn, halo_lanes), f32),
            V((zn, zn, 4, share, group), f32),
            V((zn, zn, 2, share, group), bf16),
            V((zn, zn, 2, share, group), bf16),
            V((zn, zn, share, group), f32),
            V((zn, zn, share, group), bf16),
            V((zn, zn, share, group), bf16),
            V((zn, zn, share, group), bf16),
            V((zn, zn, share, group), bf16),
            V((share, width), bf16),
            DMA((12,)),
            DMA((len(GROUPS),)),
            DMA((semaphore_places(zn)[1],)),
        ],
        compiler_params=pltpu.CompilerParams(collective_id=0, has_side_effects=True),
    )(queries.T, latents, shared_key.T, conv_weight, norm_gain, expand_weight, residual,
      out_weight, gate_weight, value_weight, down_weight)


def pick(*args):
    zn = lax.axis_size("sp") // 2
    hidden = args[10].shape[0]
    sub = hidden // zn
    fits = (
        lax.axis_size("sp") == 8
        and lax.axis_size("tp") == 4
        and hidden % zn == 0
        and sub % 64 == 0
        and args[7].shape[0] % 128 == 0
        and args[0].shape[0] % 128 == 0
        and args[4].shape[1] % args[0].shape[0] == 0
        and args[9].shape[0] == 3
    )
    return kernel_body(zn, *args) if fits else body(*args)


def solution(mesh):
    in_specs = (
        P("sp", "tp"),
        P("sp", None),
        P("sp", None),
        P(None, "tp"),
        P("sp", None),
        P(),
        P(),
        P("sp", "tp"),
        P("sp", "tp"),
        P(None, "tp"),
        P("tp", "sp"),
    )
    out_specs = P(("sp", "tp"), None)
    return jax.shard_map(pick, mesh=mesh, in_specs=in_specs, out_specs=out_specs, check_vma=False)
```
